512 devices in a mesh: sp: 32 (over z, x), tp: 16 (over y, core).
Axes of the slice: x: 4, y: 8, z: 8, core: 2. Of those that a mesh axis runs over, the one named last changes fastest.
Arguments:
- mixer_out: bfloat16 [4096, 2048], P('sp'), may hold values from -6 to 6
- out_grad: bfloat16 [4096, 2048], P('sp'), may hold values from -2 to 2
- route_ids: int32 [4096, 2], P('sp'), may hold values from 0 to 31, all different within a row; in each aligned block of 128 rows (0 to 127, 128 to 255, ...) at most 16 rows name the same one
- route_weights: float32 [4096, 2], P('sp'), may hold values from 0.2 to 1.2
- gate_branch: bfloat16 [4096, 2048], P('sp', 'tp'), may hold values from -4 to 4
- states: float32 [4096, 2048], P('sp', 'tp'), may hold values from -6 to 6
- decay: float32 [4096, 2048], P('sp', 'tp'), may hold values from 0 to 1
- w_proj: bfloat16 [2048, 2048], P(None, 'tp'), may hold values from -0.125 to 0.125
- w_gate: bfloat16 [32, 2048, 2048], P('sp', 'tp'), may hold values from -0.125 to 0.125
- w_up: bfloat16 [32, 2048, 2048], P('sp', 'tp'), may hold values from -0.125 to 0.125
- w_down: bfloat16 [32, 2048, 2048], P('sp', 'tp'), may hold values from -0.125 to 0.125
Outputs:
- grad_w_gate: bfloat16 [32, 2048, 2048], P('sp', 'tp')
- grad_w_up: bfloat16 [32, 2048, 2048], P('sp', 'tp')
- grad_w_down: bfloat16 [32, 2048, 2048], P('sp', 'tp')
- grad_w_proj: float32 [2048, 2048], P('sp', 'tp')
- grad_branch: bfloat16 [4096, 2048], P('sp', 'tp')
- grad_drive: float32 [4096, 2048], P('sp', 'tp')
- grad_decay: float32 [4096, 2048], P('sp', 'tp')
The draws below stay inside these ranges and needn't reach their ends.
Inputs may be any that keep to these rules, and one draw needn't show every extreme that they name: `route_ids`: each row names 2 different experts. In the rows of one index of sp no expert is named more than 16 times, a bound that some block reaches.
All inputs are finite; a program needn't handle non-finite values.
Results may differ from the reference program's by a relative error of at most 0.02.
Values may be sent and summed in bfloat16 or wider, within the bound.
No kernel may reach another device: no remote copies, remote signals or barrier semaphores. Data moves between devices by JAX's collectives and lax.ppermute only.
A program may use at most 64 MiB of HBM per device.

```python
import math
import jax
import jax.numpy as jnp
import numpy as np
from jax import lax

D = 2048
D_RNN = 2048
F = 2048
TOP = 2
TOK_DEV = 128
EXPERTS = 32
TOKENS = 4096
CAP = 16
N_SP = 32
N_TP = 16


def draw_decay(key, part):
    keys = jax.random.split(jax.random.fold_in(key, 17), 5)
    fast_share = 0.5
    fast = jax.random.uniform(keys[0], (D_RNN,), jnp.float32) < fast_share
    slow_rate = jax.random.uniform(keys[1], (D_RNN,), jnp.float32, 0.25, 0.8) / TOKENS
    fast_rate = jnp.exp(jax.random.uniform(keys[2], (D_RNN,), jnp.float32, jnp.log(0.01), jnp.log(1.0 / 30.0)))
    base_rate = jnp.where(fast, fast_rate, slow_rate)
    spans = TOKENS // 64
    factor = jnp.exp(jax.random.uniform(keys[3], (spans, 1), jnp.float32, jnp.log(0.4), jnp.log(1.6)))
    noise = jax.random.uniform(keys[4], (TOKENS, D_RNN), jnp.float32, 0.5, 1.5)
    return jnp.exp(-(base_rate[None, :] * jnp.repeat(factor, 64, axis=0) * noise))


def strengthened(array, own_key, source, target, shards_of, factor):
    owner, partner = [(jnp.arange(array.shape[dim]) // (array.shape[dim] // shards_of)).reshape([-1 if axis == dim else 1 for axis in range(array.ndim)]) for dim in (source, target)]
    chosen = jax.random.permutation(own_key, shards_of)[partner]
    strong = (owner == chosen) | (owner == (partner + shards_of // 2) % shards_of)
    return jnp.where(strong, factor * array, array)


def levels(stream_key, extent, cuts, smallest, largest):
    def one(axis_at, shards_of):
        steps = jax.random.uniform(jax.random.fold_in(jax.random.fold_in(stream_key, 6), axis_at), (shards_of,), jnp.float32, smallest / len(cuts), largest / len(cuts))
        return jnp.repeat(jnp.exp(steps), extent[axis_at] // shards_of).reshape((-1,) + (1,) * (len(extent) - axis_at - 1))

    loudness = one(*cuts[0])
    for cut in cuts[1:]:
        loudness = loudness * one(*cut)
    return loudness


def shared_out(key, own, number, rows, amount, top, most, skew):
    sequence = jax.random.permutation(key, amount)
    crowded, common = shares(amount, rows * top, most, skew, True), shares(amount, rows * top, most, skew, False)
    places = jnp.arange(amount)

    def named(lengths, turn):
        used = int((lengths > 0).sum())
        fixed = max(1, used // 4)
        passed = fixed + (places - fixed + turn * (used - fixed)) % max(1, amount - fixed)
        return jnp.zeros((amount,), jnp.int32).at[sequence[jnp.where(places < fixed, places, passed)]].set(jnp.asarray(lengths, jnp.int32))

    lengths = jnp.where(number % 4 == 0, named(crowded, number // 4), named(common, number - number // 4 - 1))
    mixed = jax.random.permutation(jax.random.fold_in(own, 3), amount)
    giver, receiver = mixed[0:amount // 2 * 2:2], mixed[1:amount // 2 * 2:2]
    margin = jnp.minimum(lengths[giver] - 1, most - lengths[receiver]) // 2
    margin = jnp.where((giver == sequence[0]) | (receiver == sequence[0]) | (lengths[receiver] == 0), 0, jnp.maximum(margin, 0))
    passed = jax.random.randint(jax.random.fold_in(own, 4), (amount // 2,), 0, 1 << 20) % (margin + 1)
    lengths = lengths.at[giver].add(-passed).at[receiver].add(passed)
    items = jnp.searchsorted(jnp.cumsum(lengths), jnp.arange(rows * top), side="right").astype(jnp.int32)
    listing = items.reshape(top, rows).T
    listing = listing[jax.random.permutation(jax.random.fold_in(own, 1), rows)]
    turn = jax.random.randint(jax.random.fold_in(own, 2), (rows, 1), 0, top)
    return jnp.take_along_axis(listing, (jnp.arange(top)[None, :] + turn) % top, axis=1)


def shares(count, total, limit, lean, full):
    weights = [(1 << 20) // math.isqrt(grade ** lean) + 1 for grade in range(1, count + 1)]
    largest = limit if full else min(limit, max(-(-total // count), total * weights[0] // sum(weights)))
    least = 1 if total - largest >= count - 1 else 0
    counts, rest = [largest] + [least] * (count - 1), total - largest - least * (count - 1)
    while rest > 0:
        movable = [i for i in range(1, count) if counts[i] < largest] or [i for i in range(1, count) if counts[i] < limit]
        mass, left = sum([weights[i] for i in movable]), rest
        for i in movable:
            extra = min(limit - counts[i], max(1, left * weights[i] // mass), rest)
            counts[i] = counts[i] + extra
            rest = rest - extra
    return np.array(counts)


def bell_draw(stream_key, dims, width, most, cuts=(), kind=jnp.bfloat16):
    entries = jax.random.normal(stream_key, dims, jnp.float32) * width
    if len(cuts) > 0:
        entries = levels(stream_key, dims, cuts, -0.22, 0.18) * entries
    return jnp.clip(entries, min=-most, max=most).astype(kind)


def noise_with(stream_key, shape, deviation, bound, shards, heavy, kind=jnp.bfloat16):
    entries = deviation * jax.random.normal(stream_key, shape, jnp.float32)
    if shards:
        entries = entries * levels(stream_key, shape, shards, -0.22, 0.18)
    return jnp.clip(strengthened(entries, jax.random.fold_in(stream_key, 3), *heavy), -bound, bound).astype(kind)


def setup_inputs(seed: int = 0) -> dict:
    key_list = jax.random.split(jax.random.key(seed), 12)
    mixer_out = bell_draw(key_list[0], (TOKENS, D), 1.0, 6.0, ((0, 32),))
    out_grad = noise_with(key_list[1], (TOKENS, D), 0.25, 2.0, ((0, 32),), (0, 1, 32, 2.75))
    route_ids_keys = jax.random.split(jax.random.fold_in(key_list[2], 1), TOKENS // TOK_DEV)
    route_ids_turns = jax.random.permutation(jax.random.fold_in(key_list[2], 3), TOKENS // TOK_DEV)
    route_ids = jax.vmap(lambda own, number: shared_out(jax.random.fold_in(key_list[2], 2), own, number, TOK_DEV, EXPERTS, TOP, CAP, 1))(route_ids_keys, route_ids_turns).reshape((TOKENS, TOP))
    route_weights = jnp.clip(0.2 + 1 * jax.random.uniform(key_list[3], (TOKENS, TOP), jnp.float32) ** levels(key_list[3], (TOKENS, TOP), ((0, 32),), -0.2, 0.2), 0.2, 1.2)
    gate_branch = bell_draw(key_list[4], (TOKENS, D_RNN), 0.5, 4.0, ((0, 32), (1, 16)))
    states = bell_draw(key_list[5], (TOKENS, D_RNN), 1.0, 6.0, ((0, 32), (1, 16)), jnp.float32)
    decay = draw_decay(jax.random.fold_in(key_list[11], 71), 0)
    w_proj = bell_draw(key_list[7], (D, D_RNN), D_RNN ** -0.5, 0.125, ((1, 16),))
    w_gate = bell_draw(key_list[8], (EXPERTS, F, D), D ** -0.5, 0.125, ((0, 32), (1, 16)))
    w_up = bell_draw(key_list[9], (EXPERTS, F, D), D ** -0.5, 0.125, ((0, 32), (1, 16)))
    w_down = bell_draw(key_list[10], (EXPERTS, F, D), F ** -0.5, 0.125, ((0, 32), (1, 16)))
    return dict(mixer_out=mixer_out, out_grad=out_grad, route_ids=route_ids, route_weights=route_weights, gate_branch=gate_branch, states=states, decay=decay, w_proj=w_proj, w_gate=w_gate, w_up=w_up, w_down=w_down)


def linear_combine(earlier, later):
    return earlier[0] * later[0], later[0] * earlier[1] + later[1]


def reference(mixer_out, out_grad, route_ids, route_weights, gate_branch, states, decay, w_proj, w_gate, w_up, w_down):
    routes = TOKENS * TOP
    flat_ids = route_ids.reshape(-1).astype(jnp.int32)
    onehot = (flat_ids[:, None] == jnp.arange(EXPERTS, dtype=jnp.int32)[None, :]).astype(jnp.int32)
    counted = jnp.cumsum(onehot.reshape(N_SP, TOK_DEV * TOP, EXPERTS), axis=1).reshape(routes, EXPERTS)
    position = (jnp.sum(counted * onehot, axis=1) - 1).astype(jnp.int32)
    block_id = (jnp.arange(routes, dtype=jnp.int32) // (TOK_DEV * TOP)).astype(jnp.int32)
    slot_index = ((flat_ids * N_SP + block_id) * CAP + position).astype(jnp.int32)
    table = jnp.full((EXPERTS * N_SP * CAP,), routes, jnp.int32).at[slot_index].set(jnp.arange(routes, dtype=jnp.int32))
    table = table.reshape(EXPERTS, N_SP * CAP)
    scaled = (route_weights[:, :, None].astype(jnp.float32) * out_grad[:, None, :].astype(jnp.float32)).astype(jnp.bfloat16)
    scaled_pad = jnp.concatenate([scaled.reshape(routes, D), jnp.zeros((1, D), jnp.bfloat16)], axis=0)
    token_pad = jnp.concatenate([mixer_out, jnp.zeros((1, D), jnp.bfloat16)], axis=0)

    def one_expert(carry, expert):
        slot_routes = table[expert]
        inputs = token_pad[slot_routes // TOP].astype(jnp.float32)
        cotangents = scaled_pad[slot_routes].astype(jnp.float32)
        weight_gate = w_gate[expert].astype(jnp.float32)
        weight_up = w_up[expert].astype(jnp.float32)
        weight_down = w_down[expert].astype(jnp.float32)
        gate_pre = jnp.dot(inputs, weight_gate.T, preferred_element_type=jnp.float32)
        up_pre = jnp.dot(inputs, weight_up.T, preferred_element_type=jnp.float32)
        sigmoid_gate = jax.nn.sigmoid(gate_pre)
        silu_gate = gate_pre * sigmoid_gate
        hidden = (silu_gate * up_pre).astype(jnp.bfloat16).astype(jnp.float32)
        hidden_grad = jnp.dot(cotangents, weight_down.T, preferred_element_type=jnp.float32)
        up_grad = (hidden_grad * silu_gate).astype(jnp.bfloat16).astype(jnp.float32)
        gate_grad = (hidden_grad * up_pre * sigmoid_gate * (1.0 + gate_pre * (1.0 - sigmoid_gate))).astype(jnp.bfloat16).astype(jnp.float32)
        grad_gate = jnp.dot(gate_grad.T, inputs, preferred_element_type=jnp.float32).astype(jnp.bfloat16)
        grad_up = jnp.dot(up_grad.T, inputs, preferred_element_type=jnp.float32).astype(jnp.bfloat16)
        grad_down = jnp.dot(hidden.T, cotangents, preferred_element_type=jnp.float32).astype(jnp.bfloat16)
        slots = slot_routes.shape[0]
        block_part = jnp.einsum("sbf,bfd->sbd", gate_grad.reshape(slots, N_TP, F // N_TP), weight_gate.reshape(N_TP, F // N_TP, D))
        block_part = block_part + jnp.einsum("sbf,bfd->sbd", up_grad.reshape(slots, N_TP, F // N_TP), weight_up.reshape(N_TP, F // N_TP, D))
        partial_value = jnp.sum(block_part.astype(jnp.bfloat16).astype(jnp.float32), axis=1)
        carry = carry.at[slot_routes].add(partial_value)
        return carry, (grad_gate, grad_up, grad_down)

    start_carry = jnp.zeros((routes + 1, D), jnp.float32)
    route_grad, stacked = lax.scan(one_expert, start_carry, jnp.arange(EXPERTS, dtype=jnp.int32))
    grad_w_gate, grad_w_up, grad_w_down = stacked
    routed_grad = jnp.sum(route_grad[:routes].reshape(TOKENS, TOP, D), axis=1)
    mid_grad = (out_grad.astype(jnp.float32) + routed_grad).astype(jnp.bfloat16)
    gated = (gate_branch.astype(jnp.float32) * states).astype(jnp.bfloat16)
    grad_w_proj = jnp.dot(mid_grad.T, gated, preferred_element_type=jnp.float32)
    act_grad = jnp.dot(mid_grad, w_proj, preferred_element_type=jnp.float32)
    grad_branch = (act_grad * states).astype(jnp.bfloat16)
    state_grad = act_grad * gate_branch.astype(jnp.float32)
    next_decay = jnp.concatenate([decay[1:], jnp.ones((1, D_RNN), jnp.float32)], axis=0)
    decay_prod, flipped = lax.associative_scan(linear_combine, (next_decay[::-1], state_grad[::-1]), axis=0)
    grad_drive = flipped[::-1]
    previous = jnp.concatenate([jnp.zeros((1, D_RNN), jnp.float32), states[:-1]], axis=0)
    grad_decay = grad_drive * previous
    return grad_w_gate, grad_w_up, grad_w_down, grad_w_proj, grad_branch, grad_drive, grad_decay
```

```python
import functools

import jax
import jax.numpy as jnp
from jax import lax
from jax.experimental import pallas as pl
from jax.experimental.pallas import tpu as pltpu
from jax.sharding import Mesh, PartitionSpec as P

SP = ("z", "x")
Y = ("yh", "yl")
TP = ("yh", "yl", "c")
F32, BF16 = jnp.float32, jnp.bfloat16


def nt(a, b):
    return lax.dot_general(a, b, (((1,), (1,)), ((), ())), preferred_element_type=F32)


def tn(a, b):
    return lax.dot_general(a, b, (((0,), (0,)), ((), ())), preferred_element_type=F32)


def nn(a, b):
    return jnp.dot(a, b, preferred_element_type=F32)


def call(body, out_shape, place, *args, specs=None, scratch=(), vmem=48 << 20):
    whole = lambda a: pl.BlockSpec(a.shape, lambda i, s, n=len(a.shape): (0,) * n)
    outs = out_shape if isinstance(out_shape, (list, tuple)) else [out_shape]
    in_specs = [whole(a) for a in args]
    for k, spec in (specs or {}).items():
        in_specs[k] = spec
    result = pl.pallas_call(
        body,
        grid_spec=pltpu.PrefetchScalarGridSpec(
            num_scalar_prefetch=1,
            grid=(1,),
            in_specs=in_specs,
            out_specs=[whole(o) for o in outs],
            scratch_shapes=list(scratch),
        ),
        out_shape=list(outs),
        compiler_params=pltpu.CompilerParams(
            dimension_semantics=("arbitrary",), vmem_limit_bytes=vmem
        ),
    )(place, *args)
    return result if isinstance(out_shape, (list, tuple)) else result[0]


def dispatch_body(experts, half, place, ids, weights, x, og, send, pick):
    n = ids.shape[1]
    first = (place[1] * half).astype(F32)
    row = lax.broadcasted_iota(jnp.int32, (experts, n), 0)
    m0, m1 = ids[0:1, :] == row, ids[1:2, :] == row
    named = jnp.where(m0 | m1, 1.0, 0.0).astype(F32)
    wt = jnp.where(m0, weights[0:1, :], 0.0) + jnp.where(m1, weights[1:2, :], 0.0)
    before = lax.broadcasted_iota(jnp.int32, (n, n), 0) < lax.broadcasted_iota(
        jnp.int32, (n, n), 1
    )
    position = nn(named.astype(BF16), jnp.where(before, 1.0, 0.0).astype(BF16))
    position = jnp.where(named > 0.0, position, -1.0)
    slot = lax.broadcasted_iota(jnp.int32, (experts, half, n), 1).astype(F32) + first
    hot = jnp.where(position[:, None, :] == slot, 1.0, 0.0).astype(F32)
    scale = jnp.sum(hot * wt[:, None, :], axis=2, keepdims=True).reshape(experts * half, 1)
    hot = hot.reshape(experts * half, n).astype(BF16)
    pick[...] = hot
    cols = x.shape[1]
    xs = nn(hot, x[...]).reshape(experts, 1, half, cols)
    cs = (nn(hot, og[...]) * scale).reshape(experts, 1, half, cols)
    send[...] = (
        jnp.concatenate([xs, cs], axis=1).reshape(experts * 2 * half, cols).astype(BF16)
    )


def expert_body(half, place, own, par, wg, wu, wd, wa, wb, psend, pkeep, mix, g_s, u_s, d_s):
    c = place[0]
    cols = own.shape[1]
    mine = pl.ds(pl.multiple_of(c * cols, cols), cols)
    other = pl.ds(pl.multiple_of((1 - c) * cols, cols), cols)
    h, q = wg.shape[0], wa.shape[0] // 3
    for k, (w, s) in enumerate(((wg, g_s), (wu, u_s), (wd, d_s))):
        s[0:h, :] = w[...]
        s[h : h + q, :] = wa[k * q : (k + 1) * q, :]
        s[h + q : h + 2 * q, :] = wb[k * q : (k + 1) * q, :]
    units = h + 2 * q
    groups = own.shape[0] // (2 * half)

    def product(s, which):
        r = nt(own[...], s[:, mine]) + nt(par[...], s[:, other])
        return r.reshape(groups, 2, half, units)[:, which].reshape(groups * half, units)

    gate = product(g_s, 0)
    up = product(u_s, 0)
    grad = product(d_s, 1)
    sig = jax.nn.sigmoid(gate)
    silu = gate * sig
    hidden = silu * up
    up_grad = grad * silu
    gate_grad = grad * up * sig * (1.0 + gate * (1.0 - sig))
    gb, ub = gate_grad.astype(BF16), up_grad.astype(BF16)
    parts = psend.shape[0]
    width = cols // parts
    for ref, where in ((psend, other), (pkeep, mine)):
        p = nn(gb, g_s[:, where]) + nn(ub, u_s[:, where])
        for k in range(parts):
            ref[k] = p[:, k * width : (k + 1) * width].astype(ref.dtype)
    tile = lambda v: v.reshape(groups, 1, half, units)
    zero = jnp.zeros((groups, 1, half, units), F32)
    for k, pair in enumerate(
        ((tile(gate_grad), zero), (tile(up_grad), zero), (zero, tile(hidden)))
    ):
        v = jnp.concatenate(pair, axis=1).reshape(groups * 2 * half, units)
        mix[:, k * units : (k + 1) * units] = v.astype(BF16)


def weight_body(place, own, par, mix, gown, ga, gb):
    c = place[0]
    cols = own.shape[1]
    h, q = gown.shape[0] // 3, ga.shape[0] // 3
    units = h + 2 * q
    for src, start in ((own, c * cols), (par, (1 - c) * cols)):
        where = pl.ds(pl.multiple_of(start, cols), cols)
        for k in range(3):
            g = tn(mix[:, k * units : (k + 1) * units], src[...])
            gown[k * h : (k + 1) * h, where] = g[0:h]
            ga[k * q : (k + 1) * q, where] = g[h : h + q].astype(BF16)
            gb[k * q : (k + 1) * q, where] = g[h + q :].astype(BF16)


def combine_body(place, pick, back, og, keep, give):
    part = tn(pick[...], back[...])
    n = keep.shape[1]
    low = place[1] == 0
    keep[...] = jnp.where(low, part[:, :n], part[:, n:]) + og[...].astype(F32)
    give[...] = jnp.where(low, part[:, n:], part[:, :n])


def split3(v):
    a = v.astype(BF16).astype(F32)
    b = (v - a).astype(BF16).astype(F32)
    return a, b, (v - a - b).astype(BF16).astype(F32)


def project_body(place, mid, w, gate, states, decay, out, branch, local, prod):
    pieces = mid.shape[0]
    ys = pieces // 2
    full = jnp.concatenate([mid[(b % ys) * 2 + b // ys] for b in range(pieces)], axis=1)
    act = nn(full, w[...])
    st, gt, dec = states[...], gate[...].astype(F32), decay[...]
    grad = tn(full, (gt * st).astype(BF16)).astype(BF16)
    dests, rows = out.shape[0], full.shape[1] // out.shape[0]
    branch[...] = (act * st).astype(BF16)
    n = st.shape[0]
    t = lax.broadcasted_iota(jnp.int32, st.shape, 0)
    ahead = lambda v, k, fill: jnp.where(t < n - k, pltpu.roll(v, n - k, 0), fill)
    b, a = act * gt, ahead(dec, 1, 1.0)
    k = 1
    while k < n:
        b, a = b + a * ahead(b, k, 0.0), a * ahead(a, k, 1.0)
        k *= 2
    local[...] = b
    prod[...] = a
    values = split3(dec[0:1] * b[0:1]) + split3(dec[0:1] * a[0:1])
    values = values + (None, None) + split3(st[n - 1 : n])
    tail = out.shape[1] - rows
    line = lax.broadcasted_iota(jnp.int32, (tail, st.shape[1]), 0)
    extra = jnp.zeros((tail, st.shape[1]), F32)
    for k, v in enumerate(values):
        if v is not None:
            extra = jnp.where(line == k, jnp.broadcast_to(v, extra.shape), extra)
    extra = extra.astype(BF16)
    for d in range(dests):
        out[d, 0:rows, :] = grad[d * rows : (d + 1) * rows]
        out[d, rows : rows + tail, :] = extra


def finish_body(place, got, local, prod, states, proj, drive, ddecay):
    rows = proj.shape[0]
    members, n = got.shape[0], local.shape[0]
    s = place[2]
    total = got[0, 0:rows, :].astype(F32)
    for m in range(1, members):
        total = total + got[m, 0:rows, :].astype(F32)
    proj[...] = total
    carry = jnp.zeros((1, local.shape[1]), F32)
    before = jnp.zeros((1, local.shape[1]), F32)
    for m in range(members - 1, -1, -1):
        v = got[m, rows : rows + 16, :].astype(F32)
        later = m > s
        b = jnp.where(later, v[0:1] + v[1:2] + v[2:3], 0.0)
        a = jnp.where(later, v[3:4] + v[4:5] + v[5:6], 1.0)
        carry = b + a * carry
        before = jnp.where(m == s - 1, v[8:9] + v[9:10] + v[10:11], before)
    g = local[...] + prod[...] * carry
    drive[...] = g
    st = states[...]
    t = lax.broadcasted_iota(jnp.int32, st.shape, 0)
    previous = jnp.where(t == 0, jnp.broadcast_to(before, st.shape), pltpu.roll(st, 1, 0))
    ddecay[...] = g * previous


def local(
    sizes, mixer_out, out_grad, route_ids, route_weights, gate_branch, states, decay,
    w_proj, w_gate, w_up, w_down,
):
    n_sp, n_y, n_yh = sizes
    tokens, width = mixer_out.shape
    ch = states.shape[1]
    hidden = w_gate.shape[1]
    cap = 2 * route_ids.shape[1] * tokens // n_sp
    half = cap // 2
    shape = jax.ShapeDtypeStruct
    c, yl, yh = lax.axis_index("c"), lax.axis_index("yl"), lax.axis_index("yh")
    place = jnp.stack([c, yl, lax.axis_index(SP), c * n_y + yh * 2 + yl]).astype(jnp.int32)
    ring = lambda k: [(i, (i + k) % n_y) for i in range(n_y)]
    swap = [(0, 1), (1, 0)]
    wg, wu, wd = w_gate[0], w_up[0], w_down[0]
    q = hidden // 2

    w_lo = jnp.concatenate([wg[:q], wu[:q], wd[:q]], axis=0)
    w_hi = jnp.concatenate([wg[q:], wu[q:], wd[q:]], axis=0)
    wa = lax.ppermute(w_lo, Y, ring(1))
    wb = lax.ppermute(w_hi, Y, ring(-1))

    cols = width // 2
    by_core = pl.BlockSpec((tokens, cols), lambda i, s: (0, s[0]))
    send, pick = call(
        functools.partial(dispatch_body, n_sp, half),
        [shape((n_sp * cap, cols), BF16), shape((n_sp * half, tokens), BF16)],
        place, route_ids.T, route_weights.T, mixer_out, out_grad,
        specs={2: by_core, 3: by_core},
    )
    own = lax.all_to_all(send.reshape(n_sp, cap, cols), SP, 0, 0, tiled=True)
    own = own.reshape(n_sp * cap, cols)
    par = lax.ppermute(own, "c", swap)

    slots, units = n_sp * half, hidden + 2 * q
    wide = cols // n_yh
    w_s = pltpu.VMEM((units, width), BF16)
    psend, pkeep, mix = call(
        functools.partial(expert_body, half),
        [
            shape((n_yh, slots, wide), BF16),
            shape((n_yh, slots, wide), F32),
            shape((n_sp * cap, 3 * units), BF16),
        ],
        place, own, par, wg, wu, wd, wa, wb,
        scratch=[w_s, w_s, w_s],
    )
    precv = lax.ppermute(psend, "c", swap)
    gown, ga, gb = call(
        weight_body,
        [
            shape((3 * hidden, width), F32),
            shape((3 * q, width), BF16),
            shape((3 * q, width), BF16),
        ],
        place, own, par, mix,
    )
    back_lo = lax.ppermute(ga, Y, ring(-1))
    back_hi = lax.ppermute(gb, Y, ring(1))

    psum = (pkeep + precv.astype(F32)).astype(BF16)
    parts = lax.all_to_all(psum, "yh", 0, 0, tiled=True)
    ret = jnp.sum(parts.astype(F32), axis=0).astype(BF16)
    back = lax.all_to_all(ret.reshape(n_sp, half, wide), SP, 0, 0, tiled=True)

    keep, give = call(
        combine_body,
        [shape((tokens, ch), F32), shape((tokens, ch), F32)],
        place, pick, back.reshape(slots, wide), out_grad,
        specs={2: pl.BlockSpec((tokens, ch), lambda i, s: (0, s[3]))},
    )
    taken = lax.ppermute(give, "yl", swap)
    mid = lax.all_gather((keep + taken).astype(BF16), TP)

    rows = width // n_sp
    out, branch, loc, prod = call(
        project_body,
        [
            shape((n_sp, rows + 16, ch), BF16),
            shape((tokens, ch), BF16),
            shape((tokens, ch), F32),
            shape((tokens, ch), F32),
        ],
        place, mid, w_proj, gate_branch, states, decay,
    )
    got = lax.all_to_all(out, SP, 0, 0, tiled=True)
    proj, drive, ddecay = call(
        finish_body,
        [shape((rows, ch), F32), shape((tokens, ch), F32), shape((tokens, ch), F32)],
        place, got, loc, prod, states,
    )

    def total(k):
        mine = gown[k * hidden : (k + 1) * hidden]
        other = jnp.concatenate(
            [back_lo[k * q : (k + 1) * q], back_hi[k * q : (k + 1) * q]], axis=0
        )
        return (mine + other.astype(F32)).astype(BF16)[None]

    return (total(0), total(1), total(2), proj, branch, drive, ddecay)


def solution(mesh):
    devices = mesh.devices
    n_sp, n_tp = devices.shape
    n_yh = n_tp // 4
    x = 4
    fine = Mesh(
        devices.reshape(n_sp // x, x, n_yh, 2, 2), ("z", "x", "yh", "yl", "c")
    )
    rows, both, weight = P(SP, None), P(SP, TP), P(SP, TP, None)
    return jax.shard_map(
        functools.partial(local, (n_sp, n_tp // 2, n_yh)),
        mesh=fine,
        in_specs=(rows, rows, rows, rows, both, both, both, P(None, TP), weight, weight, weight),
        out_specs=(weight, weight, weight, both, both, both, both),
        check_vma=False,
    )
```

```python
import functools

import jax
import jax.numpy as jnp
from jax import lax
from jax.experimental import pallas as pl
from jax.experimental.pallas import tpu as pltpu
from jax.sharding import Mesh, PartitionSpec as P


SP = ("z", "x")
Y = ("yh", "yl")
TP = ("yh", "yl", "c")
F32, BF16 = jnp.float32, jnp.bfloat16


def nt(a, b):
    return lax.dot_general(a, b, (((1,), (1,)), ((), ())), preferred_element_type=F32)


def tn(a, b):
    return lax.dot_general(a, b, (((0,), (0,)), ((), ())), preferred_element_type=F32)


def nn(a, b):
    return jnp.dot(a, b, preferred_element_type=F32)


def copies(pairs, sems):
    started = [
        pltpu.make_async_copy(src, dst, sems.at[k]) for k, (src, dst) in enumerate(pairs)
    ]
    for copy in started:
        copy.start()
    return started


def move(pairs_of, out_shape, count, *args):
    def body(*refs):
        for copy in copies(pairs_of(*refs[:-1]), refs[-1]):
            copy.wait()

    anywhere = pl.BlockSpec(memory_space=pl.ANY)
    return pl.pallas_call(
        body,
        in_specs=[anywhere] * len(args),
        out_specs=[anywhere] * len(out_shape),
        out_shape=list(out_shape),
        scratch_shapes=[pltpu.SemaphoreType.DMA((count,))],
    )(*args)


def call(body, out_shape, place, *args, specs=None, outs_in=None, scratch=(), vmem=24 << 20):
    whole = lambda a: pl.BlockSpec(a.shape, lambda i, s, n=len(a.shape): (0,) * n)
    outs = out_shape if isinstance(out_shape, (list, tuple)) else [out_shape]
    in_specs = [whole(a) for a in args]
    out_specs = [whole(o) for o in outs]
    for k in specs or ():
        in_specs[k] = pl.BlockSpec(memory_space=pltpu.HBM)
    for k in outs_in or ():
        out_specs[k] = pl.BlockSpec(memory_space=pltpu.HBM)
    result = pl.pallas_call(
        body,
        grid_spec=pltpu.PrefetchScalarGridSpec(
            num_scalar_prefetch=1,
            grid=(1,),
            in_specs=in_specs,
            out_specs=out_specs,
            scratch_shapes=list(scratch),
        ),
        out_shape=list(outs),
        compiler_params=pltpu.CompilerParams(
            dimension_semantics=("arbitrary",), vmem_limit_bytes=vmem
        ),
    )(place, *args)
    return result if isinstance(out_shape, (list, tuple)) else result[0]


def dispatch_body(experts, cap, place, ids_h, wts_h, x_h, og_h, send_h, pick, ids, wts, x, og, send, sems):
    n, cols = x.shape
    half = cap // 2
    mine = pl.ds(pl.multiple_of(place[0] * cols, cols), cols)
    got = copies(
        ((ids_h, ids), (wts_h, wts), (x_h.at[:, mine], x), (og_h.at[:, mine], og)), sems
    )
    before = lax.broadcasted_iota(jnp.int32, (n, n), 0) < lax.broadcasted_iota(
        jnp.int32, (n, n), 1
    )
    before = jnp.where(before, 1.0, 0.0).astype(BF16)
    row = lax.broadcasted_iota(jnp.int32, (experts, n), 0)
    got[0].wait()
    got[1].wait()
    m0, m1 = ids[0:1, :] == row, ids[1:2, :] == row
    named = jnp.where(m0 | m1, 1.0, 0.0).astype(F32)
    wt = jnp.where(m0, wts[0:1, :], 0.0) + jnp.where(m1, wts[1:2, :], 0.0)
    position = nn(named.astype(BF16), before)
    position = jnp.where(named > 0.0, position, -1.0)
    slot = lax.broadcasted_iota(jnp.int32, (experts, half, n), 1).astype(F32)
    at = lambda first: jnp.where(position[:, None, :] == slot + first, 1.0, 0.0).astype(F32)
    pick[...] = (
        jnp.concatenate([at(0.0), at(float(half))], axis=1)
        .reshape(experts * cap, n)
        .astype(BF16)
    )
    hot = at((place[1] * half).astype(F32))
    scale = jnp.sum(hot * wt[:, None, :], axis=2, keepdims=True).reshape(experts * half, 1)
    hot = hot.reshape(experts * half, n).astype(BF16)
    got[2].wait()
    got[3].wait()
    steps, out = 2, []
    wide = cols // steps
    for k in range(steps):
        where = slice(k * wide, (k + 1) * wide)
        xs = nn(hot, x[:, where]).reshape(experts, 1, half, wide)
        cs = (nn(hot, og[:, where]) * scale).reshape(experts, 1, half, wide)
        send[:, where] = (
            jnp.concatenate([xs, cs], axis=1).reshape(experts * 2 * half, wide).astype(BF16)
        )
        copy = pltpu.make_async_copy(send.at[:, where], send_h.at[:, where], sems.at[4 + k])
        copy.start()
        out.append(copy)
    for copy in out:
        copy.wait()


def expert_body(half, place, own, par, g_s, u_s, d_s, psend, pkeep, mix):
    c = place[0]
    cols = own.shape[1]
    mine = pl.ds(pl.multiple_of(c * cols, cols), cols)
    other = pl.ds(pl.multiple_of((1 - c) * cols, cols), cols)
    units = g_s.shape[0]
    groups = own.shape[0] // (2 * half)

    def product(s, which):
        r = nt(own[...], s[:, mine]) + nt(par[...], s[:, other])
        return r.reshape(groups, 2, half, units)[:, which].reshape(groups * half, units)

    gate = product(g_s, 0)
    up = product(u_s, 0)
    grad = product(d_s, 1)
    sig = jax.nn.sigmoid(gate)
    silu = gate * sig
    hidden = silu * up
    up_grad = grad * silu
    gate_grad = grad * up * sig * (1.0 + gate * (1.0 - sig))
    gb, ub = gate_grad.astype(BF16), up_grad.astype(BF16)
    parts = psend.shape[0]
    width = cols // parts
    for ref, where in ((psend, other), (pkeep, mine)):
        p = nn(gb, g_s[:, where]) + nn(ub, u_s[:, where])
        for k in range(parts):
            ref[k] = p[:, k * width : (k + 1) * width].astype(ref.dtype)
    tile = lambda v: v.reshape(groups, 1, half, units)
    zero = jnp.zeros((groups, 1, half, units), F32)
    for k, pair in enumerate(
        ((tile(gate_grad), zero), (tile(up_grad), zero), (zero, tile(hidden)))
    ):
        v = jnp.concatenate(pair, axis=1).reshape(groups * 2 * half, units)
        mix[:, k * units : (k + 1) * units] = v.astype(BF16)


def weight_body(place, own, par, mix, gown, ga, gb):
    c = place[0]
    cols = own.shape[1]
    h, q = gown.shape[0] // 3, ga.shape[0] // 3
    units = h + 2 * q
    for src, start in ((own, c * cols), (par, (1 - c) * cols)):
        where = pl.ds(pl.multiple_of(start, cols), cols)
        for k in range(3):
            g = tn(mix[:, k * units : (k + 1) * units], src[...])
            gown[k * h : (k + 1) * h, where] = g[0:h]
            ga[k * q : (k + 1) * q, where] = g[h : h + q].astype(BF16)
            gb[k * q : (k + 1) * q, where] = g[h + q :].astype(BF16)


def fold_body(place, parts, out):
    members, _, ch = parts.shape
    dests, cap = out.shape[0], out.shape[1]
    both = []
    for low in range(2):
        total = parts[low].astype(F32)
        for m in range(low + 2, members, 2):
            total = total + parts[m].astype(F32)
        both.append(total.reshape(dests, cap // 2, ch))
    out[...] = jnp.concatenate(both, axis=1).astype(BF16)


def combine_body(place, pick, back, og_h, mid, og, sems):
    n = mid.shape[1]
    where = pl.ds(pl.multiple_of(place[3] * n, n), n)
    (copy,) = copies(((og_h.at[:, where], og),), sems)
    part = tn(pick[...], back[...])
    copy.wait()
    mid[...] = (og[...].astype(F32) + part).astype(BF16)


def split3(v):
    a = v.astype(BF16).astype(F32)
    b = (v - a).astype(BF16).astype(F32)
    return a, b, (v - a - b).astype(BF16).astype(F32)


def project_body(
    place, mid, w, gate_h, states_h, decay_h, out, branch, local, prod, gate, states, decay, sems
):
    got = copies(((gate_h, gate), (states_h, states), (decay_h, decay)), sems)
    pieces = mid.shape[0]
    ys = pieces // 2
    full = jnp.concatenate([mid[(b % ys) * 2 + b // ys] for b in range(pieces)], axis=1)
    act = nn(full, w[...])
    for copy in got:
        copy.wait()
    st, gt, dec = states[...], gate[...].astype(F32), decay[...]
    grad = tn(full, (gt * st).astype(BF16)).astype(BF16)
    dests, rows = out.shape[0], full.shape[1] // out.shape[0]
    branch[...] = (act * st).astype(BF16)
    n = st.shape[0]
    t = lax.broadcasted_iota(jnp.int32, st.shape, 0)
    ahead = lambda v, k, fill: jnp.where(t < n - k, pltpu.roll(v, n - k, 0), fill)
    b, a = act * gt, ahead(dec, 1, 1.0)
    k = 1
    while k < n:
        b, a = b + a * ahead(b, k, 0.0), a * ahead(a, k, 1.0)
        k *= 2
    local[...] = b
    prod[...] = a
    values = split3(dec[0:1] * b[0:1]) + split3(dec[0:1] * a[0:1])
    values = values + (None, None) + split3(st[n - 1 : n])
    tail = out.shape[1] - rows
    line = lax.broadcasted_iota(jnp.int32, (tail, st.shape[1]), 0)
    extra = jnp.zeros((tail, st.shape[1]), F32)
    for k, v in enumerate(values):
        if v is not None:
            extra = jnp.where(line == k, jnp.broadcast_to(v, extra.shape), extra)
    extra = extra.astype(BF16)
    for d in range(dests):
        out[d, 0:rows, :] = grad[d * rows : (d + 1) * rows]
        out[d, rows : rows + tail, :] = extra


def finish_body(place, got, local, prod, states, proj, drive, ddecay):
    rows = proj.shape[0]
    members = got.shape[0]
    s = place[2]
    total = got[0, 0:rows, :].astype(F32)
    for m in range(1, members):
        total = total + got[m, 0:rows, :].astype(F32)
    proj[...] = total
    carry = jnp.zeros((1, local.shape[1]), F32)
    before = jnp.zeros((1, local.shape[1]), F32)
    for m in range(members - 1, -1, -1):
        v = got[m, rows : rows + 16, :].astype(F32)
        later = m > s
        b = jnp.where(later, v[0:1] + v[1:2] + v[2:3], 0.0)
        a = jnp.where(later, v[3:4] + v[4:5] + v[5:6], 1.0)
        carry = b + a * carry
        before = jnp.where(m == s - 1, v[8:9] + v[9:10] + v[10:11], before)
    g = local[...] + prod[...] * carry
    drive[...] = g
    st = states[...]
    t = lax.broadcasted_iota(jnp.int32, st.shape, 0)
    previous = jnp.where(t == 0, jnp.broadcast_to(before, st.shape), pltpu.roll(st, 1, 0))
    ddecay[...] = g * previous


def local(
    sizes, mixer_out, out_grad, route_ids, route_weights, gate_branch, states, decay,
    w_proj, w_gate, w_up, w_down,
):
    n_sp, n_y = sizes
    tokens, width = mixer_out.shape
    ch = states.shape[1]
    hidden = w_gate.shape[1]
    cap = 2 * route_ids.shape[1] * tokens // n_sp
    half = cap // 2
    shape = jax.ShapeDtypeStruct
    c, yl, yh = lax.axis_index("c"), lax.axis_index("yl"), lax.axis_index("yh")
    place = jnp.stack([c, yl, lax.axis_index(SP), c * n_y + yh * 2 + yl]).astype(jnp.int32)
    ring = lambda k: [(i, (i + k) % n_y) for i in range(n_y)]
    swap = [(0, 1), (1, 0)]
    wg, wu, wd = w_gate[0], w_up[0], w_down[0]
    q = hidden // 2

    cols = width // 2
    small = pltpu.VMEM((2, tokens), jnp.int32), pltpu.VMEM((2, tokens), F32)
    block = pltpu.VMEM((tokens, cols), BF16)
    send, pick = call(
        functools.partial(dispatch_body, n_sp, cap),
        [shape((n_sp * cap, cols), BF16), shape((n_sp * cap, tokens), BF16)],
        place, route_ids.T, route_weights.T, mixer_out, out_grad,
        specs=(0, 1, 2, 3), outs_in=(0,),
        scratch=[
            *small, block, block,
            pltpu.VMEM((n_sp * cap, cols), BF16), pltpu.SemaphoreType.DMA((6,)),
        ],
    )
    own = lax.all_to_all(send.reshape(n_sp, cap, cols), SP, 0, 0, tiled=True)
    own = own.reshape(n_sp * cap, cols)

    def cut(*refs):
        w, (lo, hi) = refs[:3], refs[3:]
        return [
            (w[k].at[pl.ds(side * q, q)], to.at[pl.ds(k * q, q)])
            for side, to in enumerate((lo, hi))
            for k in range(3)
        ]

    w_lo, w_hi = move(cut, [shape((3 * q, width), BF16)] * 2, 6, wg, wu, wd)
    wa = lax.ppermute(w_lo, Y, ring(1))
    wb = lax.ppermute(w_hi, Y, ring(-1))
    par = lax.ppermute(own, "c", swap)

    units = hidden + 2 * q

    def joined(*refs):
        w, (lo, hi), to = refs[:3], refs[3:5], refs[5:]
        pairs = []
        for k in range(3):
            piece = pl.ds(k * q, q)
            pairs.append((w[k], to[k].at[pl.ds(0, hidden)]))
            pairs.append((lo.at[piece], to[k].at[pl.ds(hidden, q)]))
            pairs.append((hi.at[piece], to[k].at[pl.ds(hidden + q, q)]))
        return pairs

    weights = move(joined, [shape((units, width), BF16)] * 3, 9, wg, wu, wd, wa, wb)

    slots = n_sp * half
    wide = cols // n_y
    psend, pkeep, mix = call(
        functools.partial(expert_body, half),
        [
            shape((n_y, slots, wide), BF16),
            shape((n_y, slots, wide), F32),
            shape((n_sp * cap, 3 * units), BF16),
        ],
        place, own, par, *weights,
    )
    precv = lax.ppermute(psend, "c", swap)
    gown, ga, gb = call(
        weight_body,
        [shape((3 * hidden, width), F32), shape((3 * q, width), BF16), shape((3 * q, width), BF16)],
        place, own, par, mix,
    )
    back_lo = lax.ppermute(ga, Y, ring(-1))
    back_hi = lax.ppermute(gb, Y, ring(1))

    psum = (pkeep + precv.astype(F32)).astype(BF16)
    parts = lax.all_to_all(psum, Y, 0, 0, tiled=True)
    ret = call(fold_body, shape((n_sp, cap, wide), BF16), place, parts)
    back = lax.all_to_all(ret, SP, 0, 0, tiled=True)
    mid = call(
        combine_body,
        shape((tokens, ch), BF16),
        place, pick, back.reshape(n_sp * cap, wide), out_grad,
        specs=(2,),
        scratch=[pltpu.VMEM((tokens, ch), BF16), pltpu.SemaphoreType.DMA((1,))],
    )
    mid = lax.all_gather(mid, TP)

    rows = width // n_sp
    out, branch, loc, prod = call(
        project_body,
        [
            shape((n_sp, rows + 16, ch), BF16),
            shape((tokens, ch), BF16),
            shape((tokens, ch), F32),
            shape((tokens, ch), F32),
        ],
        place, mid, w_proj, gate_branch, states, decay,
        specs=(2, 3, 4),
        scratch=[
            pltpu.VMEM((tokens, ch), BF16), pltpu.VMEM((tokens, ch), F32),
            pltpu.VMEM((tokens, ch), F32), pltpu.SemaphoreType.DMA((3,)),
        ],
    )
    got = lax.all_to_all(out, SP, 0, 0, tiled=True)
    proj, drive, ddecay = call(
        finish_body,
        [shape((rows, ch), F32), shape((tokens, ch), F32), shape((tokens, ch), F32)],
        place, got, loc, prod, states,
    )

    def total(k):
        mine = gown[k * hidden : (k + 1) * hidden]
        other = jnp.concatenate(
            [back_lo[k * q : (k + 1) * q], back_hi[k * q : (k + 1) * q]], axis=0
        )
        return (mine + other.astype(F32)).astype(BF16)[None]

    return (total(0), total(1), total(2), proj, branch, drive, ddecay)


def solution(mesh):
    devices = mesh.devices
    n_sp, n_tp = devices.shape
    n_yh = n_tp // 4
    x = 4
    fine = Mesh(
        devices.reshape(n_sp // x, x, n_yh, 2, 2), ("z", "x", "yh", "yl", "c")
    )
    rows, both, weight = P(SP, None), P(SP, TP), P(SP, TP, None)
    return jax.shard_map(
        functools.partial(local, (n_sp, n_tp // 2)),
        mesh=fine,
        in_specs=(rows, rows, rows, rows, both, both, both, P(None, TP), weight, weight, weight),
        out_specs=(weight, weight, weight, both, both, both, both),
        check_vma=False,
    )
```

```python
import functools

import jax
import jax.numpy as jnp
from jax import lax
from jax.experimental import pallas as pl
from jax.experimental.pallas import tpu as pltpu
from jax.sharding import Mesh, PartitionSpec as P


SP = ("z", "x")
Y = ("yh", "yl")
TP = ("yh", "yl", "c")
F32, BF16 = jnp.float32, jnp.bfloat16


VMEM = 12 << 20


def nt(a, b):
    return lax.dot_general(a, b, (((1,), (1,)), ((), ())), preferred_element_type=F32)


def tn(a, b):
    return lax.dot_general(a, b, (((0,), (0,)), ((), ())), preferred_element_type=F32)


def nn(a, b):
    return jnp.dot(a, b, preferred_element_type=F32)


def copies(pairs, sems):
    started = [
        pltpu.make_async_copy(src, dst, sems.at[k]) for k, (src, dst) in enumerate(pairs)
    ]
    for copy in started:
        copy.start()
    return started


def move(pairs_of, out_shape, count, *args):
    def body(*refs):
        for copy in copies(pairs_of(*refs[:-1]), refs[-1]):
            copy.wait()

    anywhere = pl.BlockSpec(memory_space=pl.ANY)
    return pl.pallas_call(
        body,
        in_specs=[anywhere] * len(args),
        out_specs=[pl.BlockSpec(memory_space=pltpu.VMEM)] * len(out_shape),
        out_shape=list(out_shape),
        scratch_shapes=[pltpu.SemaphoreType.DMA((count,))],
        compiler_params=pltpu.CompilerParams(vmem_limit_bytes=8 << 20),
    )(*args)


def call(body, out_shape, place, *args, specs=None, outs_in=None, scratch=(), vmem=VMEM):
    whole = lambda a: pl.BlockSpec(a.shape, lambda i, s, n=len(a.shape): (0,) * n)
    outs = out_shape if isinstance(out_shape, (list, tuple)) else [out_shape]
    in_specs = [whole(a) for a in args]
    out_specs = [whole(o) for o in outs]
    args, outs = list(args), list(outs)
    for k in specs or ():
        in_specs[k] = pl.BlockSpec(memory_space=pltpu.HBM)
        args[k] = pltpu.with_memory_space_constraint(args[k], pltpu.HBM)
    for k in outs_in or ():
        out_specs[k] = pl.BlockSpec(memory_space=pltpu.HBM)
        outs[k] = pltpu.HBM(outs[k].shape, outs[k].dtype)
    result = pl.pallas_call(
        body,
        grid_spec=pltpu.PrefetchScalarGridSpec(
            num_scalar_prefetch=1,
            grid=(1,),
            in_specs=in_specs,
            out_specs=out_specs,
            scratch_shapes=list(scratch),
        ),
        out_shape=list(outs),
        compiler_params=pltpu.CompilerParams(
            dimension_semantics=("arbitrary",), vmem_limit_bytes=vmem
        ),
    )(place, *args)
    return result if isinstance(out_shape, (list, tuple)) else result[0]


def dispatch_body(experts, cap, place, ids_h, wts_h, x_h, og_h, send_h, pick, ids, wts, x, og, send, sems):
    n, cols = x.shape
    half = cap // 2
    mine = pl.ds(pl.multiple_of(place[0] * cols, cols), cols)
    got = copies(
        ((ids_h, ids), (wts_h, wts), (x_h.at[:, mine], x), (og_h.at[:, mine], og)), sems
    )
    before = lax.broadcasted_iota(jnp.int32, (n, n), 0) < lax.broadcasted_iota(
        jnp.int32, (n, n), 1
    )
    before = jnp.where(before, 1.0, 0.0).astype(BF16)
    row = lax.broadcasted_iota(jnp.int32, (experts, n), 0)
    got[0].wait()
    got[1].wait()
    m0, m1 = ids[0:1, :] == row, ids[1:2, :] == row
    named = jnp.where(m0 | m1, 1.0, 0.0).astype(F32)
    wt = jnp.where(m0, wts[0:1, :], 0.0) + jnp.where(m1, wts[1:2, :], 0.0)
    position = nn(named.astype(BF16), before)
    position = jnp.where(named > 0.0, position, -1.0)
    slot = lax.broadcasted_iota(jnp.int32, (experts, half, n), 1).astype(F32)
    at = lambda first: jnp.where(position[:, None, :] == slot + first, 1.0, 0.0).astype(F32)
    pick[...] = (
        jnp.concatenate([at(0.0), at(float(half))], axis=1)
        .reshape(experts * cap, n)
        .astype(BF16)
    )
    hot = at((place[1] * half).astype(F32))
    scale = jnp.sum(hot * wt[:, None, :], axis=2, keepdims=True).reshape(experts * half, 1)
    hot = hot.reshape(experts * half, n).astype(BF16)
    got[2].wait()
    got[3].wait()
    steps, out = 2, []
    wide = cols // steps
    for k in range(steps):
        where = slice(k * wide, (k + 1) * wide)
        xs = nn(hot, x[:, where]).reshape(experts, 1, half, wide)
        cs = (nn(hot, og[:, where]) * scale).reshape(experts, 1, half, wide)
        send[:, where] = (
            jnp.concatenate([xs, cs], axis=1).reshape(experts * 2 * half, wide).astype(BF16)
        )
        copy = pltpu.make_async_copy(send.at[:, where], send_h.at[:, where], sems.at[4 + k])
        copy.start()
        out.append(copy)
    for copy in out:
        copy.wait()


def prep_body(place, gate, states, gated):
    gated[...] = (gate[...].astype(F32) * states[...]).astype(BF16)


def expert_body(
    half, place, own, par, wg_h, wu_h, wd_h, wa_h, wb_h, psend, pkeep, mix_h, w_s, mix, sems
):
    c = place[0]
    cols = own.shape[1]
    mine = pl.ds(pl.multiple_of(c * cols, cols), cols)
    other = pl.ds(pl.multiple_of((1 - c) * cols, cols), cols)
    units = w_s.shape[1]
    h = wg_h.shape[0]
    q = (units - h) // 2
    groups = own.shape[0] // (2 * half)
    pairs = []
    for k, w in enumerate((wg_h, wu_h, wd_h)):
        piece = pl.ds(k * q, q)
        pairs.append((w, w_s.at[k, pl.ds(0, h)]))
        pairs.append((wa_h.at[piece], w_s.at[k, pl.ds(h, q)]))
        pairs.append((wb_h.at[piece], w_s.at[k, pl.ds(h + q, q)]))
    loads = copies(pairs, sems)

    def product(k, which):
        for copy in loads[3 * k : 3 * k + 3]:
            copy.wait()
        r = nt(own[...], w_s[k, :, mine]) + nt(par[...], w_s[k, :, other])
        return r.reshape(groups, 2, half, units)[:, which].reshape(groups * half, units)

    gate = product(0, 0)
    up = product(1, 0)
    grad = product(2, 1)
    sig = jax.nn.sigmoid(gate)
    silu = gate * sig
    hidden = silu * up
    up_grad = grad * silu
    gate_grad = grad * up * sig * (1.0 + gate * (1.0 - sig))
    gb, ub = gate_grad.astype(BF16), up_grad.astype(BF16)
    tile = lambda v: v.reshape(groups, 1, half, units)
    zero = jnp.zeros((groups, 1, half, units), F32)
    for k, pair in enumerate(
        ((tile(gate_grad), zero), (tile(up_grad), zero), (zero, tile(hidden)))
    ):
        v = jnp.concatenate(pair, axis=1).reshape(groups * 2 * half, units)
        mix[:, k * units : (k + 1) * units] = v.astype(BF16)
    (kept,) = copies(((mix, mix_h),), sems.at[pl.ds(9, 1)])
    parts = psend.shape[0]
    width = cols // parts
    for ref, where in ((psend, other), (pkeep, mine)):
        p = nn(gb, w_s[0, :, where]) + nn(ub, w_s[1, :, where])
        for k in range(parts):
            ref[k] = p[:, k * width : (k + 1) * width].astype(ref.dtype)
    kept.wait()


def weight_body(place, own, par, mix, gown_h, ga, gb, gown, sems):
    c = place[0]
    cols = own.shape[1]
    h, q = gown.shape[1] // 3, ga.shape[0] // 3
    units = h + 2 * q
    stored = []
    for n, (src, start) in enumerate(((own, c * cols), (par, (1 - c) * cols))):
        where = pl.ds(pl.multiple_of(start, cols), cols)
        for k in range(3):
            g = tn(mix[:, k * units : (k + 1) * units], src[...])
            rows = pl.ds(k * h, h)
            gown[n, rows, :] = g[0:h]
            copy = pltpu.make_async_copy(
                gown.at[n, rows], gown_h.at[rows, where], sems.at[3 * n + k]
            )
            copy.start()
            stored.append(copy)
            ga[k * q : (k + 1) * q, where] = g[h : h + q].astype(BF16)
            gb[k * q : (k + 1) * q, where] = g[h + q :].astype(BF16)
    for copy in stored:
        copy.wait()


def fold_body(place, parts, out):
    members, _, ch = parts.shape
    dests, cap = out.shape[0], out.shape[1]
    both = []
    for low in range(2):
        total = parts[low].astype(F32)
        for m in range(low + 2, members, 2):
            total = total + parts[m].astype(F32)
        both.append(total.reshape(dests, cap // 2, ch))
    out[...] = jnp.concatenate(both, axis=1).astype(BF16)


def combine_body(place, pick, back, og_h, mid, og, sems):
    n = mid.shape[1]
    where = pl.ds(pl.multiple_of(place[3] * n, n), n)
    (copy,) = copies(((og_h.at[:, where], og),), sems)
    part = tn(pick[...], back[...])
    copy.wait()
    mid[...] = (og[...].astype(F32) + part).astype(BF16)


def split3(v):
    a = v.astype(BF16).astype(F32)
    b = (v - a).astype(BF16).astype(F32)
    return a, b, (v - a - b).astype(BF16).astype(F32)


def project_body(
    place, mid, gated, w_h, gate_h, states_h, decay_h, out_h, branch, local, prod,
    w, gate, states, decay, out, sems,
):
    got = copies(((w_h, w), (gate_h, gate), (states_h, states), (decay_h, decay)), sems)
    pieces = mid.shape[0]
    ys = pieces // 2
    full = jnp.concatenate([mid[(b % ys) * 2 + b // ys] for b in range(pieces)], axis=1)
    grad = tn(full, gated[...]).astype(BF16)
    dests, rows = out.shape[0], full.shape[1] // out.shape[0]
    for d in range(dests):
        out[d, 0:rows, :] = grad[d * rows : (d + 1) * rows]
    for copy in got:
        copy.wait()
    act = nn(full, w[...])
    st, gt, dec = states[...], gate[...].astype(F32), decay[...]
    branch[...] = (act * st).astype(BF16)
    n = st.shape[0]
    t = lax.broadcasted_iota(jnp.int32, st.shape, 0)
    ahead = lambda v, k, fill: jnp.where(t < n - k, pltpu.roll(v, n - k, 0), fill)
    b, a = act * gt, ahead(dec, 1, 1.0)
    k = 1
    while k < n:
        b, a = b + a * ahead(b, k, 0.0), a * ahead(a, k, 1.0)
        k *= 2
    local[...] = b
    prod[...] = a
    values = split3(dec[0:1] * b[0:1]) + split3(dec[0:1] * a[0:1])
    values = values + (None, None) + split3(st[n - 1 : n])
    tail = out.shape[1] - rows
    line = lax.broadcasted_iota(jnp.int32, (tail, st.shape[1]), 0)
    extra = jnp.zeros((tail, st.shape[1]), F32)
    for k, v in enumerate(values):
        if v is not None:
            extra = jnp.where(line == k, jnp.broadcast_to(v, extra.shape), extra)
    extra = extra.astype(BF16)
    for d in range(dests):
        out[d, rows : rows + tail, :] = extra
    (sent,) = copies(((out, out_h),), sems.at[pl.ds(4, 1)])
    sent.wait()


def finish_body(place, got, local, prod, states, proj, drive, ddecay):
    rows = proj.shape[0]
    members = got.shape[0]
    s = place[2]
    total = got[0, 0:rows, :].astype(F32)
    for m in range(1, members):
        total = total + got[m, 0:rows, :].astype(F32)
    proj[...] = total
    carry = jnp.zeros((1, local.shape[1]), F32)
    before = jnp.zeros((1, local.shape[1]), F32)
    for m in range(members - 1, -1, -1):
        v = got[m, rows : rows + 16, :].astype(F32)
        later = m > s
        b = jnp.where(later, v[0:1] + v[1:2] + v[2:3], 0.0)
        a = jnp.where(later, v[3:4] + v[4:5] + v[5:6], 1.0)
        carry = b + a * carry
        before = jnp.where(m == s - 1, v[8:9] + v[9:10] + v[10:11], before)
    g = local[...] + prod[...] * carry
    drive[...] = g
    st = states[...]
    t = lax.broadcasted_iota(jnp.int32, st.shape, 0)
    previous = jnp.where(t == 0, jnp.broadcast_to(before, st.shape), pltpu.roll(st, 1, 0))
    ddecay[...] = g * previous


def local(
    sizes, mixer_out, out_grad, route_ids, route_weights, gate_branch, states, decay,
    w_proj, w_gate, w_up, w_down,
):
    n_sp, n_y = sizes
    tokens, width = mixer_out.shape
    ch = states.shape[1]
    hidden = w_gate.shape[1]
    cap = 2 * route_ids.shape[1] * tokens // n_sp
    half = cap // 2
    shape = jax.ShapeDtypeStruct
    c, yl, yh = lax.axis_index("c"), lax.axis_index("yl"), lax.axis_index("yh")
    place = jnp.stack([c, yl, lax.axis_index(SP), c * n_y + yh * 2 + yl]).astype(jnp.int32)
    ring = lambda k: [(i, (i + k) % n_y) for i in range(n_y)]
    swap = [(0, 1), (1, 0)]
    wg, wu, wd = w_gate[0], w_up[0], w_down[0]
    q = hidden // 2

    cols = width // 2
    small = pltpu.VMEM((2, tokens), jnp.int32), pltpu.VMEM((2, tokens), F32)
    block = pltpu.VMEM((tokens, cols), BF16)
    send, pick = call(
        functools.partial(dispatch_body, n_sp, cap),
        [shape((n_sp * cap, cols), BF16), shape((n_sp * cap, tokens), BF16)],
        place, route_ids.T, route_weights.T, mixer_out, out_grad,
        specs=(0, 1, 2, 3), outs_in=(0,),
        scratch=[
            *small, block, block,
            pltpu.VMEM((n_sp * cap, cols), BF16), pltpu.SemaphoreType.DMA((6,)),
        ],
    )
    own = lax.all_to_all(send.reshape(n_sp, cap, cols), SP, 0, 0, tiled=True)
    own = own.reshape(n_sp * cap, cols)

    def cut(*refs):
        w, (lo, hi) = refs[:3], refs[3:]
        return [
            (w[k].at[pl.ds(side * q, q)], to.at[pl.ds(k * q, q)])
            for side, to in enumerate((lo, hi))
            for k in range(3)
        ]

    w_lo, w_hi = move(cut, [shape((3 * q, width), BF16)] * 2, 6, wg, wu, wd)
    wa = lax.ppermute(w_lo, Y, ring(1))
    wb = lax.ppermute(w_hi, Y, ring(-1))
    par = lax.ppermute(own, "c", swap)

    units = hidden + 2 * q
    gated = call(prep_body, shape((tokens, ch), BF16), place, gate_branch, states)

    slots = n_sp * half
    wide = cols // n_y
    psend, pkeep, mix = call(
        functools.partial(expert_body, half),
        [
            shape((n_y, slots, wide), BF16),
            shape((n_y, slots, wide), F32),
            shape((n_sp * cap, 3 * units), BF16),
        ],
        place, own, par, wg, wu, wd, wa, wb,
        specs=(2, 3, 4, 5, 6), outs_in=(2,),
        scratch=[
            pltpu.VMEM((3, units, width), BF16),
            pltpu.VMEM((n_sp * cap, 3 * units), BF16),
            pltpu.SemaphoreType.DMA((10,)),
        ],
    )
    precv = lax.ppermute(psend, "c", swap)
    gown, ga, gb = call(
        weight_body,
        [shape((3 * hidden, width), F32), shape((3 * q, width), BF16), shape((3 * q, width), BF16)],
        place, own, par, mix,
        outs_in=(0,),
        scratch=[
            pltpu.VMEM((2, 3 * hidden, cols), F32), pltpu.SemaphoreType.DMA((6,)),
        ],
    )
    back_lo = lax.ppermute(ga, Y, ring(-1))
    back_hi = lax.ppermute(gb, Y, ring(1))

    psum = (pkeep + precv.astype(F32)).astype(BF16)
    parts = lax.all_to_all(psum, Y, 0, 0, tiled=True)
    ret = call(fold_body, shape((n_sp, cap, wide), BF16), place, parts)
    back = lax.all_to_all(ret, SP, 0, 0, tiled=True)
    mid = call(
        combine_body,
        shape((tokens, ch), BF16),
        place, pick, back.reshape(n_sp * cap, wide), out_grad,
        specs=(2,),
        scratch=[pltpu.VMEM((tokens, ch), BF16), pltpu.SemaphoreType.DMA((1,))],
    )
    mid = lax.all_gather(mid, TP)

    rows = width // n_sp
    out, branch, loc, prod = call(
        project_body,
        [
            shape((n_sp, rows + 16, ch), BF16),
            shape((tokens, ch), BF16),
            shape((tokens, ch), F32),
            shape((tokens, ch), F32),
        ],
        place, mid, gated, w_proj, gate_branch, states, decay,
        specs=(2, 3, 4, 5), outs_in=(0,),
        scratch=[
            pltpu.VMEM((width, ch), BF16), pltpu.VMEM((tokens, ch), BF16),
            pltpu.VMEM((tokens, ch), F32), pltpu.VMEM((tokens, ch), F32),
            pltpu.VMEM((n_sp, rows + 16, ch), BF16), pltpu.SemaphoreType.DMA((5,)),
        ],
    )
    got = lax.all_to_all(out, SP, 0, 0, tiled=True)
    proj, drive, ddecay = call(
        finish_body,
        [shape((rows, ch), F32), shape((tokens, ch), F32), shape((tokens, ch), F32)],
        place, got, loc, prod, states,
    )

    def total(k):
        mine = gown[k * hidden : (k + 1) * hidden]
        other = jnp.concatenate(
            [back_lo[k * q : (k + 1) * q], back_hi[k * q : (k + 1) * q]], axis=0
        )
        return (mine + other.astype(F32)).astype(BF16)[None]

    return (total(0), total(1), total(2), proj, branch, drive, ddecay)


def solution(mesh):
    devices = mesh.devices
    n_sp, n_tp = devices.shape
    n_yh = n_tp // 4
    x = 4
    fine = Mesh(
        devices.reshape(n_sp // x, x, n_yh, 2, 2), ("z", "x", "yh", "yl", "c")
    )
    rows, both, weight = P(SP, None), P(SP, TP), P(SP, TP, None)
    return jax.shard_map(
        functools.partial(local, (n_sp, n_tp // 2)),
        mesh=fine,
        in_specs=(rows, rows, rows, rows, both, both, both, P(None, TP), weight, weight, weight),
        out_specs=(weight, weight, weight, both, both, both, both),
        check_vma=False,
    )
```

```python
import functools

import jax
import jax.numpy as jnp
from jax import lax
from jax.experimental import pallas as pl
from jax.experimental.pallas import tpu as pltpu
from jax.sharding import Mesh, PartitionSpec as P


SP = ("z", "x")
Y = ("yh", "yl")
TP = ("yh", "yl", "c")
F32, BF16 = jnp.float32, jnp.bfloat16


VMEM = 12 << 20


def nt(a, b):
    return lax.dot_general(a, b, (((1,), (1,)), ((), ())), preferred_element_type=F32)


def tn(a, b):
    return lax.dot_general(a, b, (((0,), (0,)), ((), ())), preferred_element_type=F32)


def nn(a, b):
    return jnp.dot(a, b, preferred_element_type=F32)


def copies(pairs, sems):
    started = [
        pltpu.make_async_copy(src, dst, sems.at[k]) for k, (src, dst) in enumerate(pairs)
    ]
    for copy in started:
        copy.start()
    return started


def move(pairs_of, out_shape, count, *args):
    def body(*refs):
        for copy in copies(pairs_of(*refs[:-1]), refs[-1]):
            copy.wait()

    anywhere = pl.BlockSpec(memory_space=pl.ANY)
    return pl.pallas_call(
        body,
        in_specs=[anywhere] * len(args),
        out_specs=[pl.BlockSpec(memory_space=pltpu.VMEM)] * len(out_shape),
        out_shape=list(out_shape),
        scratch_shapes=[pltpu.SemaphoreType.DMA((count,))],
        compiler_params=pltpu.CompilerParams(vmem_limit_bytes=8 << 20),
    )(*args)


def call(body, out_shape, place, *args, specs=None, outs_in=None, scratch=(), vmem=VMEM):
    whole = lambda a: pl.BlockSpec(a.shape, lambda i, s, n=len(a.shape): (0,) * n)
    outs = out_shape if isinstance(out_shape, (list, tuple)) else [out_shape]
    in_specs = [whole(a) for a in args]
    out_specs = [whole(o) for o in outs]
    args, outs = list(args), list(outs)
    for k in specs or ():
        in_specs[k] = pl.BlockSpec(memory_space=pltpu.HBM)
        args[k] = pltpu.with_memory_space_constraint(args[k], pltpu.HBM)
    for k in outs_in or ():
        out_specs[k] = pl.BlockSpec(memory_space=pltpu.HBM)
        outs[k] = pltpu.HBM(outs[k].shape, outs[k].dtype)
    result = pl.pallas_call(
        body,
        grid_spec=pltpu.PrefetchScalarGridSpec(
            num_scalar_prefetch=1,
            grid=(1,),
            in_specs=in_specs,
            out_specs=out_specs,
            scratch_shapes=list(scratch),
        ),
        out_shape=list(outs),
        compiler_params=pltpu.CompilerParams(
            dimension_semantics=("arbitrary",), vmem_limit_bytes=vmem
        ),
    )(place, *args)
    return result if isinstance(out_shape, (list, tuple)) else result[0]


def dispatch_body(experts, cap, place, ids_h, wts_h, x_h, og_h, send_h, pick_h, ids, wts, x, og, send, pick, sems):
    n, cols = x.shape
    half = cap // 2
    mine = pl.ds(pl.multiple_of(place[0] * cols, cols), cols)
    got = copies(
        ((ids_h, ids), (wts_h, wts), (x_h.at[:, mine], x), (og_h.at[:, mine], og)), sems
    )
    before = lax.broadcasted_iota(jnp.int32, (n, n), 0) < lax.broadcasted_iota(
        jnp.int32, (n, n), 1
    )
    before = jnp.where(before, 1.0, 0.0).astype(BF16)
    row = lax.broadcasted_iota(jnp.int32, (experts, n), 0)
    got[0].wait()
    got[1].wait()
    m0, m1 = ids[0:1, :] == row, ids[1:2, :] == row
    named = jnp.where(m0 | m1, 1.0, 0.0).astype(F32)
    wt = jnp.where(m0, wts[0:1, :], 0.0) + jnp.where(m1, wts[1:2, :], 0.0)
    position = nn(named.astype(BF16), before)
    position = jnp.where(named > 0.0, position, -1.0)
    slot = lax.broadcasted_iota(jnp.int32, (experts, half, n), 1).astype(F32)
    at = lambda first: jnp.where(position[:, None, :] == slot + first, 1.0, 0.0).astype(F32)
    pick[...] = (
        jnp.concatenate([at(0.0), at(float(half))], axis=1)
        .reshape(experts * cap, n)
        .astype(BF16)
    )
    hot = at((place[1] * half).astype(F32))
    scale = jnp.sum(hot * wt[:, None, :], axis=2, keepdims=True).reshape(experts * half, 1)
    hot = hot.reshape(experts * half, n).astype(BF16)
    got[2].wait()
    got[3].wait()
    out, wide = [], cols // 2
    for k in range(2):
        where = slice(k * wide, (k + 1) * wide)
        send[:, where] = nn(hot, x[:, where]).astype(BF16)
        there = slice(cols + k * wide, cols + (k + 1) * wide)
        send[:, there] = (nn(hot, og[:, where]) * scale).astype(BF16)
        for cut in (where, there):
            copy = pltpu.make_async_copy(
                send.at[:, cut], send_h.at[:, cut], sems.at[4 + len(out)]
            )
            copy.start()
            out.append(copy)
    kept = pltpu.make_async_copy(pick, pick_h, sems.at[8])
    kept.start()
    for copy in (*out, kept):
        copy.wait()


def split3(v):
    a = v.astype(BF16).astype(F32)
    b = (v - a).astype(BF16).astype(F32)
    return a, b, (v - a - b).astype(BF16).astype(F32)


def prep_body(place, gate, states, decay, gated, weight, tail):
    st, gt, dec = states[...], gate[...].astype(F32), decay[...]
    gated[...] = (gt * st).astype(BF16)
    n = st.shape[0]
    t = lax.broadcasted_iota(jnp.int32, st.shape, 0)
    prefix, k = dec, 1
    while k < n:
        prefix = prefix * jnp.where(t >= k, pltpu.roll(prefix, k, 0), 1.0)
        k *= 2
    weight[...] = prefix * gt
    values = split3(prefix[n - 1 : n])
    line = lax.broadcasted_iota(jnp.int32, tail.shape, 0)
    rows = jnp.zeros(tail.shape, F32)
    for k, v in enumerate(values):
        rows = jnp.where(line == 3 + k, jnp.broadcast_to(v, tail.shape), rows)
    for k, v in enumerate(split3(st[n - 1 : n])):
        rows = jnp.where(line == 8 + k, jnp.broadcast_to(v, tail.shape), rows)
    tail[...] = rows


def weight_copies(wg, wu, wd, wa, wb, w_s, where, count):
    h = wg.shape[0]
    q = (w_s.shape[1] - h) // 2
    pairs = []
    for k, w in enumerate((wg, wu, wd)[:count]):
        piece = pl.ds(k * q, q)
        pairs.append((w.at[:, where], w_s.at[k, pl.ds(0, h)]))
        pairs.append((wa.at[piece, where], w_s.at[k, pl.ds(h, q)]))
        pairs.append((wb.at[piece, where], w_s.at[k, pl.ds(h + q, q)]))
    return pairs


def columns(core, cols):
    return pl.ds(pl.multiple_of(core * cols, cols), cols)


def product(k, rows, w_s, loads):
    for copy in loads[3 * k : 3 * k + 3]:
        copy.wait()
    cols = w_s.shape[2]
    side = rows[:, 0:cols] if k < 2 else rows[:, cols:]
    return nt(side, w_s[k])


def first_body(place, own, wg, wu, wd, wa, wb, part, w_s, sems):
    where = columns(place[0], w_s.shape[2])
    loads = copies(weight_copies(wg, wu, wd, wa, wb, w_s, where, 3), sems)
    for k in range(3):
        part[k] = product(k, own, w_s, loads)


def partials(out, gb, ub, w_s):
    width = out.shape[2]
    p = nn(gb, w_s[0]) + nn(ub, w_s[1])
    for k in range(out.shape[0]):
        out[k] = p[:, k * width : (k + 1) * width].astype(out.dtype)


def expert_body(place, par, part, wg, wu, wd, wa, wb, psend, mix_h, w_s, mix, sems):
    where = columns(1 - place[0], w_s.shape[2])
    loads = copies(weight_copies(wg, wu, wd, wa, wb, w_s, where, 3), sems)
    units = w_s.shape[1]
    gate = part[0] + product(0, par, w_s, loads)
    up = part[1] + product(1, par, w_s, loads)
    grad = part[2] + product(2, par, w_s, loads)
    sig = jax.nn.sigmoid(gate)
    silu = gate * sig
    ub = (grad * silu).astype(BF16)
    gb = (grad * up * sig * (1.0 + gate * (1.0 - sig))).astype(BF16)
    mix[:, 0:units] = gb
    mix[:, units : 2 * units] = ub
    mix[:, 2 * units :] = (silu * up).astype(BF16)
    (kept,) = copies(((mix, mix_h),), sems.at[pl.ds(9, 1)])
    partials(psend, gb, ub, w_s)
    kept.wait()


def keep_body(place, mix_h, wg, wu, wd, wa, wb, pkeep, w_s, mix, sems):
    where = columns(place[0], w_s.shape[2])
    units = w_s.shape[1]
    pairs = weight_copies(wg, wu, wd, wa, wb, w_s, where, 2)
    for copy in copies([(mix_h.at[:, pl.ds(0, 2 * units)], mix)] + pairs, sems):
        copy.wait()
    partials(pkeep, mix[:, 0:units], mix[:, units:], w_s)


def weight_body(place, own, par, mix, gown_h, ga, gb, gown, sems):
    c = place[0]
    h, q = gown.shape[1] // 3, ga.shape[0] // 3
    units, cols = h + 2 * q, gown.shape[2]
    stored = []
    for n, (src, core) in enumerate(((own, c), (par, 1 - c))):
        where = columns(core, cols)
        for k in range(3):
            side = src[:, 0:cols] if k < 2 else src[:, cols:]
            g = tn(mix[:, k * units : (k + 1) * units], side)
            rows = pl.ds(k * h, h)
            gown[n, rows, :] = g[0:h]
            copy = pltpu.make_async_copy(
                gown.at[n, rows], gown_h.at[rows, where], sems.at[3 * n + k]
            )
            copy.start()
            stored.append(copy)
            ga[k * q : (k + 1) * q, where] = g[h : h + q].astype(BF16)
            gb[k * q : (k + 1) * q, where] = g[h + q :].astype(BF16)
    for copy in stored:
        copy.wait()


def fold_body(place, parts, out):
    members, _, ch = parts.shape
    dests, cap = out.shape[0], out.shape[1]
    both = []
    for low in range(2):
        total = parts[low].astype(F32)
        for m in range(low + 2, members, 2):
            total = total + parts[m].astype(F32)
        both.append(total.reshape(dests, cap // 2, ch))
    out[...] = jnp.concatenate(both, axis=1).astype(BF16)


def combine_body(place, pick_h, back, og_h, mid, pick, og, sems):
    n = mid.shape[1]
    got = copies(((pick_h, pick), (og_h.at[:, columns(place[3], n)], og)), sems)
    got[0].wait()
    part = tn(pick[...], back[...])
    got[1].wait()
    mid[...] = (og[...].astype(F32) + part).astype(BF16)


def project_body(
    place, mid, gated_h, w_h, weight_h, tail_h, out_h, act_o, gated, w, weight, tail, out, sems
):
    got = copies(
        ((gated_h, gated), (w_h, w), (weight_h, weight), (tail_h, tail)), sems
    )
    pieces = mid.shape[0]
    ys = pieces // 2
    full = jnp.concatenate([mid[(b % ys) * 2 + b // ys] for b in range(pieces)], axis=1)
    dests, rows = out.shape[0], full.shape[1] // out.shape[0]
    got[0].wait()
    grad = tn(full, gated[...]).astype(BF16)
    for d in range(dests):
        out[d, 0:rows, :] = grad[d * rows : (d + 1) * rows]
    head, rest = pl.ds(0, rows), pl.ds(rows, out.shape[1] - rows)
    sent = copies(((out.at[:, head], out_h.at[:, head]),), sems.at[pl.ds(4, 1)])
    got[1].wait()
    act = nn(full, w[...])
    act_o[...] = act
    got[2].wait()
    got[3].wait()
    total = jnp.sum(weight[...] * act, axis=0, keepdims=True)
    extra = tail[...]
    line = lax.broadcasted_iota(jnp.int32, extra.shape, 0)
    for k, v in enumerate(split3(total)):
        extra = jnp.where(line == k, jnp.broadcast_to(v, extra.shape), extra)
    extra = extra.astype(BF16)
    for d in range(dests):
        out[d, rows:, :] = extra
    sent += copies(((out.at[:, rest], out_h.at[:, rest]),), sems.at[pl.ds(5, 1)])
    for copy in sent:
        copy.wait()


def scan_body(place, act, gate, states, decay, branch, local, prod):
    st, gt, dec = states[...], gate[...].astype(F32), decay[...]
    branch[...] = (act[...] * st).astype(BF16)
    n = st.shape[0]
    t = lax.broadcasted_iota(jnp.int32, st.shape, 0)
    ahead = lambda v, k, fill: jnp.where(t < n - k, pltpu.roll(v, n - k, 0), fill)
    b, a = act[...] * gt, ahead(dec, 1, 1.0)
    k = 1
    while k < n:
        b, a = b + a * ahead(b, k, 0.0), a * ahead(a, k, 1.0)
        k *= 2
    local[...] = b
    prod[...] = a


def finish_body(place, got, local, prod, states, proj, drive, ddecay):
    rows = proj.shape[0]
    members = got.shape[0]
    s = place[2]
    total = got[0, 0:rows, :].astype(F32)
    for m in range(1, members):
        total = total + got[m, 0:rows, :].astype(F32)
    proj[...] = total
    carry = jnp.zeros((1, local.shape[1]), F32)
    before = jnp.zeros((1, local.shape[1]), F32)
    for m in range(members - 1, -1, -1):
        v = got[m, rows : rows + 16, :].astype(F32)
        later = m > s
        b = jnp.where(later, v[0:1] + v[1:2] + v[2:3], 0.0)
        a = jnp.where(later, v[3:4] + v[4:5] + v[5:6], 1.0)
        carry = b + a * carry
        before = jnp.where(m == s - 1, v[8:9] + v[9:10] + v[10:11], before)
    g = local[...] + prod[...] * carry
    drive[...] = g
    st = states[...]
    t = lax.broadcasted_iota(jnp.int32, st.shape, 0)
    previous = jnp.where(t == 0, jnp.broadcast_to(before, st.shape), pltpu.roll(st, 1, 0))
    ddecay[...] = g * previous


def local(
    sizes, mixer_out, out_grad, route_ids, route_weights, gate_branch, states, decay,
    w_proj, w_gate, w_up, w_down,
):
    n_sp, n_y = sizes
    tokens, width = mixer_out.shape
    ch = states.shape[1]
    hidden = w_gate.shape[1]
    cap = 2 * route_ids.shape[1] * tokens // n_sp
    half = cap // 2
    shape = jax.ShapeDtypeStruct
    c, yl, yh = lax.axis_index("c"), lax.axis_index("yl"), lax.axis_index("yh")
    place = jnp.stack([c, yl, lax.axis_index(SP), c * n_y + yh * 2 + yl]).astype(jnp.int32)
    ring = lambda k: [(i, (i + k) % n_y) for i in range(n_y)]
    swap = [(0, 1), (1, 0)]
    wg, wu, wd = w_gate[0], w_up[0], w_down[0]
    q = hidden // 2

    cols = width // 2
    small = pltpu.VMEM((2, tokens), jnp.int32), pltpu.VMEM((2, tokens), F32)
    block = pltpu.VMEM((tokens, cols), BF16)
    send, pick = call(
        functools.partial(dispatch_body, n_sp, cap),
        [shape((n_sp * half, width), BF16), shape((n_sp * cap, tokens), BF16)],
        place, route_ids.T, route_weights.T, mixer_out, out_grad,
        specs=(0, 1, 2, 3), outs_in=(0, 1),
        scratch=[
            *small, block, block,
            pltpu.VMEM((n_sp * half, width), BF16),
            pltpu.VMEM((n_sp * cap, tokens), BF16),
            pltpu.SemaphoreType.DMA((9,)),
        ],
    )
    own = lax.all_to_all(send.reshape(n_sp, half, width), SP, 0, 0, tiled=True)
    own = own.reshape(n_sp * half, width)

    def cut(*refs):
        w, (lo, hi) = refs[:3], refs[3:]
        return [
            (w[k].at[pl.ds(side * q, q)], to.at[pl.ds(k * q, q)])
            for side, to in enumerate((lo, hi))
            for k in range(3)
        ]

    w_lo, w_hi = move(cut, [shape((3 * q, width), BF16)] * 2, 6, wg, wu, wd)
    wa = lax.ppermute(w_lo, Y, ring(1))
    wb = lax.ppermute(w_hi, Y, ring(-1))
    par = lax.ppermute(own, "c", swap)

    units = hidden + 2 * q
    tail = 16
    gated, weight, tails = call(
        prep_body,
        [shape((tokens, ch), BF16), shape((tokens, ch), F32), shape((tail, ch), F32)],
        place, gate_branch, states, decay,
    )

    slots = n_sp * half
    wide = cols // n_y
    held = pltpu.VMEM((3, units, cols), BF16)
    weights = (wg, wu, wd, wa, wb)
    part = call(
        first_body, shape((3, slots, units), F32), place, own, *weights,
        specs=(1, 2, 3, 4, 5), scratch=[held, pltpu.SemaphoreType.DMA((9,))],
    )
    psend, mix = call(
        expert_body,
        [shape((n_y, slots, wide), BF16), shape((slots, 3 * units), BF16)],
        place, par, part, *weights,
        specs=(2, 3, 4, 5, 6), outs_in=(1,),
        scratch=[
            held, pltpu.VMEM((slots, 3 * units), BF16), pltpu.SemaphoreType.DMA((10,)),
        ],
    )
    pkeep = call(
        keep_body, shape((n_y, slots, wide), F32), place, mix, *weights,
        specs=(0, 1, 2, 3, 4, 5),
        scratch=[
            pltpu.VMEM((2, units, cols), BF16), pltpu.VMEM((slots, 2 * units), BF16),
            pltpu.SemaphoreType.DMA((7,)),
        ],
    )
    precv = lax.ppermute(psend, "c", swap)
    gown, ga, gb = call(
        weight_body,
        [shape((3 * hidden, width), F32), shape((3 * q, width), BF16), shape((3 * q, width), BF16)],
        place, own, par, mix,
        outs_in=(0,),
        scratch=[
            pltpu.VMEM((2, 3 * hidden, cols), F32), pltpu.SemaphoreType.DMA((6,)),
        ],
    )
    back_lo = lax.ppermute(ga, Y, ring(-1))
    back_hi = lax.ppermute(gb, Y, ring(1))

    psum = (pkeep + precv.astype(F32)).astype(BF16)
    parts = lax.all_to_all(psum, Y, 0, 0, tiled=True)
    ret = call(fold_body, shape((n_sp, cap, wide), BF16), place, parts)
    back = lax.all_to_all(ret, SP, 0, 0, tiled=True)
    mid = call(
        combine_body,
        shape((tokens, ch), BF16),
        place, pick, back.reshape(n_sp * cap, wide), out_grad,
        specs=(0, 2),
        scratch=[
            pltpu.VMEM((n_sp * cap, tokens), BF16), pltpu.VMEM((tokens, ch), BF16),
            pltpu.SemaphoreType.DMA((2,)),
        ],
    )
    mid = lax.all_gather(mid, TP)

    rows = width // n_sp
    row = lambda t: shape((tokens, ch), t)
    out, act = call(
        project_body,
        [shape((n_sp, rows + tail, ch), BF16), row(F32)],
        place, mid, gated, w_proj, weight, tails,
        specs=(1, 2, 3, 4), outs_in=(0,),
        scratch=[
            pltpu.VMEM((tokens, ch), BF16), pltpu.VMEM((width, ch), BF16),
            pltpu.VMEM((tokens, ch), F32), pltpu.VMEM((tail, ch), F32),
            pltpu.VMEM((n_sp, rows + tail, ch), BF16), pltpu.SemaphoreType.DMA((6,)),
        ],
    )
    branch, loc, prod = call(
        scan_body, [row(BF16), row(F32), row(F32)],
        place, act, gate_branch, states, decay,
    )
    got = lax.all_to_all(out, SP, 0, 0, tiled=True)
    proj, drive, ddecay = call(
        finish_body, [shape((rows, ch), F32), row(F32), row(F32)],
        place, got, loc, prod, states,
    )

    def total(k):
        mine = gown[k * hidden : (k + 1) * hidden]
        other = jnp.concatenate(
            [back_lo[k * q : (k + 1) * q], back_hi[k * q : (k + 1) * q]], axis=0
        )
        return (mine + other.astype(F32)).astype(BF16)[None]

    return (total(0), total(1), total(2), proj, branch, drive, ddecay)


def solution(mesh):
    devices = mesh.devices
    n_sp, n_tp = devices.shape
    n_yh = n_tp // 4
    x = 4
    fine = Mesh(
        devices.reshape(n_sp // x, x, n_yh, 2, 2), ("z", "x", "yh", "yl", "c")
    )
    rows, both, weight = P(SP, None), P(SP, TP), P(SP, TP, None)
    return jax.shard_map(
        functools.partial(local, (n_sp, n_tp // 2)),
        mesh=fine,
        in_specs=(rows, rows, rows, rows, both, both, both, P(None, TP), weight, weight, weight),
        out_specs=(weight, weight, weight, both, both, both, both),
        check_vma=False,
    )
```

```python
import functools

import jax
import jax.numpy as jnp
from jax import lax
from jax.experimental import pallas as pl
from jax.experimental.pallas import tpu as pltpu
from jax.sharding import Mesh, PartitionSpec as P


SP = ("z", "x")
Y = ("yh", "yl")
TP = ("yh", "yl", "c")
F32, BF16 = jnp.float32, jnp.bfloat16


VMEM = 12 << 20


def nt(a, b):
    return lax.dot_general(a, b, (((1,), (1,)), ((), ())), preferred_element_type=F32)


def tn(a, b):
    return lax.dot_general(a, b, (((0,), (0,)), ((), ())), preferred_element_type=F32)


def nn(a, b):
    return jnp.dot(a, b, preferred_element_type=F32)


def copies(pairs, sems):
    started = [
        pltpu.make_async_copy(src, dst, sems.at[k]) for k, (src, dst) in enumerate(pairs)
    ]
    for copy in started:
        copy.start()
    return started


def move(pairs_of, out_shape, count, *args):
    def body(*refs):
        for copy in copies(pairs_of(*refs[:-1]), refs[-1]):
            copy.wait()

    anywhere = pl.BlockSpec(memory_space=pl.ANY)
    return pl.pallas_call(
        body,
        in_specs=[anywhere] * len(args),
        out_specs=[pl.BlockSpec(memory_space=pltpu.VMEM)] * len(out_shape),
        out_shape=list(out_shape),
        scratch_shapes=[pltpu.SemaphoreType.DMA((count,))],
        compiler_params=pltpu.CompilerParams(vmem_limit_bytes=8 << 20),
    )(*args)


def call(body, out_shape, place, *args, specs=None, free=(), outs_in=None, scratch=(), vmem=VMEM):
    whole = lambda a: pl.BlockSpec(a.shape, lambda i, s, n=len(a.shape): (0,) * n)
    outs = out_shape if isinstance(out_shape, (list, tuple)) else [out_shape]
    in_specs = [whole(a) for a in args]
    out_specs = [whole(o) for o in outs]
    args, outs = list(args), list(outs)
    for k in specs or ():
        in_specs[k] = pl.BlockSpec(memory_space=pltpu.HBM)
        args[k] = pltpu.with_memory_space_constraint(args[k], pltpu.HBM)
    for k in free:
        in_specs[k] = pl.BlockSpec(memory_space=pl.ANY)
    for k in outs_in or ():
        out_specs[k] = pl.BlockSpec(memory_space=pltpu.HBM)
        outs[k] = pltpu.HBM(outs[k].shape, outs[k].dtype)
    result = pl.pallas_call(
        body,
        grid_spec=pltpu.PrefetchScalarGridSpec(
            num_scalar_prefetch=1,
            grid=(1,),
            in_specs=in_specs,
            out_specs=out_specs,
            scratch_shapes=list(scratch),
        ),
        out_shape=list(outs),
        compiler_params=pltpu.CompilerParams(
            dimension_semantics=("arbitrary",), vmem_limit_bytes=vmem
        ),
    )(place, *args)
    return result if isinstance(out_shape, (list, tuple)) else result[0]


def dispatch_body(experts, cap, place, ids_h, wts_h, x_h, og_h, send_h, pick_h, ids, wts, x, og, send, pick, sems):
    n, cols = x.shape
    half = cap // 2
    mine = pl.ds(pl.multiple_of(place[0] * cols, cols), cols)
    got = copies(
        ((ids_h, ids), (wts_h, wts), (x_h.at[:, mine], x), (og_h.at[:, mine], og)), sems
    )
    before = lax.broadcasted_iota(jnp.int32, (n, n), 0) < lax.broadcasted_iota(
        jnp.int32, (n, n), 1
    )
    before = jnp.where(before, 1.0, 0.0).astype(BF16)
    row = lax.broadcasted_iota(jnp.int32, (experts, n), 0)
    got[0].wait()
    got[1].wait()
    m0, m1 = ids[0:1, :] == row, ids[1:2, :] == row
    named = jnp.where(m0 | m1, 1.0, 0.0).astype(F32)
    wt = jnp.where(m0, wts[0:1, :], 0.0) + jnp.where(m1, wts[1:2, :], 0.0)
    position = nn(named.astype(BF16), before)
    position = jnp.where(named > 0.0, position, -1.0)
    slot = lax.broadcasted_iota(jnp.int32, (experts, half, n), 1).astype(F32)
    at = lambda first: jnp.where(position[:, None, :] == slot + first, 1.0, 0.0).astype(F32)
    hot = at((place[1] * half).astype(F32))
    scale = jnp.sum(hot * wt[:, None, :], axis=2, keepdims=True).reshape(experts * half, 1)
    hot = hot.reshape(experts * half, n).astype(BF16)
    got[2].wait()
    got[3].wait()
    out, wide = [], cols // 2
    for k in range(2):
        where = slice(k * wide, (k + 1) * wide)
        send[:, where] = nn(hot, x[:, where]).astype(BF16)
        there = slice(cols + k * wide, cols + (k + 1) * wide)
        send[:, there] = (nn(hot, og[:, where]) * scale).astype(BF16)
        for cut in (where, there):
            copy = pltpu.make_async_copy(
                send.at[:, cut], send_h.at[:, cut], sems.at[4 + len(out)]
            )
            copy.start()
            out.append(copy)
    pick[...] = (
        jnp.concatenate([at(0.0), at(float(half))], axis=1)
        .reshape(experts * cap, n)
        .astype(BF16)
    )
    kept = pltpu.make_async_copy(pick, pick_h, sems.at[8])
    kept.start()
    for copy in (*out, kept):
        copy.wait()


def split3(v):
    a = v.astype(BF16).astype(F32)
    b = (v - a).astype(BF16).astype(F32)
    return a, b, (v - a - b).astype(BF16).astype(F32)


def prep_body(place, gate, states, gated):
    gated[...] = (gate[...].astype(F32) * states[...]).astype(BF16)


def past_body(place, gate, states, decay, weight, tail):
    st, gt, dec = states[...], gate[...].astype(F32), decay[...]
    n = st.shape[0]
    t = lax.broadcasted_iota(jnp.int32, st.shape, 0)
    prefix, k = dec, 1
    while k < n:
        prefix = prefix * jnp.where(t >= k, pltpu.roll(prefix, k, 0), 1.0)
        k *= 2
    weight[...] = prefix * gt
    line = lax.broadcasted_iota(jnp.int32, tail.shape, 0)
    rows = jnp.zeros(tail.shape, F32)
    for first, value in ((3, prefix[n - 1 : n]), (8, st[n - 1 : n])):
        for k, v in enumerate(split3(value)):
            rows = jnp.where(line == first + k, jnp.broadcast_to(v, tail.shape), rows)
    tail[...] = rows


def weight_copies(wg, wu, wd, wa, wb, w_s, where, count):
    h = wg.shape[0]
    q = (w_s.shape[1] - h) // 2
    pairs = []
    for k, w in enumerate((wg, wu, wd)[:count]):
        piece = pl.ds(k * q, q)
        pairs.append((w.at[:, where], w_s.at[k, pl.ds(0, h)]))
        pairs.append((wa.at[piece, where], w_s.at[k, pl.ds(h, q)]))
        pairs.append((wb.at[piece, where], w_s.at[k, pl.ds(h + q, q)]))
    return pairs


def columns(core, cols):
    return pl.ds(pl.multiple_of(core * cols, cols), cols)


def product(k, rows, w_s, loads):
    for copy in loads[3 * k : 3 * k + 3]:
        copy.wait()
    cols = w_s.shape[2]
    side = rows[:, 0:cols] if k < 2 else rows[:, cols:]
    return nt(side, w_s[k])


def first_body(place, own, wg, wu, wd, wa, wb, part, w_s, sems):
    where = columns(place[0], w_s.shape[2])
    loads = copies(weight_copies(wg, wu, wd, wa, wb, w_s, where, 3), sems)
    for k in range(3):
        part[k] = product(k, own, w_s, loads)


def partials(out, gb, ub, w_s):
    width = out.shape[2]
    p = nn(gb, w_s[0]) + nn(ub, w_s[1])
    for k in range(out.shape[0]):
        out[k] = p[:, k * width : (k + 1) * width].astype(out.dtype)


def activations(gate, up, grad):
    sig = jax.nn.sigmoid(gate)
    silu = gate * sig
    gate_grad = grad * up * sig * (1.0 + gate * (1.0 - sig))
    return gate_grad.astype(BF16), (grad * silu).astype(BF16), (silu * up).astype(BF16)


def expert_body(place, par, part, wg, wu, wd, wa, wb, psend, mix_h, w_s, mix, sems):
    where = columns(1 - place[0], w_s.shape[2])
    loads = copies(weight_copies(wg, wu, wd, wa, wb, w_s, where, 3), sems)
    units = w_s.shape[1]
    gate = part[0] + product(0, par, w_s, loads)
    up = part[1] + product(1, par, w_s, loads)
    grad = part[2] + product(2, par, w_s, loads)
    gb, ub, hb = activations(gate, up, grad)
    mix[:, 0:units] = gb
    mix[:, units : 2 * units] = ub
    mix[:, 2 * units :] = hb
    (kept,) = copies(((mix, mix_h),), sems.at[pl.ds(9, 1)])
    partials(psend, gb, ub, w_s)
    kept.wait()


def keep_body(place, mix_h, wg, wu, wd, wa, wb, pkeep, w_s, mix, sems):
    where = columns(place[0], w_s.shape[2])
    units = w_s.shape[1]
    pairs = weight_copies(wg, wu, wd, wa, wb, w_s, where, 2)
    for copy in copies([(mix_h.at[:, pl.ds(0, 2 * units)], mix)] + pairs, sems):
        copy.wait()
    partials(pkeep, mix[:, 0:units], mix[:, units:], w_s)


def weight_body(place, own, par, mix, gown_h, gown, sems):
    c = place[0]
    h, cols = gown.shape[1] // 3, gown.shape[2]
    units = mix.shape[1] // 3
    stored = []
    for n, (src, core) in enumerate(((own, c), (par, 1 - c))):
        for k in range(3):
            side = src[:, 0:cols] if k < 2 else src[:, cols:]
            rows = pl.ds(k * h, h)
            gown[n, rows, :] = tn(mix[:, k * units : k * units + h], side)
            copy = pltpu.make_async_copy(
                gown.at[n, rows],
                gown_h.at[rows, columns(core, cols)],
                sems.at[3 * n + k],
            )
            copy.start()
            stored.append(copy)
    for copy in stored:
        copy.wait()


def rest_body(
    place, xa_h, xb_h, pa_h, pb_h, wg, wu, wd, gown_h, dg_h, du_h, dd_h,
    own, par, w_s, held, sum_s, sems,
):
    c = place[0]
    rows, h = xa_h.shape[0], wg.shape[0]
    cols = own.shape[1] // 2
    top, low = pl.ds(0, rows), pl.ds(rows, rows)
    loads = copies(
        (
            (xa_h, own.at[top]), (xb_h, own.at[low]), (pa_h, par.at[top]),
            (pb_h, par.at[low]), (wg, w_s.at[0]), (wu, w_s.at[1]), (wd, w_s.at[2]),
            (gown_h, held),
        ),
        sems,
    )
    for copy in loads[:7]:
        copy.wait()
    mine, other = columns(c, cols), columns(1 - c, cols)

    def pre(k):
        cut = slice(0, cols) if k < 2 else slice(cols, 2 * cols)
        return nt(own[:, cut], w_s[k, :, mine]) + nt(par[:, cut], w_s[k, :, other])

    three = activations(pre(0), pre(1), pre(2))
    loads[7].wait()
    stored = []
    for k, to in enumerate((dg_h, du_h, dd_h)):
        cut = slice(0, cols) if k < 2 else slice(cols, 2 * cols)
        for src, where in ((own, mine), (par, other)):
            total = held[k * h : (k + 1) * h, where] + tn(three[k], src[:, cut])
            sum_s[k, :, where] = total.astype(BF16)
        copy = pltpu.make_async_copy(sum_s.at[k], to.at[0], sems.at[8 + k])
        copy.start()
        stored.append(copy)
    for copy in stored:
        copy.wait()


def fold_body(place, parts, out):
    members, _, ch = parts.shape
    dests, cap = out.shape[0], out.shape[1]
    both = []
    for low in range(2):
        total = parts[low].astype(F32)
        for m in range(low + 2, members, 2):
            total = total + parts[m].astype(F32)
        both.append(total.reshape(dests, cap // 2, ch))
    out[...] = jnp.concatenate(both, axis=1).astype(BF16)


def combine_body(place, pick_h, back, og_h, mid, pick, og, sems):
    n = mid.shape[1]
    got = copies(((pick_h, pick), (og_h.at[:, columns(place[3], n)], og)), sems)
    got[0].wait()
    part = tn(pick[...], back[...])
    got[1].wait()
    mid[...] = (og[...].astype(F32) + part).astype(BF16)


def project_body(
    place, mid, gated_h, w_h, weight_h, tail_h, out_h, act_o, gated, w, weight, tail, out, sems
):
    got = copies(
        ((gated_h, gated), (w_h, w), (weight_h, weight), (tail_h, tail)), sems
    )
    pieces = mid.shape[0]
    ys = pieces // 2
    full = jnp.concatenate([mid[(b % ys) * 2 + b // ys] for b in range(pieces)], axis=1)
    dests, rows = out.shape[0], full.shape[1] // out.shape[0]
    got[0].wait()
    grad = tn(full, gated[...]).astype(BF16)
    for d in range(dests):
        out[d, 0:rows, :] = grad[d * rows : (d + 1) * rows]
    head, rest = pl.ds(0, rows), pl.ds(rows, out.shape[1] - rows)
    sent = copies(((out.at[:, head], out_h.at[:, head]),), sems.at[pl.ds(4, 1)])
    got[1].wait()
    act = nn(full, w[...])
    act_o[...] = act
    got[2].wait()
    got[3].wait()
    total = jnp.sum(weight[...] * act, axis=0, keepdims=True)
    extra = tail[...]
    line = lax.broadcasted_iota(jnp.int32, extra.shape, 0)
    for k, v in enumerate(split3(total)):
        extra = jnp.where(line == k, jnp.broadcast_to(v, extra.shape), extra)
    extra = extra.astype(BF16)
    for d in range(dests):
        out[d, rows:, :] = extra
    sent += copies(((out.at[:, rest], out_h.at[:, rest]),), sems.at[pl.ds(5, 1)])
    for copy in sent:
        copy.wait()


def scan_body(place, act, gate, states, decay, branch, local, prod):
    st, gt, dec = states[...], gate[...].astype(F32), decay[...]
    branch[...] = (act[...] * st).astype(BF16)
    n = st.shape[0]
    t = lax.broadcasted_iota(jnp.int32, st.shape, 0)
    ahead = lambda v, k, fill: jnp.where(t < n - k, pltpu.roll(v, n - k, 0), fill)
    b, a = act[...] * gt, ahead(dec, 1, 1.0)
    k = 1
    while k < n:
        b, a = b + a * ahead(b, k, 0.0), a * ahead(a, k, 1.0)
        k *= 2
    local[...] = b
    prod[...] = a


def finish_body(place, got, local, prod, states, proj, drive, ddecay):
    rows = proj.shape[0]
    members = got.shape[0]
    s = place[2]
    total = got[0, 0:rows, :].astype(F32)
    for m in range(1, members):
        total = total + got[m, 0:rows, :].astype(F32)
    proj[...] = total
    carry = jnp.zeros((1, local.shape[1]), F32)
    before = jnp.zeros((1, local.shape[1]), F32)
    for m in range(members - 1, -1, -1):
        v = got[m, rows : rows + 16, :].astype(F32)
        later = m > s
        b = jnp.where(later, v[0:1] + v[1:2] + v[2:3], 0.0)
        a = jnp.where(later, v[3:4] + v[4:5] + v[5:6], 1.0)
        carry = b + a * carry
        before = jnp.where(m == s - 1, v[8:9] + v[9:10] + v[10:11], before)
    g = local[...] + prod[...] * carry
    drive[...] = g
    st = states[...]
    t = lax.broadcasted_iota(jnp.int32, st.shape, 0)
    previous = jnp.where(t == 0, jnp.broadcast_to(before, st.shape), pltpu.roll(st, 1, 0))
    ddecay[...] = g * previous


def local(
    sizes, mixer_out, out_grad, route_ids, route_weights, gate_branch, states, decay,
    w_proj, w_gate, w_up, w_down,
):
    n_sp, n_y = sizes
    tokens, width = mixer_out.shape
    ch = states.shape[1]
    hidden = w_gate.shape[1]
    cap = 2 * route_ids.shape[1] * tokens // n_sp
    half = cap // 2
    shape = jax.ShapeDtypeStruct
    c, yl, yh = lax.axis_index("c"), lax.axis_index("yl"), lax.axis_index("yh")
    place = jnp.stack([c, yl, lax.axis_index(SP), c * n_y + yh * 2 + yl]).astype(jnp.int32)
    ring = lambda k: [(i, (i + k) % n_y) for i in range(n_y)]
    swap = [(0, 1), (1, 0)]
    wg, wu, wd = w_gate[0], w_up[0], w_down[0]
    q = hidden // 2

    cols = width // 2
    small = pltpu.VMEM((2, tokens), jnp.int32), pltpu.VMEM((2, tokens), F32)
    block = pltpu.VMEM((tokens, cols), BF16)
    send, pick = call(
        functools.partial(dispatch_body, n_sp, cap),
        [shape((n_sp * half, width), BF16), shape((n_sp * cap, tokens), BF16)],
        place, route_ids.T, route_weights.T, mixer_out, out_grad,
        specs=(0, 1, 2, 3), outs_in=(0, 1),
        scratch=[
            *small, block, block,
            pltpu.VMEM((n_sp * half, width), BF16),
            pltpu.VMEM((n_sp * cap, tokens), BF16),
            pltpu.SemaphoreType.DMA((9,)),
        ],
    )
    own = lax.all_to_all(send.reshape(n_sp, half, width), SP, 0, 0, tiled=True)
    own = own.reshape(n_sp * half, width)

    def cut(*refs):
        w, (lo, hi) = refs[:3], refs[3:]
        return [
            (w[k].at[pl.ds(side * q, q)], to.at[pl.ds(k * q, q)])
            for side, to in enumerate((lo, hi))
            for k in range(3)
        ]

    w_lo, w_hi = move(cut, [shape((3 * q, width), BF16)] * 2, 6, wg, wu, wd)
    wa = lax.ppermute(w_lo, Y, ring(1))
    wb = lax.ppermute(w_hi, Y, ring(-1))
    par = lax.ppermute(own, "c", swap)

    units = hidden + 2 * q
    tail = 16
    gated = call(prep_body, shape((tokens, ch), BF16), place, gate_branch, states)
    weight, tails = call(
        past_body, [shape((tokens, ch), F32), shape((tail, ch), F32)],
        place, gate_branch, states, decay,
    )

    slots = n_sp * half
    wide = cols // n_y
    held = pltpu.VMEM((3, units, cols), BF16)
    weights = (wg, wu, wd, wa, wb)
    part = call(
        first_body, shape((3, slots, units), F32), place, own, *weights,
        specs=(1, 2, 3), free=(4, 5), scratch=[held, pltpu.SemaphoreType.DMA((9,))],
    )
    psend, mix = call(
        expert_body,
        [shape((n_y, slots, wide), BF16), shape((slots, 3 * units), BF16)],
        place, par, part, *weights,
        specs=(2, 3, 4), free=(5, 6), outs_in=(1,),
        scratch=[
            held, pltpu.VMEM((slots, 3 * units), BF16), pltpu.SemaphoreType.DMA((10,)),
        ],
    )
    pkeep = call(
        keep_body, shape((n_y, slots, wide), F32), place, mix, *weights,
        specs=(0, 1, 2, 3), free=(4, 5),
        scratch=[
            pltpu.VMEM((2, units, cols), BF16), pltpu.VMEM((slots, 2 * units), BF16),
            pltpu.SemaphoreType.DMA((7,)),
        ],
    )
    precv = lax.ppermute(psend, "c", swap)
    gown = call(
        weight_body, [shape((3 * hidden, width), F32)], place, own, par, mix,
        outs_in=(0,),
        scratch=[
            pltpu.VMEM((2, 3 * hidden, cols), F32), pltpu.SemaphoreType.DMA((6,)),
        ],
    )[0]
    xa = lax.ppermute(own[: slots // 2], Y, ring(1))
    xb = lax.ppermute(own[slots // 2 :], Y, ring(-1))
    pa = lax.ppermute(xa, "c", swap)
    pb = lax.ppermute(xb, "c", swap)
    grads = call(
        rest_body, [shape((1, hidden, width), BF16)] * 3,
        place, xa, xb, pa, pb, wg, wu, wd, gown,
        specs=(4, 5, 6, 7), free=(0, 1, 2, 3), outs_in=(0, 1, 2),
        scratch=[
            pltpu.VMEM((slots, width), BF16), pltpu.VMEM((slots, width), BF16),
            pltpu.VMEM((3, hidden, width), BF16), pltpu.VMEM((3 * hidden, width), F32),
            pltpu.VMEM((3, hidden, width), BF16), pltpu.SemaphoreType.DMA((11,)),
        ],
    )

    psum = (pkeep + precv.astype(F32)).astype(BF16)
    parts = lax.all_to_all(psum, Y, 0, 0, tiled=True)
    ret = call(fold_body, shape((n_sp, cap, wide), BF16), place, parts)
    back = lax.all_to_all(ret, SP, 0, 0, tiled=True)
    mid = call(
        combine_body,
        shape((tokens, ch), BF16),
        place, pick, back.reshape(n_sp * cap, wide), out_grad,
        specs=(0, 2),
        scratch=[
            pltpu.VMEM((n_sp * cap, tokens), BF16), pltpu.VMEM((tokens, ch), BF16),
            pltpu.SemaphoreType.DMA((2,)),
        ],
    )
    mid = lax.all_gather(mid, TP)

    rows = width // n_sp
    row = lambda t: shape((tokens, ch), t)
    out, act = call(
        project_body,
        [shape((n_sp, rows + tail, ch), BF16), row(F32)],
        place, mid, gated, w_proj, weight, tails,
        specs=(1, 2, 3, 4), outs_in=(0,),
        scratch=[
            pltpu.VMEM((tokens, ch), BF16), pltpu.VMEM((width, ch), BF16),
            pltpu.VMEM((tokens, ch), F32), pltpu.VMEM((tail, ch), F32),
            pltpu.VMEM((n_sp, rows + tail, ch), BF16), pltpu.SemaphoreType.DMA((6,)),
        ],
    )
    branch, loc, prod = call(
        scan_body, [row(BF16), row(F32), row(F32)],
        place, act, gate_branch, states, decay,
    )
    got = lax.all_to_all(out, SP, 0, 0, tiled=True)
    proj, drive, ddecay = call(
        finish_body, [shape((rows, ch), F32), row(F32), row(F32)],
        place, got, loc, prod, states,
    )

    return (*grads, proj, branch, drive, ddecay)


def solution(mesh):
    devices = mesh.devices
    n_sp, n_tp = devices.shape
    n_yh = n_tp // 4
    x = 4
    fine = Mesh(
        devices.reshape(n_sp // x, x, n_yh, 2, 2), ("z", "x", "yh", "yl", "c")
    )
    rows, both, weight = P(SP, None), P(SP, TP), P(SP, TP, None)
    return jax.shard_map(
        functools.partial(local, (n_sp, n_tp // 2)),
        mesh=fine,
        in_specs=(rows, rows, rows, rows, both, both, both, P(None, TP), weight, weight, weight),
        out_specs=(weight, weight, weight, both, both, both, both),
        check_vma=False,
    )
```

```python
import functools

import jax
import jax.numpy as jnp
from jax import lax
from jax.experimental import pallas as pl
from jax.experimental.pallas import tpu as pltpu
from jax.sharding import Mesh, PartitionSpec as P


SP = ("z", "x")
Y = ("yh", "yl")
TP = ("yh", "yl", "c")
F32, BF16 = jnp.float32, jnp.bfloat16


VMEM = 12 << 20


def nt(a, b):
    return lax.dot_general(a, b, (((1,), (1,)), ((), ())), preferred_element_type=F32)


def tn(a, b):
    return lax.dot_general(a, b, (((0,), (0,)), ((), ())), preferred_element_type=F32)


def nn(a, b):
    return jnp.dot(a, b, preferred_element_type=F32)


def copies(pairs, sems):
    started = [
        pltpu.make_async_copy(src, dst, sems.at[k]) for k, (src, dst) in enumerate(pairs)
    ]
    for copy in started:
        copy.start()
    return started


def move(pairs_of, out_shape, count, *args):
    def body(*refs):
        for copy in copies(pairs_of(*refs[:-1]), refs[-1]):
            copy.wait()

    anywhere = pl.BlockSpec(memory_space=pl.ANY)
    return pl.pallas_call(
        body,
        in_specs=[anywhere] * len(args),
        out_specs=[pl.BlockSpec(memory_space=pltpu.VMEM)] * len(out_shape),
        out_shape=list(out_shape),
        scratch_shapes=[pltpu.SemaphoreType.DMA((count,))],
        compiler_params=pltpu.CompilerParams(vmem_limit_bytes=8 << 20),
    )(*args)


def call(body, out_shape, place, *args, specs=None, free=(), outs_in=None, scratch=(), vmem=VMEM):
    whole = lambda a: pl.BlockSpec(a.shape, lambda i, s, n=len(a.shape): (0,) * n)
    outs = out_shape if isinstance(out_shape, (list, tuple)) else [out_shape]
    in_specs = [whole(a) for a in args]
    out_specs = [whole(o) for o in outs]
    args, outs = list(args), list(outs)
    for k in specs or ():
        in_specs[k] = pl.BlockSpec(memory_space=pltpu.HBM)
        args[k] = pltpu.with_memory_space_constraint(args[k], pltpu.HBM)
    for k in free:
        in_specs[k] = pl.BlockSpec(memory_space=pl.ANY)
    for k in outs_in or ():
        out_specs[k] = pl.BlockSpec(memory_space=pltpu.HBM)
        outs[k] = pltpu.HBM(outs[k].shape, outs[k].dtype)
    result = pl.pallas_call(
        body,
        grid_spec=pltpu.PrefetchScalarGridSpec(
            num_scalar_prefetch=1,
            grid=(1,),
            in_specs=in_specs,
            out_specs=out_specs,
            scratch_shapes=list(scratch),
        ),
        out_shape=list(outs),
        compiler_params=pltpu.CompilerParams(
            dimension_semantics=("arbitrary",), vmem_limit_bytes=vmem
        ),
    )(place, *args)
    return result if isinstance(out_shape, (list, tuple)) else result[0]


def dispatch_body(experts, cap, place, ids_h, wts_h, x_h, og_h, send_h, pick_h, ids, wts, x, og, send, pick, sems):
    n, cols = x.shape
    half = cap // 2
    mine = pl.ds(pl.multiple_of(place[0] * cols, cols), cols)
    got = copies(
        ((ids_h, ids), (wts_h, wts), (x_h.at[:, mine], x), (og_h.at[:, mine], og)), sems
    )
    before = lax.broadcasted_iota(jnp.int32, (n, n), 0) < lax.broadcasted_iota(
        jnp.int32, (n, n), 1
    )
    before = jnp.where(before, 1.0, 0.0).astype(BF16)
    row = lax.broadcasted_iota(jnp.int32, (experts, n), 0)
    got[0].wait()
    got[1].wait()
    m0, m1 = ids[0:1, :] == row, ids[1:2, :] == row
    named = jnp.where(m0 | m1, 1.0, 0.0).astype(F32)
    wt = jnp.where(m0, wts[0:1, :], 0.0) + jnp.where(m1, wts[1:2, :], 0.0)
    position = nn(named.astype(BF16), before)
    position = jnp.where(named > 0.0, position, -1.0)
    slot = lax.broadcasted_iota(jnp.int32, (experts, half, n), 1).astype(F32)
    at = lambda first: jnp.where(position[:, None, :] == slot + first, 1.0, 0.0).astype(F32)
    hot = at((place[1] * half).astype(F32))
    scale = jnp.sum(hot * wt[:, None, :], axis=2, keepdims=True).reshape(experts * half, 1)
    hot = hot.reshape(experts * half, n).astype(BF16)
    got[2].wait()
    got[3].wait()
    out, wide = [], cols // 2
    for k in range(2):
        where = slice(k * wide, (k + 1) * wide)
        send[:, where] = nn(hot, x[:, where]).astype(BF16)
        there = slice(cols + k * wide, cols + (k + 1) * wide)
        send[:, there] = (nn(hot, og[:, where]) * scale).astype(BF16)
        for cut in (where, there):
            copy = pltpu.make_async_copy(
                send.at[:, cut], send_h.at[:, cut], sems.at[4 + len(out)]
            )
            copy.start()
            out.append(copy)
    pick[...] = (
        jnp.concatenate([at(0.0), at(float(half))], axis=1)
        .reshape(experts * cap, n)
        .astype(BF16)
    )
    kept = pltpu.make_async_copy(pick, pick_h, sems.at[8])
    kept.start()
    for copy in (*out, kept):
        copy.wait()


def split3(v):
    a = v.astype(BF16).astype(F32)
    b = (v - a).astype(BF16).astype(F32)
    return a, b, (v - a - b).astype(BF16).astype(F32)


def prep_body(place, gate, states, decay, gated, weight, tail):
    st, gt, dec = states[...], gate[...].astype(F32), decay[...]
    gated[...] = (gt * st).astype(BF16)
    n = st.shape[0]
    t = lax.broadcasted_iota(jnp.int32, st.shape, 0)
    prefix, k = dec, 1
    while k < n:
        prefix = prefix * jnp.where(t >= k, pltpu.roll(prefix, k, 0), 1.0)
        k *= 2
    weight[...] = prefix * gt
    values = split3(prefix[n - 1 : n])
    line = lax.broadcasted_iota(jnp.int32, tail.shape, 0)
    rows = jnp.zeros(tail.shape, F32)
    for k, v in enumerate(values):
        rows = jnp.where(line == 3 + k, jnp.broadcast_to(v, tail.shape), rows)
    tail[...] = rows


def weight_copies(wg, wu, wd, wa, wb, w_s, where, count):
    h = wg.shape[0]
    q = (w_s.shape[1] - h) // 2
    pairs = []
    for k, w in enumerate((wg, wu, wd)[:count]):
        piece = pl.ds(k * q, q)
        pairs.append((w.at[:, where], w_s.at[k, pl.ds(0, h)]))
        pairs.append((wa.at[piece, where], w_s.at[k, pl.ds(h, q)]))
        pairs.append((wb.at[piece, where], w_s.at[k, pl.ds(h + q, q)]))
    return pairs


def columns(core, cols):
    return pl.ds(pl.multiple_of(core * cols, cols), cols)


def product(k, rows, w_s, loads):
    for copy in loads[3 * k : 3 * k + 3]:
        copy.wait()
    cols = w_s.shape[2]
    side = rows[:, 0:cols] if k < 2 else rows[:, cols:]
    return nt(side, w_s[k])


def first_body(place, own, wg, wu, wd, wa, wb, part, other, w_s, sems):
    cols = w_s.shape[2]
    sides = (w_s, columns(place[0], cols)), (other, columns(1 - place[0], cols))
    pairs = []
    for to, where in sides:
        pairs += weight_copies(wg, wu, wd, wa, wb, to, where, 3)
    loads = copies(pairs, sems)
    for k in range(3):
        part[k] = product(k, own, w_s, loads)
    for copy in loads[9:]:
        copy.wait()


def partials(out, gb, ub, w_s):
    width = out.shape[2]
    p = nn(gb, w_s[0]) + nn(ub, w_s[1])
    for k in range(out.shape[0]):
        out[k] = p[:, k * width : (k + 1) * width].astype(out.dtype)


def expert_body(place, par, part, w_s, psend, mix_h, mix, sems):
    units = w_s.shape[1]
    gate = part[0] + product(0, par, w_s, ())
    up = part[1] + product(1, par, w_s, ())
    grad = part[2] + product(2, par, w_s, ())
    sig = jax.nn.sigmoid(gate)
    silu = gate * sig
    ub = (grad * silu).astype(BF16)
    gb = (grad * up * sig * (1.0 + gate * (1.0 - sig))).astype(BF16)
    mix[:, 0:units] = gb
    mix[:, units : 2 * units] = ub
    mix[:, 2 * units :] = (silu * up).astype(BF16)
    (kept,) = copies(((mix, mix_h),), sems)
    partials(psend, gb, ub, w_s)
    kept.wait()


def keep_body(place, mix_h, wg, wu, wd, wa, wb, pkeep, w_s, mix, sems):
    where = columns(place[0], w_s.shape[2])
    units = w_s.shape[1]
    pairs = weight_copies(wg, wu, wd, wa, wb, w_s, where, 2)
    for copy in copies([(mix_h.at[:, pl.ds(0, 2 * units)], mix)] + pairs, sems):
        copy.wait()
    partials(pkeep, mix[:, 0:units], mix[:, units:], w_s)


def weight_body(place, own, par, mix, gown_h, ga, gb, gown, sems):
    c = place[0]
    h, q = gown.shape[1] // 3, ga.shape[0] // 3
    units, cols = h + 2 * q, gown.shape[2]
    stored = []
    for n, (src, core) in enumerate(((own, c), (par, 1 - c))):
        where = columns(core, cols)
        for k in range(3):
            side = src[:, 0:cols] if k < 2 else src[:, cols:]
            g = tn(mix[:, k * units : (k + 1) * units], side)
            rows = pl.ds(k * h, h)
            gown[n, rows, :] = g[0:h]
            copy = pltpu.make_async_copy(
                gown.at[n, rows], gown_h.at[rows, where], sems.at[3 * n + k]
            )
            copy.start()
            stored.append(copy)
            ga[k * q : (k + 1) * q, where] = g[h : h + q].astype(BF16)
            gb[k * q : (k + 1) * q, where] = g[h + q :].astype(BF16)
    for copy in stored:
        copy.wait()


def fold_body(place, parts, out):
    members, _, ch = parts.shape
    dests, cap = out.shape[0], out.shape[1]
    both = []
    for low in range(2):
        total = parts[low].astype(F32)
        for m in range(low + 2, members, 2):
            total = total + parts[m].astype(F32)
        both.append(total.reshape(dests, cap // 2, ch))
    out[...] = jnp.concatenate(both, axis=1).astype(BF16)


def combine_body(place, pick_h, back, og_h, mid, pick, og, sems):
    n = mid.shape[1]
    got = copies(((pick_h, pick), (og_h.at[:, columns(place[3], n)], og)), sems)
    got[0].wait()
    part = tn(pick[...], back[...])
    got[1].wait()
    mid[...] = (og[...].astype(F32) + part).astype(BF16)


def project_body(
    place, mid, gated_h, w_h, weight_h, tail_h, out_h, act_o, gated, w, weight, tail, out, sems
):
    got = copies(
        ((gated_h, gated), (w_h, w), (weight_h, weight), (tail_h, tail)), sems
    )
    pieces = mid.shape[0]
    ys = pieces // 2
    full = jnp.concatenate([mid[(b % ys) * 2 + b // ys] for b in range(pieces)], axis=1)
    dests, rows = out.shape[0], full.shape[1] // out.shape[0]
    got[0].wait()
    grad = tn(full, gated[...]).astype(BF16)
    for d in range(dests):
        out[d, 0:rows, :] = grad[d * rows : (d + 1) * rows]
    head, rest = pl.ds(0, rows), pl.ds(rows, out.shape[1] - rows)
    sent = copies(((out.at[:, head], out_h.at[:, head]),), sems.at[pl.ds(4, 1)])
    got[1].wait()
    act = nn(full, w[...])
    act_o[...] = act
    got[2].wait()
    got[3].wait()
    total = jnp.sum(weight[...] * act, axis=0, keepdims=True)
    extra = tail[...]
    line = lax.broadcasted_iota(jnp.int32, extra.shape, 0)
    for k, v in enumerate(split3(total)):
        extra = jnp.where(line == k, jnp.broadcast_to(v, extra.shape), extra)
    extra = extra.astype(BF16)
    for d in range(dests):
        out[d, rows:, :] = extra
    sent += copies(((out.at[:, rest], out_h.at[:, rest]),), sems.at[pl.ds(5, 1)])
    for copy in sent:
        copy.wait()


def scan_body(place, act, gate, states, decay, branch, local, prod):
    st, gt, dec = states[...], gate[...].astype(F32), decay[...]
    branch[...] = (act[...] * st).astype(BF16)
    n = st.shape[0]
    t = lax.broadcasted_iota(jnp.int32, st.shape, 0)
    ahead = lambda v, k, fill: jnp.where(t < n - k, pltpu.roll(v, n - k, 0), fill)
    b, a = act[...] * gt, ahead(dec, 1, 1.0)
    k = 1
    while k < n:
        b, a = b + a * ahead(b, k, 0.0), a * ahead(a, k, 1.0)
        k *= 2
    local[...] = b
    prod[...] = a


def finish_body(place, got, local, prod, states, before, proj, drive, ddecay):
    rows = proj.shape[0]
    members = got.shape[0]
    s = place[2]
    total = got[0, 0:rows, :].astype(F32)
    for m in range(1, members):
        total = total + got[m, 0:rows, :].astype(F32)
    proj[...] = total
    carry = jnp.zeros((1, local.shape[1]), F32)
    for m in range(members - 1, -1, -1):
        v = got[m, rows : rows + 8, :].astype(F32)
        later = m > s
        b = jnp.where(later, v[0:1] + v[1:2] + v[2:3], 0.0)
        a = jnp.where(later, v[3:4] + v[4:5] + v[5:6], 1.0)
        carry = b + a * carry
    g = local[...] + prod[...] * carry
    drive[...] = g
    st = states[...]
    t = lax.broadcasted_iota(jnp.int32, st.shape, 0)
    previous = jnp.where(t == 0, jnp.broadcast_to(before[...], st.shape), pltpu.roll(st, 1, 0))
    ddecay[...] = g * previous


def local(
    sizes, mixer_out, out_grad, route_ids, route_weights, gate_branch, states, decay,
    w_proj, w_gate, w_up, w_down,
):
    n_sp, n_y = sizes
    tokens, width = mixer_out.shape
    ch = states.shape[1]
    hidden = w_gate.shape[1]
    cap = 2 * route_ids.shape[1] * tokens // n_sp
    half = cap // 2
    shape = jax.ShapeDtypeStruct
    c, yl, yh = lax.axis_index("c"), lax.axis_index("yl"), lax.axis_index("yh")
    place = jnp.stack([c, yl, lax.axis_index(SP), c * n_y + yh * 2 + yl]).astype(jnp.int32)
    ring = lambda k: [(i, (i + k) % n_y) for i in range(n_y)]
    swap = [(0, 1), (1, 0)]
    wg, wu, wd = w_gate[0], w_up[0], w_down[0]
    q = hidden // 2

    cols = width // 2
    small = pltpu.VMEM((2, tokens), jnp.int32), pltpu.VMEM((2, tokens), F32)
    block = pltpu.VMEM((tokens, cols), BF16)
    send, pick = call(
        functools.partial(dispatch_body, n_sp, cap),
        [shape((n_sp * half, width), BF16), shape((n_sp * cap, tokens), BF16)],
        place, route_ids.T, route_weights.T, mixer_out, out_grad,
        specs=(0, 1, 2, 3), outs_in=(0, 1),
        scratch=[
            *small, block, block,
            pltpu.VMEM((n_sp * half, width), BF16),
            pltpu.VMEM((n_sp * cap, tokens), BF16),
            pltpu.SemaphoreType.DMA((9,)),
        ],
    )
    own = lax.all_to_all(send.reshape(n_sp, half, width), SP, 0, 0, tiled=True)
    own = own.reshape(n_sp * half, width)

    def cut(*refs):
        w, (lo, hi) = refs[:3], refs[3:]
        return [
            (w[k].at[pl.ds(side * q, q)], to.at[pl.ds(k * q, q)])
            for side, to in enumerate((lo, hi))
            for k in range(3)
        ]

    w_lo, w_hi = move(cut, [shape((3 * q, width), BF16)] * 2, 6, wg, wu, wd)
    wa = lax.ppermute(w_lo, Y, ring(1))
    wb = lax.ppermute(w_hi, Y, ring(-1))
    par = lax.ppermute(own, "c", swap)

    units = hidden + 2 * q
    tail = 8
    before = lax.ppermute(states[tokens - 1 :], SP, [(k, k + 1) for k in range(n_sp - 1)])
    gated, weight, tails = call(
        prep_body,
        [shape((tokens, ch), BF16), shape((tokens, ch), F32), shape((tail, ch), F32)],
        place, gate_branch, states, decay,
    )

    slots = n_sp * half
    wide = cols // n_y
    held = pltpu.VMEM((3, units, cols), BF16)
    weights = (wg, wu, wd, wa, wb)
    part, other = call(
        first_body,
        [shape((3, slots, units), F32), shape((3, units, cols), BF16)],
        place, own, *weights,
        specs=(1, 2, 3), free=(4, 5),
        scratch=[held, pltpu.SemaphoreType.DMA((18,))],
    )
    psend, mix = call(
        expert_body,
        [shape((n_y, slots, wide), BF16), shape((slots, 3 * units), BF16)],
        place, par, part, other,
        outs_in=(1,),
        scratch=[pltpu.VMEM((slots, 3 * units), BF16), pltpu.SemaphoreType.DMA((1,))],
    )
    pkeep = call(
        keep_body, shape((n_y, slots, wide), F32), place, mix, *weights,
        specs=(0, 1, 2, 3), free=(4, 5),
        scratch=[
            pltpu.VMEM((2, units, cols), BF16), pltpu.VMEM((slots, 2 * units), BF16),
            pltpu.SemaphoreType.DMA((7,)),
        ],
    )
    precv = lax.ppermute(psend, "c", swap)
    gown, ga, gb = call(
        weight_body,
        [shape((3 * hidden, width), F32), shape((3 * q, width), BF16), shape((3 * q, width), BF16)],
        place, own, par, mix,
        outs_in=(0,),
        scratch=[
            pltpu.VMEM((2, 3 * hidden, cols), F32), pltpu.SemaphoreType.DMA((6,)),
        ],
    )
    back_lo = lax.ppermute(ga, Y, ring(-1))
    back_hi = lax.ppermute(gb, Y, ring(1))

    psum = (pkeep + precv.astype(F32)).astype(BF16)
    parts = lax.all_to_all(psum, Y, 0, 0, tiled=True)
    ret = call(fold_body, shape((n_sp, cap, wide), BF16), place, parts)
    back = lax.all_to_all(ret, SP, 0, 0, tiled=True)
    mid = call(
        combine_body,
        shape((tokens, ch), BF16),
        place, pick, back.reshape(n_sp * cap, wide), out_grad,
        specs=(0, 2),
        scratch=[
            pltpu.VMEM((n_sp * cap, tokens), BF16), pltpu.VMEM((tokens, ch), BF16),
            pltpu.SemaphoreType.DMA((2,)),
        ],
    )
    mid = lax.all_gather(mid, TP)

    rows = width // n_sp
    row = lambda t: shape((tokens, ch), t)
    out, act = call(
        project_body,
        [shape((n_sp, rows + tail, ch), BF16), row(F32)],
        place, mid, gated, w_proj, weight, tails,
        specs=(1, 2, 3, 4), outs_in=(0,),
        scratch=[
            pltpu.VMEM((tokens, ch), BF16), pltpu.VMEM((width, ch), BF16),
            pltpu.VMEM((tokens, ch), F32), pltpu.VMEM((tail, ch), F32),
            pltpu.VMEM((n_sp, rows + tail, ch), BF16), pltpu.SemaphoreType.DMA((6,)),
        ],
    )
    branch, loc, prod = call(
        scan_body, [row(BF16), row(F32), row(F32)],
        place, act, gate_branch, states, decay,
    )
    got = lax.all_to_all(out, SP, 0, 0, tiled=True)
    proj, drive, ddecay = call(
        finish_body, [shape((rows, ch), F32), row(F32), row(F32)],
        place, got, loc, prod, states, before,
    )

    def total(k):
        mine = gown[k * hidden : (k + 1) * hidden]
        other = jnp.concatenate(
            [back_lo[k * q : (k + 1) * q], back_hi[k * q : (k + 1) * q]], axis=0
        )
        return (mine + other.astype(F32)).astype(BF16)[None]

    return (total(0), total(1), total(2), proj, branch, drive, ddecay)


def solution(mesh):
    devices = mesh.devices
    n_sp, n_tp = devices.shape
    n_yh = n_tp // 4
    x = 4
    fine = Mesh(
        devices.reshape(n_sp // x, x, n_yh, 2, 2), ("z", "x", "yh", "yl", "c")
    )
    rows, both, weight = P(SP, None), P(SP, TP), P(SP, TP, None)
    return jax.shard_map(
        functools.partial(local, (n_sp, n_tp // 2)),
        mesh=fine,
        in_specs=(rows, rows, rows, rows, both, both, both, P(None, TP), weight, weight, weight),
        out_specs=(weight, weight, weight, both, both, both, both),
        check_vma=False,
    )
```

```python
import functools

import jax
import jax.numpy as jnp
from jax import lax
from jax.experimental import pallas as pl
from jax.experimental.pallas import tpu as pltpu
from jax.sharding import Mesh, PartitionSpec as P


SP = ("z", "x")
Y = ("yh", "yl")
TP = ("yh", "yl", "c")
F32, BF16 = jnp.float32, jnp.bfloat16


VMEM = 12 << 20


def nt(a, b):
    return lax.dot_general(a, b, (((1,), (1,)), ((), ())), preferred_element_type=F32)


def tn(a, b):
    return lax.dot_general(a, b, (((0,), (0,)), ((), ())), preferred_element_type=F32)


def nn(a, b):
    return jnp.dot(a, b, preferred_element_type=F32)


def copies(pairs, sems):
    started = [
        pltpu.make_async_copy(src, dst, sems.at[k]) for k, (src, dst) in enumerate(pairs)
    ]
    for copy in started:
        copy.start()
    return started


def move(pairs_of, out_shape, count, *args):
    def body(*refs):
        for copy in copies(pairs_of(*refs[:-1]), refs[-1]):
            copy.wait()

    anywhere = pl.BlockSpec(memory_space=pl.ANY)
    return pl.pallas_call(
        body,
        in_specs=[anywhere] * len(args),
        out_specs=[pl.BlockSpec(memory_space=pltpu.VMEM)] * len(out_shape),
        out_shape=list(out_shape),
        scratch_shapes=[pltpu.SemaphoreType.DMA((count,))],
        compiler_params=pltpu.CompilerParams(vmem_limit_bytes=8 << 20),
    )(*args)


def call(body, out_shape, place, *args, specs=None, free=(), outs_in=None, scratch=(), vmem=VMEM):
    whole = lambda a: pl.BlockSpec(a.shape, lambda i, s, n=len(a.shape): (0,) * n)
    outs = out_shape if isinstance(out_shape, (list, tuple)) else [out_shape]
    in_specs = [whole(a) for a in args]
    out_specs = [whole(o) for o in outs]
    args, outs = list(args), list(outs)
    for k in specs or ():
        in_specs[k] = pl.BlockSpec(memory_space=pltpu.HBM)
        args[k] = pltpu.with_memory_space_constraint(args[k], pltpu.HBM)
    for k in free:
        in_specs[k] = pl.BlockSpec(memory_space=pl.ANY)
    for k in outs_in or ():
        out_specs[k] = pl.BlockSpec(memory_space=pltpu.HBM)
        outs[k] = pltpu.HBM(outs[k].shape, outs[k].dtype)
    result = pl.pallas_call(
        body,
        grid_spec=pltpu.PrefetchScalarGridSpec(
            num_scalar_prefetch=1,
            grid=(1,),
            in_specs=in_specs,
            out_specs=out_specs,
            scratch_shapes=list(scratch),
        ),
        out_shape=list(outs),
        compiler_params=pltpu.CompilerParams(
            dimension_semantics=("arbitrary",), vmem_limit_bytes=vmem
        ),
    )(place, *args)
    return result if isinstance(out_shape, (list, tuple)) else result[0]


def dispatch_body(experts, cap, place, ids_h, wts_h, x_h, og_h, send_h, pick_h, ids, wts, x, og, send, pick, sems):
    n, cols = x.shape
    half = cap // 2
    mine = pl.ds(pl.multiple_of(place[0] * cols, cols), cols)
    got = copies(
        ((ids_h, ids), (wts_h, wts), (x_h.at[:, mine], x), (og_h.at[:, mine], og)), sems
    )
    before = lax.broadcasted_iota(jnp.int32, (n, n), 0) < lax.broadcasted_iota(
        jnp.int32, (n, n), 1
    )
    before = jnp.where(before, 1.0, 0.0).astype(BF16)
    row = lax.broadcasted_iota(jnp.int32, (experts, n), 0)
    got[0].wait()
    got[1].wait()
    m0, m1 = ids[0:1, :] == row, ids[1:2, :] == row
    named = jnp.where(m0 | m1, 1.0, 0.0).astype(F32)
    wt = jnp.where(m0, wts[0:1, :], 0.0) + jnp.where(m1, wts[1:2, :], 0.0)
    position = nn(named.astype(BF16), before)
    position = jnp.where(named > 0.0, position, -1.0)
    slot = lax.broadcasted_iota(jnp.int32, (experts, half, n), 1).astype(F32)
    at = lambda first: jnp.where(position[:, None, :] == slot + first, 1.0, 0.0).astype(F32)
    hot = at((place[1] * half).astype(F32))
    scale = jnp.sum(hot * wt[:, None, :], axis=2, keepdims=True).reshape(experts * half, 1)
    hot = hot.reshape(experts * half, n).astype(BF16)
    got[2].wait()
    got[3].wait()
    out, wide = [], cols // 2
    for k in range(2):
        where = slice(k * wide, (k + 1) * wide)
        send[:, where] = nn(hot, x[:, where]).astype(BF16)
        there = slice(cols + k * wide, cols + (k + 1) * wide)
        send[:, there] = (nn(hot, og[:, where]) * scale).astype(BF16)
        for cut in (where, there):
            copy = pltpu.make_async_copy(
                send.at[:, cut], send_h.at[:, cut], sems.at[4 + len(out)]
            )
            copy.start()
            out.append(copy)
    pick[...] = (
        jnp.concatenate([at(0.0), at(float(half))], axis=1)
        .reshape(experts * cap, n)
        .astype(BF16)
    )
    kept = pltpu.make_async_copy(pick, pick_h, sems.at[8])
    kept.start()
    for copy in (*out, kept):
        copy.wait()


def split3(v):
    a = v.astype(BF16).astype(F32)
    b = (v - a).astype(BF16).astype(F32)
    return a, b, (v - a - b).astype(BF16).astype(F32)


def prep_body(place, gate, states, decay, gated, weight, tail):
    st, gt, dec = states[...], gate[...].astype(F32), decay[...]
    gated[...] = (gt * st).astype(BF16)
    n = st.shape[0]
    t = lax.broadcasted_iota(jnp.int32, st.shape, 0)
    prefix, k = dec, 1
    while k < n:
        prefix = prefix * jnp.where(t >= k, pltpu.roll(prefix, k, 0), 1.0)
        k *= 2
    weight[...] = prefix * gt
    values = split3(prefix[n - 1 : n])
    line = lax.broadcasted_iota(jnp.int32, tail.shape, 0)
    rows = jnp.zeros(tail.shape, F32)
    for k, v in enumerate(values):
        rows = jnp.where(line == 3 + k, jnp.broadcast_to(v, tail.shape), rows)
    tail[...] = rows


def weight_copies(wg, wu, wd, wa, wb, w_s, where, count):
    h = wg.shape[0]
    q = (w_s.shape[1] - h) // 2
    pairs = []
    for k, w in enumerate((wg, wu, wd)[:count]):
        piece = pl.ds(k * q, q)
        pairs.append((w.at[:, where], w_s.at[k, pl.ds(0, h)]))
        pairs.append((wa.at[piece, where], w_s.at[k, pl.ds(h, q)]))
        pairs.append((wb.at[piece, where], w_s.at[k, pl.ds(h + q, q)]))
    return pairs


def columns(core, cols):
    return pl.ds(pl.multiple_of(core * cols, cols), cols)


def product(k, rows, w_s, loads):
    for copy in loads[3 * k : 3 * k + 3]:
        copy.wait()
    cols = w_s.shape[2]
    side = rows[:, 0:cols] if k < 2 else rows[:, cols:]
    return nt(side, w_s[k])


def first_body(place, own, wg, wu, wd, wa, wb, part, other, w_s, sems):
    cols = w_s.shape[2]
    sides = (w_s, columns(place[0], cols)), (other, columns(1 - place[0], cols))
    pairs = []
    for to, where in sides:
        pairs += weight_copies(wg, wu, wd, wa, wb, to, where, 3)
    loads = copies(pairs, sems)
    for k in range(3):
        part[k] = product(k, own, w_s, loads)
    for copy in loads[9:]:
        copy.wait()


def partials(out, gb, ub, w_s):
    width = out.shape[2]
    p = nn(gb, w_s[0]) + nn(ub, w_s[1])
    for k in range(out.shape[0]):
        out[k] = p[:, k * width : (k + 1) * width].astype(out.dtype)


def expert_body(place, par, part, w_s, psend, pair, mix_h, mix, sems):
    units = w_s.shape[1]
    gate = part[0] + product(0, par, w_s, ())
    up = part[1] + product(1, par, w_s, ())
    grad = part[2] + product(2, par, w_s, ())
    sig = jax.nn.sigmoid(gate)
    silu = gate * sig
    ub = (grad * silu).astype(BF16)
    gb = (grad * up * sig * (1.0 + gate * (1.0 - sig))).astype(BF16)
    mix[:, 0:units] = gb
    mix[:, units : 2 * units] = ub
    mix[:, 2 * units :] = (silu * up).astype(BF16)
    (kept,) = copies(((mix, mix_h),), sems)
    partials(psend, gb, ub, w_s)
    pair[:, 0:units] = gb
    pair[:, units:] = ub
    kept.wait()


def keep_body(place, pair, w_s, pkeep):
    units = w_s.shape[1]
    partials(pkeep, pair[:, 0:units], pair[:, units:], w_s)


def fetch_body(place, pick_h, og_h, w_h, gated_h, weight_h, tail_h, pick, og, w, gated, weight, tail, sems):
    there = og_h.at[:, columns(place[3], og.shape[1])]
    for copy in copies(
        (
            (pick_h, pick), (there, og), (w_h, w),
            (gated_h, gated), (weight_h, weight), (tail_h, tail),
        ),
        sems,
    ):
        copy.wait()


def weight_body(place, own, par, mix, gown_h, ga, gb, gown, sems):
    c = place[0]
    h, q = gown.shape[1] // 3, ga.shape[0] // 3
    units, cols = h + 2 * q, gown.shape[2]
    stored = []
    for n, (src, core) in enumerate(((own, c), (par, 1 - c))):
        where = columns(core, cols)
        for k in range(3):
            side = src[:, 0:cols] if k < 2 else src[:, cols:]
            g = tn(mix[:, k * units : (k + 1) * units], side)
            rows = pl.ds(k * h, h)
            gown[n, rows, :] = g[0:h]
            copy = pltpu.make_async_copy(
                gown.at[n, rows], gown_h.at[rows, where], sems.at[3 * n + k]
            )
            copy.start()
            stored.append(copy)
            ga[k * q : (k + 1) * q, where] = g[h : h + q].astype(BF16)
            gb[k * q : (k + 1) * q, where] = g[h + q :].astype(BF16)
    for copy in stored:
        copy.wait()


def fold_body(place, parts, out):
    members, _, ch = parts.shape
    dests, cap = out.shape[0], out.shape[1]
    both = []
    for low in range(2):
        total = parts[low].astype(F32)
        for m in range(low + 2, members, 2):
            total = total + parts[m].astype(F32)
        both.append(total.reshape(dests, cap // 2, ch))
    out[...] = jnp.concatenate(both, axis=1).astype(BF16)


def combine_body(place, pick, back, og, mid):
    mid[...] = (og[...].astype(F32) + tn(pick[...], back[...])).astype(BF16)


def project_body(place, mid, gated, w, weight, tail, out_h, act_o, out, sems):
    pieces = mid.shape[0]
    ys = pieces // 2
    full = jnp.concatenate([mid[(b % ys) * 2 + b // ys] for b in range(pieces)], axis=1)
    dests, rows = out.shape[0], full.shape[1] // out.shape[0]
    grad = tn(full, gated[...]).astype(BF16)
    for d in range(dests):
        out[d, 0:rows, :] = grad[d * rows : (d + 1) * rows]
    head, rest = pl.ds(0, rows), pl.ds(rows, out.shape[1] - rows)
    sent = copies(((out.at[:, head], out_h.at[:, head]),), sems.at[pl.ds(0, 1)])
    act = nn(full, w[...])
    act_o[...] = act
    total = jnp.sum(weight[...] * act, axis=0, keepdims=True)
    extra = tail[...]
    line = lax.broadcasted_iota(jnp.int32, extra.shape, 0)
    for k, v in enumerate(split3(total)):
        extra = jnp.where(line == k, jnp.broadcast_to(v, extra.shape), extra)
    extra = extra.astype(BF16)
    for d in range(dests):
        out[d, rows:, :] = extra
    sent += copies(((out.at[:, rest], out_h.at[:, rest]),), sems.at[pl.ds(1, 1)])
    for copy in sent:
        copy.wait()


def scan_body(place, act, gate, states, decay, branch, local, prod):
    st, gt, dec = states[...], gate[...].astype(F32), decay[...]
    branch[...] = (act[...] * st).astype(BF16)
    n = st.shape[0]
    t = lax.broadcasted_iota(jnp.int32, st.shape, 0)
    ahead = lambda v, k, fill: jnp.where(t < n - k, pltpu.roll(v, n - k, 0), fill)
    b, a = act[...] * gt, ahead(dec, 1, 1.0)
    k = 1
    while k < n:
        b, a = b + a * ahead(b, k, 0.0), a * ahead(a, k, 1.0)
        k *= 2
    local[...] = b
    prod[...] = a


def finish_body(place, got, local, prod, states, before, proj, drive, ddecay):
    rows = proj.shape[0]
    members = got.shape[0]
    s = place[2]
    total = got[0, 0:rows, :].astype(F32)
    for m in range(1, members):
        total = total + got[m, 0:rows, :].astype(F32)
    proj[...] = total
    carry = jnp.zeros((1, local.shape[1]), F32)
    for m in range(members - 1, -1, -1):
        v = got[m, rows : rows + 8, :].astype(F32)
        later = m > s
        b = jnp.where(later, v[0:1] + v[1:2] + v[2:3], 0.0)
        a = jnp.where(later, v[3:4] + v[4:5] + v[5:6], 1.0)
        carry = b + a * carry
    g = local[...] + prod[...] * carry
    drive[...] = g
    st = states[...]
    t = lax.broadcasted_iota(jnp.int32, st.shape, 0)
    previous = jnp.where(t == 0, jnp.broadcast_to(before[...], st.shape), pltpu.roll(st, 1, 0))
    ddecay[...] = g * previous


def local(
    sizes, mixer_out, out_grad, route_ids, route_weights, gate_branch, states, decay,
    w_proj, w_gate, w_up, w_down,
):
    n_sp, n_y = sizes
    tokens, width = mixer_out.shape
    ch = states.shape[1]
    hidden = w_gate.shape[1]
    cap = 2 * route_ids.shape[1] * tokens // n_sp
    half = cap // 2
    shape = jax.ShapeDtypeStruct
    c, yl, yh = lax.axis_index("c"), lax.axis_index("yl"), lax.axis_index("yh")
    place = jnp.stack([c, yl, lax.axis_index(SP), c * n_y + yh * 2 + yl]).astype(jnp.int32)
    ring = lambda k: [(i, (i + k) % n_y) for i in range(n_y)]
    swap = [(0, 1), (1, 0)]
    wg, wu, wd = w_gate[0], w_up[0], w_down[0]
    q = hidden // 2

    cols = width // 2
    small = pltpu.VMEM((2, tokens), jnp.int32), pltpu.VMEM((2, tokens), F32)
    block = pltpu.VMEM((tokens, cols), BF16)
    send, pick = call(
        functools.partial(dispatch_body, n_sp, cap),
        [shape((n_sp * half, width), BF16), shape((n_sp * cap, tokens), BF16)],
        place, route_ids.T, route_weights.T, mixer_out, out_grad,
        specs=(0, 1, 2, 3), outs_in=(0, 1),
        scratch=[
            *small, block, block,
            pltpu.VMEM((n_sp * half, width), BF16),
            pltpu.VMEM((n_sp * cap, tokens), BF16),
            pltpu.SemaphoreType.DMA((9,)),
        ],
    )
    own = lax.all_to_all(send.reshape(n_sp, half, width), SP, 0, 0, tiled=True)
    own = own.reshape(n_sp * half, width)

    def cut(*refs):
        w, (lo, hi) = refs[:3], refs[3:]
        return [
            (w[k].at[pl.ds(side * q, q)], to.at[pl.ds(k * q, q)])
            for side, to in enumerate((lo, hi))
            for k in range(3)
        ]

    w_lo, w_hi = move(cut, [shape((3 * q, width), BF16)] * 2, 6, wg, wu, wd)
    wa = lax.ppermute(w_lo, Y, ring(1))
    wb = lax.ppermute(w_hi, Y, ring(-1))
    par = lax.ppermute(own, "c", swap)

    units = hidden + 2 * q
    tail = 8
    before = lax.ppermute(states[tokens - 1 :], SP, [(k, k + 1) for k in range(n_sp - 1)])
    gated, weight, tails = call(
        prep_body,
        [shape((tokens, ch), BF16), shape((tokens, ch), F32), shape((tail, ch), F32)],
        place, gate_branch, states, decay,
    )

    slots = n_sp * half
    wide = cols // n_y
    weights = (wg, wu, wd, wa, wb)
    part, other, mine = call(
        first_body,
        [shape((3, slots, units), F32)] + [shape((3, units, cols), BF16)] * 2,
        place, own, *weights,
        specs=(1, 2, 3), free=(4, 5), scratch=[pltpu.SemaphoreType.DMA((18,))],
    )
    psend, pair, mix = call(
        expert_body,
        [
            shape((n_y, slots, wide), BF16), shape((slots, 2 * units), BF16),
            shape((slots, 3 * units), BF16),
        ],
        place, par, part, other,
        outs_in=(2,),
        scratch=[pltpu.VMEM((slots, 3 * units), BF16), pltpu.SemaphoreType.DMA((1,))],
    )
    pkeep = call(keep_body, shape((n_y, slots, wide), F32), place, pair, mine)
    precv = lax.ppermute(psend, "c", swap)
    gown, ga, gb = call(
        weight_body,
        [shape((3 * hidden, width), F32), shape((3 * q, width), BF16), shape((3 * q, width), BF16)],
        place, own, par, mix,
        outs_in=(0,),
        scratch=[
            pltpu.VMEM((2, 3 * hidden, cols), F32), pltpu.SemaphoreType.DMA((6,)),
        ],
    )
    pick, og, w_p, gated, weight, tails = call(
        fetch_body,
        [
            shape(pick.shape, BF16), shape((tokens, ch), BF16), shape(w_proj.shape, BF16),
            shape(gated.shape, BF16), shape(weight.shape, F32), shape(tails.shape, F32),
        ],
        place, pick, out_grad, w_proj, gated, weight, tails,
        specs=tuple(range(6)), scratch=[pltpu.SemaphoreType.DMA((6,))],
    )
    back_lo = lax.ppermute(ga, Y, ring(-1))
    back_hi = lax.ppermute(gb, Y, ring(1))

    psum = (pkeep + precv.astype(F32)).astype(BF16)
    parts = lax.all_to_all(psum, Y, 0, 0, tiled=True)
    ret = call(fold_body, shape((n_sp, cap, wide), BF16), place, parts)
    back = lax.all_to_all(ret, SP, 0, 0, tiled=True)
    mid = call(
        combine_body,
        shape((tokens, ch), BF16),
        place, pick, back.reshape(n_sp * cap, wide), og,
    )
    mid = lax.all_gather(mid, TP)

    rows = width // n_sp
    row = lambda t: shape((tokens, ch), t)
    out, act = call(
        project_body,
        [shape((n_sp, rows + tail, ch), BF16), row(F32)],
        place, mid, gated, w_p, weight, tails,
        outs_in=(0,),
        scratch=[
            pltpu.VMEM((n_sp, rows + tail, ch), BF16), pltpu.SemaphoreType.DMA((2,)),
        ],
    )
    branch, loc, prod = call(
        scan_body, [row(BF16), row(F32), row(F32)],
        place, act, gate_branch, states, decay,
    )
    got = lax.all_to_all(out, SP, 0, 0, tiled=True)
    proj, drive, ddecay = call(
        finish_body, [shape((rows, ch), F32), row(F32), row(F32)],
        place, got, loc, prod, states, before,
    )

    def total(k):
        mine = gown[k * hidden : (k + 1) * hidden]
        other = jnp.concatenate(
            [back_lo[k * q : (k + 1) * q], back_hi[k * q : (k + 1) * q]], axis=0
        )
        return (mine + other.astype(F32)).astype(BF16)[None]

    return (total(0), total(1), total(2), proj, branch, drive, ddecay)


def solution(mesh):
    devices = mesh.devices
    n_sp, n_tp = devices.shape
    n_yh = n_tp // 4
    x = 4
    fine = Mesh(
        devices.reshape(n_sp // x, x, n_yh, 2, 2), ("z", "x", "yh", "yl", "c")
    )
    rows, both, weight = P(SP, None), P(SP, TP), P(SP, TP, None)
    return jax.shard_map(
        functools.partial(local, (n_sp, n_tp // 2)),
        mesh=fine,
        in_specs=(rows, rows, rows, rows, both, both, both, P(None, TP), weight, weight, weight),
        out_specs=(weight, weight, weight, both, both, both, both),
        check_vma=False,
    )
```

```python
import functools

import jax
import jax.numpy as jnp
from jax import lax
from jax.experimental import pallas as pl
from jax.experimental.pallas import tpu as pltpu
from jax.sharding import Mesh, PartitionSpec as P


SP = ("z", "x")
Y = ("yh", "yl")
TP = ("yh", "yl", "c")
F32, BF16 = jnp.float32, jnp.bfloat16


VMEM = 12 << 20


def nt(a, b):
    return lax.dot_general(a, b, (((1,), (1,)), ((), ())), preferred_element_type=F32)


def tn(a, b):
    return lax.dot_general(a, b, (((0,), (0,)), ((), ())), preferred_element_type=F32)


def nn(a, b):
    return jnp.dot(a, b, preferred_element_type=F32)


def copies(pairs, sems):
    started = [
        pltpu.make_async_copy(src, dst, sems.at[k]) for k, (src, dst) in enumerate(pairs)
    ]
    for copy in started:
        copy.start()
    return started


def move(pairs_of, out_shape, count, *args):
    def body(*refs):
        for copy in copies(pairs_of(*refs[:-1]), refs[-1]):
            copy.wait()

    anywhere = pl.BlockSpec(memory_space=pl.ANY)
    return pl.pallas_call(
        body,
        in_specs=[anywhere] * len(args),
        out_specs=[pl.BlockSpec(memory_space=pltpu.VMEM)] * len(out_shape),
        out_shape=list(out_shape),
        scratch_shapes=[pltpu.SemaphoreType.DMA((count,))],
        compiler_params=pltpu.CompilerParams(vmem_limit_bytes=8 << 20),
    )(*args)


def call(body, out_shape, place, *args, specs=None, free=(), outs_in=None, scratch=(), vmem=VMEM):
    whole = lambda a: pl.BlockSpec(a.shape, lambda i, s, n=len(a.shape): (0,) * n)
    outs = out_shape if isinstance(out_shape, (list, tuple)) else [out_shape]
    in_specs = [whole(a) for a in args]
    out_specs = [whole(o) for o in outs]
    args, outs = list(args), list(outs)
    for k in specs or ():
        in_specs[k] = pl.BlockSpec(memory_space=pltpu.HBM)
        args[k] = pltpu.with_memory_space_constraint(args[k], pltpu.HBM)
    for k in free:
        in_specs[k] = pl.BlockSpec(memory_space=pl.ANY)
    for k in outs_in or ():
        out_specs[k] = pl.BlockSpec(memory_space=pltpu.HBM)
        outs[k] = pltpu.HBM(outs[k].shape, outs[k].dtype)
    result = pl.pallas_call(
        body,
        grid_spec=pltpu.PrefetchScalarGridSpec(
            num_scalar_prefetch=1,
            grid=(1,),
            in_specs=in_specs,
            out_specs=out_specs,
            scratch_shapes=list(scratch),
        ),
        out_shape=list(outs),
        compiler_params=pltpu.CompilerParams(
            dimension_semantics=("arbitrary",), vmem_limit_bytes=vmem
        ),
    )(place, *args)
    return result if isinstance(out_shape, (list, tuple)) else result[0]


def dispatch_body(experts, cap, place, ids_h, wts_h, x_h, og_h, send_h, pick_h, ids, wts, x, og, send, pick, sems):
    n, cols = x.shape
    half = cap // 2
    mine = pl.ds(pl.multiple_of(place[0] * cols, cols), cols)
    got = copies(
        ((ids_h, ids), (wts_h, wts), (x_h.at[:, mine], x), (og_h.at[:, mine], og)), sems
    )
    before = lax.broadcasted_iota(jnp.int32, (n, n), 0) < lax.broadcasted_iota(
        jnp.int32, (n, n), 1
    )
    before = jnp.where(before, 1.0, 0.0).astype(BF16)
    row = lax.broadcasted_iota(jnp.int32, (experts, n), 0)
    got[0].wait()
    got[1].wait()
    m0, m1 = ids[0:1, :] == row, ids[1:2, :] == row
    named = jnp.where(m0 | m1, 1.0, 0.0).astype(F32)
    wt = jnp.where(m0, wts[0:1, :], 0.0) + jnp.where(m1, wts[1:2, :], 0.0)
    position = nn(named.astype(BF16), before)
    position = jnp.where(named > 0.0, position, -1.0)
    slot = lax.broadcasted_iota(jnp.int32, (experts, half, n), 1).astype(F32)
    at = lambda first: jnp.where(position[:, None, :] == slot + first, 1.0, 0.0).astype(F32)
    hot = at((place[1] * half).astype(F32))
    scale = jnp.sum(hot * wt[:, None, :], axis=2, keepdims=True).reshape(experts * half, 1)
    hot = hot.reshape(experts * half, n).astype(BF16)
    got[2].wait()
    got[3].wait()
    out, wide = [], cols // 2
    for k in range(2):
        where = slice(k * wide, (k + 1) * wide)
        send[:, where] = nn(hot, x[:, where]).astype(BF16)
        there = slice(cols + k * wide, cols + (k + 1) * wide)
        send[:, there] = (nn(hot, og[:, where]) * scale).astype(BF16)
        for cut in (where, there):
            copy = pltpu.make_async_copy(
                send.at[:, cut], send_h.at[:, cut], sems.at[4 + len(out)]
            )
            copy.start()
            out.append(copy)
    pick[...] = (
        jnp.concatenate([at(0.0), at(float(half))], axis=1)
        .reshape(experts * cap, n)
        .astype(BF16)
    )
    kept = pltpu.make_async_copy(pick, pick_h, sems.at[8])
    kept.start()
    for copy in (*out, kept):
        copy.wait()


def split3(v):
    a = v.astype(BF16).astype(F32)
    b = (v - a).astype(BF16).astype(F32)
    return a, b, (v - a - b).astype(BF16).astype(F32)


def prep_body(place, gate, states, decay, gated, weight, tail):
    st, gt, dec = states[...], gate[...].astype(F32), decay[...]
    gated[...] = (gt * st).astype(BF16)
    n = st.shape[0]
    t = lax.broadcasted_iota(jnp.int32, st.shape, 0)
    prefix, k = dec, 1
    while k < n:
        prefix = prefix * jnp.where(t >= k, pltpu.roll(prefix, k, 0), 1.0)
        k *= 2
    weight[...] = prefix * gt
    values = split3(prefix[n - 1 : n])
    line = lax.broadcasted_iota(jnp.int32, tail.shape, 0)
    rows = jnp.zeros(tail.shape, F32)
    for k, v in enumerate(values):
        rows = jnp.where(line == 3 + k, jnp.broadcast_to(v, tail.shape), rows)
    tail[...] = rows


def weight_copies(wg, wu, wd, wa, wb, w_s, where, count):
    h = wg.shape[0]
    q = (w_s.shape[1] - h) // 2
    pairs = []
    for k, w in enumerate((wg, wu, wd)[:count]):
        piece = pl.ds(k * q, q)
        pairs.append((w.at[:, where], w_s.at[k, pl.ds(0, h)]))
        pairs.append((wa.at[piece, where], w_s.at[k, pl.ds(h, q)]))
        pairs.append((wb.at[piece, where], w_s.at[k, pl.ds(h + q, q)]))
    return pairs


def columns(core, cols):
    return pl.ds(pl.multiple_of(core * cols, cols), cols)


def product(k, rows, w_s, loads):
    for copy in loads[3 * k : 3 * k + 3]:
        copy.wait()
    cols = w_s.shape[2]
    side = rows[:, 0:cols] if k < 2 else rows[:, cols:]
    return nt(side, w_s[k])


def hold_body(place, wg, wu, wd, w, sems):
    for copy in copies([(v, w.at[k]) for k, v in enumerate((wg, wu, wd))], sems):
        copy.wait()


def first_body(place, own, w, wa, wb, part, other, w_s, sems):
    wg, wu, wd = (w.at[k] for k in range(3))
    cols = w_s.shape[2]
    sides = (w_s, columns(place[0], cols)), (other, columns(1 - place[0], cols))
    pairs = []
    for to, where in sides:
        pairs += weight_copies(wg, wu, wd, wa, wb, to, where, 3)
    loads = copies(pairs, sems)
    for k in range(3):
        part[k] = product(k, own, w_s, loads)
    for copy in loads[9:]:
        copy.wait()


def partials(out, gb, ub, w_s):
    width = out.shape[2]
    p = nn(gb, w_s[0]) + nn(ub, w_s[1])
    for k in range(out.shape[0]):
        out[k] = p[:, k * width : (k + 1) * width].astype(out.dtype)


def expert_body(place, par, part, w_s, psend, pair, mix_h, mix, sems):
    units = w_s.shape[1]
    gate = part[0] + product(0, par, w_s, ())
    up = part[1] + product(1, par, w_s, ())
    grad = part[2] + product(2, par, w_s, ())
    sig = jax.nn.sigmoid(gate)
    silu = gate * sig
    ub = (grad * silu).astype(BF16)
    gb = (grad * up * sig * (1.0 + gate * (1.0 - sig))).astype(BF16)
    mix[:, 0:units] = gb
    mix[:, units : 2 * units] = ub
    mix[:, 2 * units :] = (silu * up).astype(BF16)
    (kept,) = copies(((mix, mix_h),), sems)
    partials(psend, gb, ub, w_s)
    pair[:, 0:units] = gb
    pair[:, units:] = ub
    kept.wait()


def keep_body(place, pair, w_s, pkeep):
    units = w_s.shape[1]
    partials(pkeep, pair[:, 0:units], pair[:, units:], w_s)


def fetch_body(place, pick_h, og_h, w_h, gated_h, weight_h, tail_h, pick, og, w, gated, weight, tail, sems):
    there = og_h.at[:, columns(place[3], og.shape[1])]
    for copy in copies(
        (
            (pick_h, pick), (there, og), (w_h, w),
            (gated_h, gated), (weight_h, weight), (tail_h, tail),
        ),
        sems,
    ):
        copy.wait()


def weight_body(place, own, par, mix, gown_h, ga, gb, gown, sems):
    c = place[0]
    h, q = gown.shape[1] // 3, ga.shape[0] // 3
    units, cols = h + 2 * q, gown.shape[2]
    stored = []
    for n, (src, core) in enumerate(((own, c), (par, 1 - c))):
        where = columns(core, cols)
        for k in range(3):
            side = src[:, 0:cols] if k < 2 else src[:, cols:]
            g = tn(mix[:, k * units : (k + 1) * units], side)
            rows = pl.ds(k * h, h)
            gown[n, rows, :] = g[0:h]
            copy = pltpu.make_async_copy(
                gown.at[n, rows], gown_h.at[rows, where], sems.at[3 * n + k]
            )
            copy.start()
            stored.append(copy)
            ga[k * q : (k + 1) * q, where] = g[h : h + q].astype(BF16)
            gb[k * q : (k + 1) * q, where] = g[h + q :].astype(BF16)
    for copy in stored:
        copy.wait()


def fold_body(place, parts, out):
    members, _, ch = parts.shape
    dests, cap = out.shape[0], out.shape[1]
    both = []
    for low in range(2):
        total = parts[low].astype(F32)
        for m in range(low + 2, members, 2):
            total = total + parts[m].astype(F32)
        both.append(total.reshape(dests, cap // 2, ch))
    out[...] = jnp.concatenate(both, axis=1).astype(BF16)


def combine_body(place, pick, back, og, mid):
    mid[...] = (og[...].astype(F32) + tn(pick[...], back[...])).astype(BF16)


def project_body(place, mid, gated, w, weight, tail, out_h, act_o, out, sems):
    pieces = mid.shape[0]
    ys = pieces // 2
    full = jnp.concatenate([mid[(b % ys) * 2 + b // ys] for b in range(pieces)], axis=1)
    dests, rows = out.shape[0], full.shape[1] // out.shape[0]
    grad = tn(full, gated[...]).astype(BF16)
    for d in range(dests):
        out[d, 0:rows, :] = grad[d * rows : (d + 1) * rows]
    head, rest = pl.ds(0, rows), pl.ds(rows, out.shape[1] - rows)
    sent = copies(((out.at[:, head], out_h.at[:, head]),), sems.at[pl.ds(0, 1)])
    act = nn(full, w[...])
    act_o[...] = act
    total = jnp.sum(weight[...] * act, axis=0, keepdims=True)
    extra = tail[...]
    line = lax.broadcasted_iota(jnp.int32, extra.shape, 0)
    for k, v in enumerate(split3(total)):
        extra = jnp.where(line == k, jnp.broadcast_to(v, extra.shape), extra)
    extra = extra.astype(BF16)
    for d in range(dests):
        out[d, rows:, :] = extra
    sent += copies(((out.at[:, rest], out_h.at[:, rest]),), sems.at[pl.ds(1, 1)])
    for copy in sent:
        copy.wait()


def scan_body(place, act, gate, states, decay, branch, local, prod):
    st, gt, dec = states[...], gate[...].astype(F32), decay[...]
    branch[...] = (act[...] * st).astype(BF16)
    n = st.shape[0]
    t = lax.broadcasted_iota(jnp.int32, st.shape, 0)
    ahead = lambda v, k, fill: jnp.where(t < n - k, pltpu.roll(v, n - k, 0), fill)
    b, a = act[...] * gt, ahead(dec, 1, 1.0)
    k = 1
    while k < n:
        b, a = b + a * ahead(b, k, 0.0), a * ahead(a, k, 1.0)
        k *= 2
    local[...] = b
    prod[...] = a


def finish_body(place, got, local, prod, states, before, proj, drive, ddecay):
    rows = proj.shape[0]
    members = got.shape[0]
    s = place[2]
    total = got[0, 0:rows, :].astype(F32)
    for m in range(1, members):
        total = total + got[m, 0:rows, :].astype(F32)
    proj[...] = total
    carry = jnp.zeros((1, local.shape[1]), F32)
    for m in range(members - 1, -1, -1):
        v = got[m, rows : rows + 8, :].astype(F32)
        later = m > s
        b = jnp.where(later, v[0:1] + v[1:2] + v[2:3], 0.0)
        a = jnp.where(later, v[3:4] + v[4:5] + v[5:6], 1.0)
        carry = b + a * carry
    g = local[...] + prod[...] * carry
    drive[...] = g
    st = states[...]
    t = lax.broadcasted_iota(jnp.int32, st.shape, 0)
    previous = jnp.where(t == 0, jnp.broadcast_to(before[...], st.shape), pltpu.roll(st, 1, 0))
    ddecay[...] = g * previous


def local(
    sizes, mixer_out, out_grad, route_ids, route_weights, gate_branch, states, decay,
    w_proj, w_gate, w_up, w_down,
):
    n_sp, n_y = sizes
    tokens, width = mixer_out.shape
    ch = states.shape[1]
    hidden = w_gate.shape[1]
    cap = 2 * route_ids.shape[1] * tokens // n_sp
    half = cap // 2
    shape = jax.ShapeDtypeStruct
    c, yl, yh = lax.axis_index("c"), lax.axis_index("yl"), lax.axis_index("yh")
    place = jnp.stack([c, yl, lax.axis_index(SP), c * n_y + yh * 2 + yl]).astype(jnp.int32)
    ring = lambda k: [(i, (i + k) % n_y) for i in range(n_y)]
    swap = [(0, 1), (1, 0)]
    wg, wu, wd = w_gate[0], w_up[0], w_down[0]
    q = hidden // 2

    cols = width // 2
    small = pltpu.VMEM((2, tokens), jnp.int32), pltpu.VMEM((2, tokens), F32)
    block = pltpu.VMEM((tokens, cols), BF16)
    send, pick = call(
        functools.partial(dispatch_body, n_sp, cap),
        [shape((n_sp * half, width), BF16), shape((n_sp * cap, tokens), BF16)],
        place, route_ids.T, route_weights.T, mixer_out, out_grad,
        specs=(0, 1, 2, 3), outs_in=(0, 1),
        scratch=[
            *small, block, block,
            pltpu.VMEM((n_sp * half, width), BF16),
            pltpu.VMEM((n_sp * cap, tokens), BF16),
            pltpu.SemaphoreType.DMA((9,)),
        ],
    )
    own = lax.all_to_all(send.reshape(n_sp, half, width), SP, 0, 0, tiled=True)
    own = own.reshape(n_sp * half, width)

    def cut(*refs):
        w, (lo, hi) = refs[:3], refs[3:]
        return [
            (w[k].at[pl.ds(side * q, q)], to.at[pl.ds(k * q, q)])
            for side, to in enumerate((lo, hi))
            for k in range(3)
        ]

    w_lo, w_hi = move(cut, [shape((3 * q, width), BF16)] * 2, 6, wg, wu, wd)
    wa = lax.ppermute(w_lo, Y, ring(1))
    wb = lax.ppermute(w_hi, Y, ring(-1))
    par = lax.ppermute(own, "c", swap)

    units = hidden + 2 * q
    tail = 8
    before = lax.ppermute(states[tokens - 1 :], SP, [(k, k + 1) for k in range(n_sp - 1)])
    gated, weight, tails = call(
        prep_body,
        [shape((tokens, ch), BF16), shape((tokens, ch), F32), shape((tail, ch), F32)],
        place, gate_branch, states, decay,
    )

    slots = n_sp * half
    wide = cols // n_y
    held = call(
        hold_body, shape((3, hidden, width), BF16), place, wg, wu, wd,
        specs=(0, 1, 2), scratch=[pltpu.SemaphoreType.DMA((3,))],
    )
    part, other, mine = call(
        first_body,
        [shape((3, slots, units), F32)] + [shape((3, units, cols), BF16)] * 2,
        place, own, held, wa, wb,
        free=(1, 2, 3), scratch=[pltpu.SemaphoreType.DMA((18,))],
    )
    psend, pair, mix = call(
        expert_body,
        [
            shape((n_y, slots, wide), BF16), shape((slots, 2 * units), BF16),
            shape((slots, 3 * units), BF16),
        ],
        place, par, part, other,
        outs_in=(2,),
        scratch=[pltpu.VMEM((slots, 3 * units), BF16), pltpu.SemaphoreType.DMA((1,))],
    )
    pkeep = call(keep_body, shape((n_y, slots, wide), F32), place, pair, mine)
    precv = lax.ppermute(psend, "c", swap)
    gown, ga, gb = call(
        weight_body,
        [shape((3 * hidden, width), F32), shape((3 * q, width), BF16), shape((3 * q, width), BF16)],
        place, own, par, mix,
        outs_in=(0,),
        scratch=[
            pltpu.VMEM((2, 3 * hidden, cols), F32), pltpu.SemaphoreType.DMA((6,)),
        ],
    )
    pick, og, w_p, gated, weight, tails = call(
        fetch_body,
        [
            shape(pick.shape, BF16), shape((tokens, ch), BF16), shape(w_proj.shape, BF16),
            shape(gated.shape, BF16), shape(weight.shape, F32), shape(tails.shape, F32),
        ],
        place, pick, out_grad, w_proj, gated, weight, tails,
        specs=tuple(range(6)), scratch=[pltpu.SemaphoreType.DMA((6,))],
    )
    back_lo = lax.ppermute(ga, Y, ring(-1))
    back_hi = lax.ppermute(gb, Y, ring(1))

    psum = (pkeep + precv.astype(F32)).astype(BF16)
    parts = lax.all_to_all(psum, Y, 0, 0, tiled=True)
    ret = call(fold_body, shape((n_sp, cap, wide), BF16), place, parts)
    back = lax.all_to_all(ret, SP, 0, 0, tiled=True)
    mid = call(
        combine_body,
        shape((tokens, ch), BF16),
        place, pick, back.reshape(n_sp * cap, wide), og,
    )
    mid = lax.all_gather(mid, TP)

    rows = width // n_sp
    row = lambda t: shape((tokens, ch), t)
    out, act = call(
        project_body,
        [shape((n_sp, rows + tail, ch), BF16), row(F32)],
        place, mid, gated, w_p, weight, tails,
        outs_in=(0,),
        scratch=[
            pltpu.VMEM((n_sp, rows + tail, ch), BF16), pltpu.SemaphoreType.DMA((2,)),
        ],
    )
    branch, loc, prod = call(
        scan_body, [row(BF16), row(F32), row(F32)],
        place, act, gate_branch, states, decay,
    )
    got = lax.all_to_all(out, SP, 0, 0, tiled=True)
    proj, drive, ddecay = call(
        finish_body, [shape((rows, ch), F32), row(F32), row(F32)],
        place, got, loc, prod, states, before,
    )

    def total(k):
        mine = gown[k * hidden : (k + 1) * hidden]
        other = jnp.concatenate(
            [back_lo[k * q : (k + 1) * q], back_hi[k * q : (k + 1) * q]], axis=0
        )
        return (mine + other.astype(F32)).astype(BF16)[None]

    return (total(0), total(1), total(2), proj, branch, drive, ddecay)


def solution(mesh):
    devices = mesh.devices
    n_sp, n_tp = devices.shape
    n_yh = n_tp // 4
    x = 4
    fine = Mesh(
        devices.reshape(n_sp // x, x, n_yh, 2, 2), ("z", "x", "yh", "yl", "c")
    )
    rows, both, weight = P(SP, None), P(SP, TP), P(SP, TP, None)
    return jax.shard_map(
        functools.partial(local, (n_sp, n_tp // 2)),
        mesh=fine,
        in_specs=(rows, rows, rows, rows, both, both, both, P(None, TP), weight, weight, weight),
        out_specs=(weight, weight, weight, both, both, both, both),
        check_vma=False,
    )
```

```python
import functools

import jax
import jax.numpy as jnp
from jax import lax
from jax.experimental import pallas as pl
from jax.experimental.pallas import tpu as pltpu
from jax.sharding import Mesh, PartitionSpec as P


SP = ("z", "x")
Y = ("yh", "yl")
TP = ("yh", "yl", "c")
F32, BF16 = jnp.float32, jnp.bfloat16


VMEM = 12 << 20


def nt(a, b):
    return lax.dot_general(a, b, (((1,), (1,)), ((), ())), preferred_element_type=F32)


def tn(a, b):
    return lax.dot_general(a, b, (((0,), (0,)), ((), ())), preferred_element_type=F32)


def nn(a, b):
    return jnp.dot(a, b, preferred_element_type=F32)


def copies(pairs, sems):
    started = [
        pltpu.make_async_copy(src, dst, sems.at[k]) for k, (src, dst) in enumerate(pairs)
    ]
    for copy in started:
        copy.start()
    return started


def move(pairs_of, out_shape, count, *args):
    def body(*refs):
        for copy in copies(pairs_of(*refs[:-1]), refs[-1]):
            copy.wait()

    anywhere = pl.BlockSpec(memory_space=pl.ANY)
    return pl.pallas_call(
        body,
        in_specs=[anywhere] * len(args),
        out_specs=[pl.BlockSpec(memory_space=pltpu.VMEM)] * len(out_shape),
        out_shape=list(out_shape),
        scratch_shapes=[pltpu.SemaphoreType.DMA((count,))],
        compiler_params=pltpu.CompilerParams(vmem_limit_bytes=8 << 20),
    )(*args)


def call(body, out_shape, place, *args, specs=None, free=(), outs_in=None, scratch=(), vmem=VMEM):
    whole = lambda a: pl.BlockSpec(a.shape, lambda i, s, n=len(a.shape): (0,) * n)
    outs = out_shape if isinstance(out_shape, (list, tuple)) else [out_shape]
    in_specs = [whole(a) for a in args]
    out_specs = [whole(o) for o in outs]
    args, outs = list(args), list(outs)
    for k in specs or ():
        in_specs[k] = pl.BlockSpec(memory_space=pltpu.HBM)
        args[k] = pltpu.with_memory_space_constraint(args[k], pltpu.HBM)
    for k in free:
        in_specs[k] = pl.BlockSpec(memory_space=pl.ANY)
    for k in outs_in or ():
        out_specs[k] = pl.BlockSpec(memory_space=pltpu.HBM)
        outs[k] = pltpu.HBM(outs[k].shape, outs[k].dtype)
    result = pl.pallas_call(
        body,
        grid_spec=pltpu.PrefetchScalarGridSpec(
            num_scalar_prefetch=1,
            grid=(1,),
            in_specs=in_specs,
            out_specs=out_specs,
            scratch_shapes=list(scratch),
        ),
        out_shape=list(outs),
        compiler_params=pltpu.CompilerParams(
            dimension_semantics=("arbitrary",), vmem_limit_bytes=vmem
        ),
    )(place, *args)
    return result if isinstance(out_shape, (list, tuple)) else result[0]


def dispatch_body(experts, cap, place, ids_h, wts_h, x_h, og_h, send_h, pick_h, ids, wts, x, og, send, pick, sems):
    n, cols = x.shape
    half = cap // 2
    mine = pl.ds(pl.multiple_of(place[0] * cols, cols), cols)
    got = copies(
        ((ids_h, ids), (wts_h, wts), (x_h.at[:, mine], x), (og_h.at[:, mine], og)), sems
    )
    before = lax.broadcasted_iota(jnp.int32, (n, n), 0) < lax.broadcasted_iota(
        jnp.int32, (n, n), 1
    )
    before = jnp.where(before, 1.0, 0.0).astype(BF16)
    row = lax.broadcasted_iota(jnp.int32, (experts, n), 0)
    got[0].wait()
    got[1].wait()
    m0, m1 = ids[0:1, :] == row, ids[1:2, :] == row
    named = jnp.where(m0 | m1, 1.0, 0.0).astype(F32)
    wt = jnp.where(m0, wts[0:1, :], 0.0) + jnp.where(m1, wts[1:2, :], 0.0)
    position = nn(named.astype(BF16), before)
    position = jnp.where(named > 0.0, position, -1.0)
    slot = lax.broadcasted_iota(jnp.int32, (experts, half, n), 1).astype(F32)
    at = lambda first: jnp.where(position[:, None, :] == slot + first, 1.0, 0.0).astype(F32)
    hot = at((place[1] * half).astype(F32))
    scale = jnp.sum(hot * wt[:, None, :], axis=2, keepdims=True).reshape(experts * half, 1)
    hot = hot.reshape(experts * half, n).astype(BF16)
    got[2].wait()
    got[3].wait()
    out, wide = [], cols // 2
    for k in range(2):
        where = slice(k * wide, (k + 1) * wide)
        send[:, where] = nn(hot, x[:, where]).astype(BF16)
        there = slice(cols + k * wide, cols + (k + 1) * wide)
        send[:, there] = (nn(hot, og[:, where]) * scale).astype(BF16)
        for cut in (where, there):
            copy = pltpu.make_async_copy(
                send.at[:, cut], send_h.at[:, cut], sems.at[4 + len(out)]
            )
            copy.start()
            out.append(copy)
    pick[...] = (
        jnp.concatenate([at(0.0), at(float(half))], axis=1)
        .reshape(experts * cap, n)
        .astype(BF16)
    )
    kept = pltpu.make_async_copy(pick, pick_h, sems.at[8])
    kept.start()
    for copy in (*out, kept):
        copy.wait()


def split3(v):
    a = v.astype(BF16).astype(F32)
    b = (v - a).astype(BF16).astype(F32)
    return a, b, (v - a - b).astype(BF16).astype(F32)


def prep_body(place, gate, states, decay, gated, weight, tail):
    st, gt, dec = states[...], gate[...].astype(F32), decay[...]
    gated[...] = (gt * st).astype(BF16)
    n = st.shape[0]
    t = lax.broadcasted_iota(jnp.int32, st.shape, 0)
    prefix, k = dec, 1
    while k < n:
        prefix = prefix * jnp.where(t >= k, pltpu.roll(prefix, k, 0), 1.0)
        k *= 2
    weight[...] = prefix * gt
    values = split3(prefix[n - 1 : n])
    line = lax.broadcasted_iota(jnp.int32, tail.shape, 0)
    rows = jnp.zeros(tail.shape, F32)
    for k, v in enumerate(values):
        rows = jnp.where(line == 3 + k, jnp.broadcast_to(v, tail.shape), rows)
    tail[...] = rows


def weight_copies(wg, wu, wd, wa, wb, w_s, where, count):
    h = wg.shape[0]
    q = (w_s.shape[1] - h) // 2
    pairs = []
    for k, w in enumerate((wg, wu, wd)[:count]):
        piece = pl.ds(k * q, q)
        pairs.append((w.at[:, where], w_s.at[k, pl.ds(0, h)]))
        pairs.append((wa.at[piece, where], w_s.at[k, pl.ds(h, q)]))
        pairs.append((wb.at[piece, where], w_s.at[k, pl.ds(h + q, q)]))
    return pairs


def columns(core, cols):
    return pl.ds(pl.multiple_of(core * cols, cols), cols)


def product(k, rows, w_s, loads):
    for copy in loads[3 * k : 3 * k + 3]:
        copy.wait()
    cols = w_s.shape[2]
    side = rows[:, 0:cols] if k < 2 else rows[:, cols:]
    return nt(side, w_s[k])


def first_body(place, own, wg, wu, wd, wa, wb, part, other, w_s, sems):
    cols = w_s.shape[2]
    sides = (w_s, columns(place[0], cols)), (other, columns(1 - place[0], cols))
    pairs = []
    for to, where in sides:
        pairs += weight_copies(wg, wu, wd, wa, wb, to, where, 3)
    loads = copies(pairs, sems)
    for k in range(3):
        part[k] = product(k, own, w_s, loads)
    for copy in loads[9:]:
        copy.wait()


def partials(out, gb, ub, w_s):
    width = out.shape[2]
    p = nn(gb, w_s[0]) + nn(ub, w_s[1])
    for k in range(out.shape[0]):
        out[k] = p[:, k * width : (k + 1) * width].astype(out.dtype)


def expert_body(place, par, part, w_s, psend, pair, mix_h, mix, sems):
    units = w_s.shape[1]
    gate = part[0] + product(0, par, w_s, ())
    up = part[1] + product(1, par, w_s, ())
    grad = part[2] + product(2, par, w_s, ())
    sig = jax.nn.sigmoid(gate)
    silu = gate * sig
    ub = (grad * silu).astype(BF16)
    gb = (grad * up * sig * (1.0 + gate * (1.0 - sig))).astype(BF16)
    mix[:, 0:units] = gb
    mix[:, units : 2 * units] = ub
    mix[:, 2 * units :] = (silu * up).astype(BF16)
    (kept,) = copies(((mix, mix_h),), sems)
    partials(psend, gb, ub, w_s)
    pair[:, 0:units] = gb
    pair[:, units:] = ub
    kept.wait()


def keep_body(place, pair, w_s, pkeep):
    units = w_s.shape[1]
    partials(pkeep, pair[:, 0:units], pair[:, units:], w_s)


def fetch_body(place, pick_h, og_h, w_h, gated_h, weight_h, tail_h, pick, og, w, gated, weight, tail, sems):
    there = og_h.at[:, columns(place[3], og.shape[1])]
    for copy in copies(
        (
            (pick_h, pick), (there, og), (w_h, w),
            (gated_h, gated), (weight_h, weight), (tail_h, tail),
        ),
        sems,
    ):
        copy.wait()


def weight_body(place, own, par, mix, gown_h, ga_h, gb_h, gown, ga, gb, sems):
    c = place[0]
    h, q = gown.shape[0] // 3, ga.shape[0] // 3
    units, cols = h + 2 * q, gown.shape[1] // 2
    stored = []
    for k in range(3):
        mine, near = pl.ds(k * h, h), pl.ds(k * q, q)
        for src, core in ((own, c), (par, 1 - c)):
            where = columns(core, cols)
            side = src[:, 0:cols] if k < 2 else src[:, cols:]
            g = tn(mix[:, k * units : (k + 1) * units], side)
            gown[mine, where] = g[0:h]
            ga[near, where] = g[h : h + q].astype(BF16)
            gb[near, where] = g[h + q :].astype(BF16)
        stored += copies(
            (
                (ga.at[near], ga_h.at[near]), (gb.at[near], gb_h.at[near]),
                (gown.at[mine], gown_h.at[mine]),
            ),
            sems.at[pl.ds(3 * k, 3)],
        )
    for copy in stored:
        copy.wait()


def fold_body(place, parts, out):
    members, _, ch = parts.shape
    dests, cap = out.shape[0], out.shape[1]
    both = []
    for low in range(2):
        total = parts[low].astype(F32)
        for m in range(low + 2, members, 2):
            total = total + parts[m].astype(F32)
        both.append(total.reshape(dests, cap // 2, ch))
    out[...] = jnp.concatenate(both, axis=1).astype(BF16)


def combine_body(place, pick, back, og, mid):
    mid[...] = (og[...].astype(F32) + tn(pick[...], back[...])).astype(BF16)


def project_body(place, mid, gated, w, weight, tail, out_h, act_o, out, sems):
    pieces = mid.shape[0]
    ys = pieces // 2
    full = jnp.concatenate([mid[(b % ys) * 2 + b // ys] for b in range(pieces)], axis=1)
    dests, rows = out.shape[0], full.shape[1] // out.shape[0]
    grad = tn(full, gated[...]).astype(BF16)
    for d in range(dests):
        out[d, 0:rows, :] = grad[d * rows : (d + 1) * rows]
    head, rest = pl.ds(0, rows), pl.ds(rows, out.shape[1] - rows)
    sent = copies(((out.at[:, head], out_h.at[:, head]),), sems.at[pl.ds(0, 1)])
    act = nn(full, w[...])
    act_o[...] = act
    total = jnp.sum(weight[...] * act, axis=0, keepdims=True)
    extra = tail[...]
    line = lax.broadcasted_iota(jnp.int32, extra.shape, 0)
    for k, v in enumerate(split3(total)):
        extra = jnp.where(line == k, jnp.broadcast_to(v, extra.shape), extra)
    extra = extra.astype(BF16)
    for d in range(dests):
        out[d, rows:, :] = extra
    sent += copies(((out.at[:, rest], out_h.at[:, rest]),), sems.at[pl.ds(1, 1)])
    for copy in sent:
        copy.wait()


def scan_body(place, act, gate, states, decay, branch, local, prod):
    st, gt, dec = states[...], gate[...].astype(F32), decay[...]
    branch[...] = (act[...] * st).astype(BF16)
    n = st.shape[0]
    t = lax.broadcasted_iota(jnp.int32, st.shape, 0)
    ahead = lambda v, k, fill: jnp.where(t < n - k, pltpu.roll(v, n - k, 0), fill)
    b, a = act[...] * gt, ahead(dec, 1, 1.0)
    k = 1
    while k < n:
        b, a = b + a * ahead(b, k, 0.0), a * ahead(a, k, 1.0)
        k *= 2
    local[...] = b
    prod[...] = a


def finish_body(place, got, local, prod, states, before, proj, drive, ddecay):
    rows = proj.shape[0]
    members = got.shape[0]
    s = place[2]
    total = got[0, 0:rows, :].astype(F32)
    for m in range(1, members):
        total = total + got[m, 0:rows, :].astype(F32)
    proj[...] = total
    carry = jnp.zeros((1, local.shape[1]), F32)
    for m in range(members - 1, -1, -1):
        v = got[m, rows : rows + 8, :].astype(F32)
        later = m > s
        b = jnp.where(later, v[0:1] + v[1:2] + v[2:3], 0.0)
        a = jnp.where(later, v[3:4] + v[4:5] + v[5:6], 1.0)
        carry = b + a * carry
    g = local[...] + prod[...] * carry
    drive[...] = g
    st = states[...]
    t = lax.broadcasted_iota(jnp.int32, st.shape, 0)
    previous = jnp.where(t == 0, jnp.broadcast_to(before[...], st.shape), pltpu.roll(st, 1, 0))
    ddecay[...] = g * previous


def local(
    sizes, mixer_out, out_grad, route_ids, route_weights, gate_branch, states, decay,
    w_proj, w_gate, w_up, w_down,
):
    n_sp, n_y = sizes
    tokens, width = mixer_out.shape
    ch = states.shape[1]
    hidden = w_gate.shape[1]
    cap = 2 * route_ids.shape[1] * tokens // n_sp
    half = cap // 2
    shape = jax.ShapeDtypeStruct
    c, yl, yh = lax.axis_index("c"), lax.axis_index("yl"), lax.axis_index("yh")
    place = jnp.stack([c, yl, lax.axis_index(SP), c * n_y + yh * 2 + yl]).astype(jnp.int32)
    ring = lambda k: [(i, (i + k) % n_y) for i in range(n_y)]
    swap = [(0, 1), (1, 0)]
    wg, wu, wd = w_gate[0], w_up[0], w_down[0]
    q = hidden // 2

    cols = width // 2
    small = pltpu.VMEM((2, tokens), jnp.int32), pltpu.VMEM((2, tokens), F32)
    block = pltpu.VMEM((tokens, cols), BF16)
    send, pick = call(
        functools.partial(dispatch_body, n_sp, cap),
        [shape((n_sp * half, width), BF16), shape((n_sp * cap, tokens), BF16)],
        place, route_ids.T, route_weights.T, mixer_out, out_grad,
        specs=(0, 1, 2, 3), outs_in=(0, 1),
        scratch=[
            *small, block, block,
            pltpu.VMEM((n_sp * half, width), BF16),
            pltpu.VMEM((n_sp * cap, tokens), BF16),
            pltpu.SemaphoreType.DMA((9,)),
        ],
    )
    own = lax.all_to_all(send.reshape(n_sp, half, width), SP, 0, 0, tiled=True)
    own = own.reshape(n_sp * half, width)

    def cut(*refs):
        w, (lo, hi) = refs[:3], refs[3:]
        return [
            (w[k].at[pl.ds(side * q, q)], to.at[pl.ds(k * q, q)])
            for side, to in enumerate((lo, hi))
            for k in range(3)
        ]

    w_lo, w_hi = move(cut, [shape((3 * q, width), BF16)] * 2, 6, wg, wu, wd)
    wa = lax.ppermute(w_lo, Y, ring(1))
    wb = lax.ppermute(w_hi, Y, ring(-1))
    par = lax.ppermute(own, "c", swap)

    units = hidden + 2 * q
    tail = 8
    before = lax.ppermute(states[tokens - 1 :], SP, [(k, k + 1) for k in range(n_sp - 1)])
    gated, weight, tails = call(
        prep_body,
        [shape((tokens, ch), BF16), shape((tokens, ch), F32), shape((tail, ch), F32)],
        place, gate_branch, states, decay,
    )

    slots = n_sp * half
    wide = cols // n_y
    weights = (wg, wu, wd, wa, wb)
    part, other, mine = call(
        first_body,
        [shape((3, slots, units), F32)] + [shape((3, units, cols), BF16)] * 2,
        place, own, *weights,
        specs=(1, 2, 3), free=(4, 5), scratch=[pltpu.SemaphoreType.DMA((18,))],
    )
    psend, pair, mix = call(
        expert_body,
        [
            shape((n_y, slots, wide), BF16), shape((slots, 2 * units), BF16),
            shape((slots, 3 * units), BF16),
        ],
        place, par, part, other,
        outs_in=(2,),
        scratch=[pltpu.VMEM((slots, 3 * units), BF16), pltpu.SemaphoreType.DMA((1,))],
    )
    pkeep = call(keep_body, shape((n_y, slots, wide), F32), place, pair, mine)
    precv = lax.ppermute(psend, "c", swap)
    gown, ga, gb = call(
        weight_body,
        [shape((3 * hidden, width), F32), shape((3 * q, width), BF16), shape((3 * q, width), BF16)],
        place, own, par, mix,
        outs_in=(0, 1, 2),
        scratch=[
            pltpu.VMEM((3 * hidden, width), F32), pltpu.VMEM((3 * q, width), BF16),
            pltpu.VMEM((3 * q, width), BF16), pltpu.SemaphoreType.DMA((9,)),
        ],
    )
    pick, og, w_p, gated, weight, tails = call(
        fetch_body,
        [
            shape(pick.shape, BF16), shape((tokens, ch), BF16), shape(w_proj.shape, BF16),
            shape(gated.shape, BF16), shape(weight.shape, F32), shape(tails.shape, F32),
        ],
        place, pick, out_grad, w_proj, gated, weight, tails,
        specs=tuple(range(6)), scratch=[pltpu.SemaphoreType.DMA((6,))],
    )
    back_lo = lax.ppermute(ga, Y, ring(-1))
    back_hi = lax.ppermute(gb, Y, ring(1))

    psum = (pkeep + precv.astype(F32)).astype(BF16)
    parts = lax.all_to_all(psum, Y, 0, 0, tiled=True)
    ret = call(fold_body, shape((n_sp, cap, wide), BF16), place, parts)
    back = lax.all_to_all(ret, SP, 0, 0, tiled=True)
    mid = call(
        combine_body,
        shape((tokens, ch), BF16),
        place, pick, back.reshape(n_sp * cap, wide), og,
    )
    mid = lax.all_gather(mid, TP)

    rows = width // n_sp
    row = lambda t: shape((tokens, ch), t)
    out, act = call(
        project_body,
        [shape((n_sp, rows + tail, ch), BF16), row(F32)],
        place, mid, gated, w_p, weight, tails,
        outs_in=(0,),
        scratch=[
            pltpu.VMEM((n_sp, rows + tail, ch), BF16), pltpu.SemaphoreType.DMA((2,)),
        ],
    )
    branch, loc, prod = call(
        scan_body, [row(BF16), row(F32), row(F32)],
        place, act, gate_branch, states, decay,
    )
    got = lax.all_to_all(out, SP, 0, 0, tiled=True)
    proj, drive, ddecay = call(
        finish_body, [shape((rows, ch), F32), row(F32), row(F32)],
        place, got, loc, prod, states, before,
    )

    def total(k):
        mine = gown[k * hidden : (k + 1) * hidden]
        other = jnp.concatenate(
            [back_lo[k * q : (k + 1) * q], back_hi[k * q : (k + 1) * q]], axis=0
        )
        return (mine + other.astype(F32)).astype(BF16)[None]

    return (total(0), total(1), total(2), proj, branch, drive, ddecay)


def solution(mesh):
    devices = mesh.devices
    n_sp, n_tp = devices.shape
    n_yh = n_tp // 4
    x = 4
    fine = Mesh(
        devices.reshape(n_sp // x, x, n_yh, 2, 2), ("z", "x", "yh", "yl", "c")
    )
    rows, both, weight = P(SP, None), P(SP, TP), P(SP, TP, None)
    return jax.shard_map(
        functools.partial(local, (n_sp, n_tp // 2)),
        mesh=fine,
        in_specs=(rows, rows, rows, rows, both, both, both, P(None, TP), weight, weight, weight),
        out_specs=(weight, weight, weight, both, both, both, both),
        check_vma=False,
    )
```

```python
import functools

import jax
import jax.numpy as jnp
from jax import lax
from jax.experimental import pallas as pl
from jax.experimental.pallas import tpu as pltpu
from jax.sharding import Mesh, PartitionSpec as P


SP = ("z", "x")
Y = ("yh", "yl")
TP = ("yh", "yl", "c")
F32, BF16 = jnp.float32, jnp.bfloat16


VMEM = 12 << 20


def nt(a, b):
    return lax.dot_general(a, b, (((1,), (1,)), ((), ())), preferred_element_type=F32)


def tn(a, b):
    return lax.dot_general(a, b, (((0,), (0,)), ((), ())), preferred_element_type=F32)


def nn(a, b):
    return jnp.dot(a, b, preferred_element_type=F32)


def copies(pairs, sems):
    started = [
        pltpu.make_async_copy(src, dst, sems.at[k]) for k, (src, dst) in enumerate(pairs)
    ]
    for copy in started:
        copy.start()
    return started


def move(pairs_of, out_shape, count, *args):
    def body(*refs):
        for copy in copies(pairs_of(*refs[:-1]), refs[-1]):
            copy.wait()

    anywhere = pl.BlockSpec(memory_space=pl.ANY)
    return pl.pallas_call(
        body,
        in_specs=[anywhere] * len(args),
        out_specs=[pl.BlockSpec(memory_space=pltpu.VMEM)] * len(out_shape),
        out_shape=list(out_shape),
        scratch_shapes=[pltpu.SemaphoreType.DMA((count,))],
        compiler_params=pltpu.CompilerParams(vmem_limit_bytes=8 << 20),
    )(*args)


def call(body, out_shape, place, *args, specs=None, free=(), outs_in=None, scratch=(), vmem=VMEM):
    whole = lambda a: pl.BlockSpec(a.shape, lambda i, s, n=len(a.shape): (0,) * n)
    outs = out_shape if isinstance(out_shape, (list, tuple)) else [out_shape]
    in_specs = [whole(a) for a in args]
    out_specs = [whole(o) for o in outs]
    args, outs = list(args), list(outs)
    for k in specs or ():
        in_specs[k] = pl.BlockSpec(memory_space=pltpu.HBM)
        args[k] = pltpu.with_memory_space_constraint(args[k], pltpu.HBM)
    for k in free:
        in_specs[k] = pl.BlockSpec(memory_space=pl.ANY)
    for k in outs_in or ():
        out_specs[k] = pl.BlockSpec(memory_space=pltpu.HBM)
        outs[k] = pltpu.HBM(outs[k].shape, outs[k].dtype)
    result = pl.pallas_call(
        body,
        grid_spec=pltpu.PrefetchScalarGridSpec(
            num_scalar_prefetch=1,
            grid=(1,),
            in_specs=in_specs,
            out_specs=out_specs,
            scratch_shapes=list(scratch),
        ),
        out_shape=list(outs),
        compiler_params=pltpu.CompilerParams(
            dimension_semantics=("arbitrary",), vmem_limit_bytes=vmem
        ),
    )(place, *args)
    return result if isinstance(out_shape, (list, tuple)) else result[0]


def positions(ids, experts):
    n = ids.shape[1]
    before = lax.broadcasted_iota(jnp.int32, (n, n), 0) < lax.broadcasted_iota(
        jnp.int32, (n, n), 1
    )
    before = jnp.where(before, 1.0, 0.0).astype(BF16)
    row = lax.broadcasted_iota(jnp.int32, (experts, n), 0)
    m0, m1 = ids[0:1, :] == row, ids[1:2, :] == row
    named = jnp.where(m0 | m1, 1.0, 0.0).astype(F32)
    position = jnp.where(named > 0.0, nn(named.astype(BF16), before), -1.0)
    return m0, m1, position


def one_hot(position, first, count):
    experts, n = position.shape
    slot = lax.broadcasted_iota(jnp.int32, (experts, count, n), 1).astype(F32)
    return jnp.where(position[:, None, :] == slot + first, 1.0, 0.0).astype(F32)


def dispatch_body(experts, cap, place, ids_h, wts_h, x_h, og_h, send_h, ids, wts, x, og, send, sems):
    n, cols = x.shape
    half = cap // 2
    mine = pl.ds(pl.multiple_of(place[0] * cols, cols), cols)
    got = copies(
        ((ids_h, ids), (wts_h, wts), (x_h.at[:, mine], x), (og_h.at[:, mine], og)), sems
    )
    got[0].wait()
    got[1].wait()
    m0, m1, position = positions(ids[...], experts)
    wt = jnp.where(m0, wts[0:1, :], 0.0) + jnp.where(m1, wts[1:2, :], 0.0)
    hot = one_hot(position, (place[1] * half).astype(F32), half)
    scale = jnp.sum(hot * wt[:, None, :], axis=2, keepdims=True).reshape(experts * half, 1)
    hot = hot.reshape(experts * half, n).astype(BF16)
    got[2].wait()
    got[3].wait()
    out, wide = [], cols // 2
    for k in range(2):
        where = slice(k * wide, (k + 1) * wide)
        send[:, where] = nn(hot, x[:, where]).astype(BF16)
        there = slice(cols + k * wide, cols + (k + 1) * wide)
        send[:, there] = (nn(hot, og[:, where]) * scale).astype(BF16)
        for cut in (where, there):
            copy = pltpu.make_async_copy(
                send.at[:, cut], send_h.at[:, cut], sems.at[4 + len(out)]
            )
            copy.start()
            out.append(copy)
    for copy in out:
        copy.wait()


def split3(v):
    a = v.astype(BF16).astype(F32)
    b = (v - a).astype(BF16).astype(F32)
    return a, b, (v - a - b).astype(BF16).astype(F32)


def prep_body(place, gate, states, decay, gated, weight, tail):
    st, gt, dec = states[...], gate[...].astype(F32), decay[...]
    gated[...] = (gt * st).astype(BF16)
    n = st.shape[0]
    t = lax.broadcasted_iota(jnp.int32, st.shape, 0)
    prefix, k = dec, 1
    while k < n:
        prefix = prefix * jnp.where(t >= k, pltpu.roll(prefix, k, 0), 1.0)
        k *= 2
    weight[...] = prefix * gt
    values = split3(prefix[n - 1 : n])
    line = lax.broadcasted_iota(jnp.int32, tail.shape, 0)
    rows = jnp.zeros(tail.shape, F32)
    for k, v in enumerate(values):
        rows = jnp.where(line == 3 + k, jnp.broadcast_to(v, tail.shape), rows)
    tail[...] = rows


def weight_copies(wg, wu, wd, wa, wb, w_s, where, count):
    h = wg.shape[0]
    q = (w_s.shape[1] - h) // 2
    pairs = []
    for k, w in enumerate((wg, wu, wd)[:count]):
        piece = pl.ds(k * q, q)
        pairs.append((w.at[:, where], w_s.at[k, pl.ds(0, h)]))
        pairs.append((wa.at[piece, where], w_s.at[k, pl.ds(h, q)]))
        pairs.append((wb.at[piece, where], w_s.at[k, pl.ds(h + q, q)]))
    return pairs


def columns(core, cols):
    return pl.ds(pl.multiple_of(core * cols, cols), cols)


def product(k, rows, w_s, loads):
    for copy in loads[3 * k : 3 * k + 3]:
        copy.wait()
    cols = w_s.shape[2]
    side = rows[:, 0:cols] if k < 2 else rows[:, cols:]
    return nt(side, w_s[k])


def first_body(place, own, wg, wu, wd, wa, wb, part, other, w_s, sems):
    cols = w_s.shape[2]
    sides = (w_s, columns(place[0], cols)), (other, columns(1 - place[0], cols))
    pairs = []
    for to, where in sides:
        pairs += weight_copies(wg, wu, wd, wa, wb, to, where, 3)
    loads = copies(pairs, sems)
    for k in range(3):
        part[k] = product(k, own, w_s, loads)
    for copy in loads[9:]:
        copy.wait()


def partials(out, gb, ub, w_s):
    width = out.shape[2]
    p = nn(gb, w_s[0]) + nn(ub, w_s[1])
    for k in range(out.shape[0]):
        out[k] = p[:, k * width : (k + 1) * width].astype(out.dtype)


def expert_body(place, par, part, w_s, psend, pair, mix_h, mix, sems):
    units = w_s.shape[1]
    gate = part[0] + product(0, par, w_s, ())
    up = part[1] + product(1, par, w_s, ())
    grad = part[2] + product(2, par, w_s, ())
    sig = jax.nn.sigmoid(gate)
    silu = gate * sig
    ub = (grad * silu).astype(BF16)
    gb = (grad * up * sig * (1.0 + gate * (1.0 - sig))).astype(BF16)
    mix[:, 0:units] = gb
    mix[:, units : 2 * units] = ub
    mix[:, 2 * units :] = (silu * up).astype(BF16)
    (kept,) = copies(((mix, mix_h),), sems)
    partials(psend, gb, ub, w_s)
    pair[:, 0:units] = gb
    pair[:, units:] = ub
    kept.wait()


def keep_body(place, pair, w_s, pkeep):
    units = w_s.shape[1]
    partials(pkeep, pair[:, 0:units], pair[:, units:], w_s)


def fetch_body(
    experts, place, ids_h, og_h, w_h, gated_h, weight_h, tail_h,
    pick, og, w, gated, weight, tail, ids, sems,
):
    there = og_h.at[:, columns(place[3], og.shape[1])]
    got = copies(
        (
            (ids_h, ids), (there, og), (w_h, w),
            (gated_h, gated), (weight_h, weight), (tail_h, tail),
        ),
        sems,
    )
    got[0].wait()
    position = positions(ids[...], experts)[2]
    pick[...] = one_hot(position, 0.0, pick.shape[0] // experts).reshape(pick.shape).astype(BF16)
    for copy in got[1:]:
        copy.wait()


def weight_body(place, own, par, mix, gown_h, ga_h, gb_h, gown, ga, gb, sems):
    c = place[0]
    h, q = gown.shape[0] // 3, ga.shape[0] // 3
    units, cols = h + 2 * q, gown.shape[1] // 2
    stored = []
    for k in range(3):
        mine, near = pl.ds(k * h, h), pl.ds(k * q, q)
        for src, core in ((own, c), (par, 1 - c)):
            where = columns(core, cols)
            side = src[:, 0:cols] if k < 2 else src[:, cols:]
            g = tn(mix[:, k * units : (k + 1) * units], side)
            gown[mine, where] = g[0:h]
            ga[near, where] = g[h : h + q].astype(BF16)
            gb[near, where] = g[h + q :].astype(BF16)
        stored += copies(
            (
                (ga.at[near], ga_h.at[near]), (gb.at[near], gb_h.at[near]),
                (gown.at[mine], gown_h.at[mine]),
            ),
            sems.at[pl.ds(3 * k, 3)],
        )
    for copy in stored:
        copy.wait()


def fold_body(place, parts, out):
    members, _, ch = parts.shape
    dests, cap = out.shape[0], out.shape[1]
    both = []
    for low in range(2):
        total = parts[low].astype(F32)
        for m in range(low + 2, members, 2):
            total = total + parts[m].astype(F32)
        both.append(total.reshape(dests, cap // 2, ch))
    out[...] = jnp.concatenate(both, axis=1).astype(BF16)


def combine_body(place, pick, back, og, mid):
    mid[...] = (og[...].astype(F32) + tn(pick[...], back[...])).astype(BF16)


def project_body(place, mid, gated, w, weight, tail, out_h, act_o, out, sems):
    pieces = mid.shape[0]
    ys = pieces // 2
    full = jnp.concatenate([mid[(b % ys) * 2 + b // ys] for b in range(pieces)], axis=1)
    dests = out.shape[0]
    rows = full.shape[1] // dests
    act = nn(full, w[...])
    act_o[...] = act
    total = jnp.sum(weight[...] * act, axis=0, keepdims=True)
    extra = tail[...]
    line = lax.broadcasted_iota(jnp.int32, extra.shape, 0)
    for k, v in enumerate(split3(total)):
        extra = jnp.where(line == k, jnp.broadcast_to(v, extra.shape), extra)
    extra = extra.astype(BF16)
    sent, steps = [], 4
    each = dests // steps
    for k in range(steps):
        first = k * each
        grad = tn(full[:, first * rows : (first + each) * rows], gated[...]).astype(BF16)
        for d in range(each):
            out[first + d, 0:rows, :] = grad[d * rows : (d + 1) * rows]
            out[first + d, rows:, :] = extra
        part = pl.ds(first, each)
        sent += copies(((out.at[part], out_h.at[part]),), sems.at[pl.ds(k, 1)])
    for copy in sent:
        copy.wait()


def scan_body(place, act, gate, states, decay, branch, local, prod):
    st, gt, dec = states[...], gate[...].astype(F32), decay[...]
    branch[...] = (act[...] * st).astype(BF16)
    n = st.shape[0]
    t = lax.broadcasted_iota(jnp.int32, st.shape, 0)
    ahead = lambda v, k, fill: jnp.where(t < n - k, pltpu.roll(v, n - k, 0), fill)
    b, a = act[...] * gt, ahead(dec, 1, 1.0)
    k = 1
    while k < n:
        b, a = b + a * ahead(b, k, 0.0), a * ahead(a, k, 1.0)
        k *= 2
    local[...] = b
    prod[...] = a


def finish_body(place, got, local, prod, states, before, proj, drive, ddecay):
    rows = proj.shape[0]
    members = got.shape[0]
    s = place[2]
    total = got[0, 0:rows, :].astype(F32)
    for m in range(1, members):
        total = total + got[m, 0:rows, :].astype(F32)
    proj[...] = total
    carry = jnp.zeros((1, local.shape[1]), F32)
    for m in range(members - 1, -1, -1):
        v = got[m, rows : rows + 8, :].astype(F32)
        later = m > s
        b = jnp.where(later, v[0:1] + v[1:2] + v[2:3], 0.0)
        a = jnp.where(later, v[3:4] + v[4:5] + v[5:6], 1.0)
        carry = b + a * carry
    g = local[...] + prod[...] * carry
    drive[...] = g
    st = states[...]
    t = lax.broadcasted_iota(jnp.int32, st.shape, 0)
    previous = jnp.where(t == 0, jnp.broadcast_to(before[...], st.shape), pltpu.roll(st, 1, 0))
    ddecay[...] = g * previous


def local(
    sizes, mixer_out, out_grad, route_ids, route_weights, gate_branch, states, decay,
    w_proj, w_gate, w_up, w_down,
):
    n_sp, n_y = sizes
    tokens, width = mixer_out.shape
    ch = states.shape[1]
    hidden = w_gate.shape[1]
    cap = 2 * route_ids.shape[1] * tokens // n_sp
    half = cap // 2
    shape = jax.ShapeDtypeStruct
    c, yl, yh = lax.axis_index("c"), lax.axis_index("yl"), lax.axis_index("yh")
    place = jnp.stack([c, yl, lax.axis_index(SP), c * n_y + yh * 2 + yl]).astype(jnp.int32)
    ring = lambda k: [(i, (i + k) % n_y) for i in range(n_y)]
    swap = [(0, 1), (1, 0)]
    wg, wu, wd = w_gate[0], w_up[0], w_down[0]
    q = hidden // 2

    cols = width // 2
    small = pltpu.VMEM((2, tokens), jnp.int32), pltpu.VMEM((2, tokens), F32)
    block = pltpu.VMEM((tokens, cols), BF16)
    send = call(
        functools.partial(dispatch_body, n_sp, cap),
        [shape((n_sp * half, width), BF16)],
        place, route_ids.T, route_weights.T, mixer_out, out_grad,
        specs=(0, 1, 2, 3), outs_in=(0,),
        scratch=[
            *small, block, block,
            pltpu.VMEM((n_sp * half, width), BF16), pltpu.SemaphoreType.DMA((8,)),
        ],
    )[0]
    own = lax.all_to_all(send.reshape(n_sp, half, width), SP, 0, 0, tiled=True)
    own = own.reshape(n_sp * half, width)

    def cut(*refs):
        w, (lo, hi) = refs[:3], refs[3:]
        return [
            (w[k].at[pl.ds(side * q, q)], to.at[pl.ds(k * q, q)])
            for side, to in enumerate((lo, hi))
            for k in range(3)
        ]

    w_lo, w_hi = move(cut, [shape((3 * q, width), BF16)] * 2, 6, wg, wu, wd)
    wa = lax.ppermute(w_lo, Y, ring(1))
    wb = lax.ppermute(w_hi, Y, ring(-1))
    par = lax.ppermute(own, "c", swap)

    units = hidden + 2 * q
    tail = 8
    before = lax.ppermute(states[tokens - 1 :], SP, [(k, k + 1) for k in range(n_sp - 1)])
    gated, weight, tails = call(
        prep_body,
        [shape((tokens, ch), BF16), shape((tokens, ch), F32), shape((tail, ch), F32)],
        place, gate_branch, states, decay,
    )

    slots = n_sp * half
    wide = cols // n_y
    weights = (wg, wu, wd, wa, wb)
    part, other, mine = call(
        first_body,
        [shape((3, slots, units), F32)] + [shape((3, units, cols), BF16)] * 2,
        place, own, *weights,
        specs=(1, 2, 3), free=(4, 5), scratch=[pltpu.SemaphoreType.DMA((18,))],
    )
    psend, pair, mix = call(
        expert_body,
        [
            shape((n_y, slots, wide), BF16), shape((slots, 2 * units), BF16),
            shape((slots, 3 * units), BF16),
        ],
        place, par, part, other,
        outs_in=(2,),
        scratch=[pltpu.VMEM((slots, 3 * units), BF16), pltpu.SemaphoreType.DMA((1,))],
    )
    pkeep = call(keep_body, shape((n_y, slots, wide), F32), place, pair, mine)
    precv = lax.ppermute(psend, "c", swap)
    gown, ga, gb = call(
        weight_body,
        [shape((3 * hidden, width), F32), shape((3 * q, width), BF16), shape((3 * q, width), BF16)],
        place, own, par, mix,
        outs_in=(0, 1, 2),
        scratch=[
            pltpu.VMEM((3 * hidden, width), F32), pltpu.VMEM((3 * q, width), BF16),
            pltpu.VMEM((3 * q, width), BF16), pltpu.SemaphoreType.DMA((9,)),
        ],
    )
    pick, og, w_p, gated, weight, tails = call(
        functools.partial(fetch_body, n_sp),
        [
            shape((n_sp * cap, tokens), BF16), shape((tokens, ch), BF16),
            shape(w_proj.shape, BF16),
            shape(gated.shape, BF16), shape(weight.shape, F32), shape(tails.shape, F32),
        ],
        place, route_ids.T, out_grad, w_proj, gated, weight, tails,
        specs=tuple(range(6)), scratch=[small[0], pltpu.SemaphoreType.DMA((6,))],
    )
    back_lo = lax.ppermute(ga, Y, ring(-1))
    back_hi = lax.ppermute(gb, Y, ring(1))

    psum = (pkeep + precv.astype(F32)).astype(BF16)
    parts = lax.all_to_all(psum, Y, 0, 0, tiled=True)
    ret = call(fold_body, shape((n_sp, cap, wide), BF16), place, parts)
    back = lax.all_to_all(ret, SP, 0, 0, tiled=True)
    mid = call(
        combine_body,
        shape((tokens, ch), BF16),
        place, pick, back.reshape(n_sp * cap, wide), og,
    )
    mid = lax.all_gather(mid, TP)

    rows = width // n_sp
    row = lambda t: shape((tokens, ch), t)
    out, act = call(
        project_body,
        [shape((n_sp, rows + tail, ch), BF16), row(F32)],
        place, mid, gated, w_p, weight, tails,
        outs_in=(0,),
        scratch=[
            pltpu.VMEM((n_sp, rows + tail, ch), BF16), pltpu.SemaphoreType.DMA((4,)),
        ],
    )
    branch, loc, prod = call(
        scan_body, [row(BF16), row(F32), row(F32)],
        place, act, gate_branch, states, decay,
    )
    got = lax.all_to_all(out, SP, 0, 0, tiled=True)
    proj, drive, ddecay = call(
        finish_body, [shape((rows, ch), F32), row(F32), row(F32)],
        place, got, loc, prod, states, before,
    )

    def total(k):
        mine = gown[k * hidden : (k + 1) * hidden]
        other = jnp.concatenate(
            [back_lo[k * q : (k + 1) * q], back_hi[k * q : (k + 1) * q]], axis=0
        )
        return (mine + other.astype(F32)).astype(BF16)[None]

    return (total(0), total(1), total(2), proj, branch, drive, ddecay)


def solution(mesh):
    devices = mesh.devices
    n_sp, n_tp = devices.shape
    n_yh = n_tp // 4
    x = 4
    fine = Mesh(
        devices.reshape(n_sp // x, x, n_yh, 2, 2), ("z", "x", "yh", "yl", "c")
    )
    rows, both, weight = P(SP, None), P(SP, TP), P(SP, TP, None)
    return jax.shard_map(
        functools.partial(local, (n_sp, n_tp // 2)),
        mesh=fine,
        in_specs=(rows, rows, rows, rows, both, both, both, P(None, TP), weight, weight, weight),
        out_specs=(weight, weight, weight, both, both, both, both),
        check_vma=False,
    )
```

```python
import functools

import jax
import jax.numpy as jnp
from jax import lax
from jax.experimental import pallas as pl
from jax.experimental.pallas import tpu as pltpu
from jax.sharding import Mesh, PartitionSpec as P


SP = ("z", "x")
Y = ("yh", "yl")
TP = ("yh", "yl", "c")
F32, BF16 = jnp.float32, jnp.bfloat16


VMEM = 12 << 20


def nt(a, b):
    return lax.dot_general(a, b, (((1,), (1,)), ((), ())), preferred_element_type=F32)


def tn(a, b):
    return lax.dot_general(a, b, (((0,), (0,)), ((), ())), preferred_element_type=F32)


def nn(a, b):
    return jnp.dot(a, b, preferred_element_type=F32)


def copies(pairs, sems):
    started = [
        pltpu.make_async_copy(src, dst, sems.at[k]) for k, (src, dst) in enumerate(pairs)
    ]
    for copy in started:
        copy.start()
    return started


def move(pairs_of, out_shape, count, *args):
    def body(*refs):
        for copy in copies(pairs_of(*refs[:-1]), refs[-1]):
            copy.wait()

    anywhere = pl.BlockSpec(memory_space=pl.ANY)
    return pl.pallas_call(
        body,
        in_specs=[anywhere] * len(args),
        out_specs=[pl.BlockSpec(memory_space=pltpu.VMEM)] * len(out_shape),
        out_shape=list(out_shape),
        scratch_shapes=[pltpu.SemaphoreType.DMA((count,))],
        compiler_params=pltpu.CompilerParams(vmem_limit_bytes=8 << 20),
    )(*args)


def call(body, out_shape, place, *args, specs=None, free=(), outs_in=None, scratch=(), vmem=VMEM):
    whole = lambda a: pl.BlockSpec(a.shape, lambda i, s, n=len(a.shape): (0,) * n)
    outs = out_shape if isinstance(out_shape, (list, tuple)) else [out_shape]
    in_specs = [whole(a) for a in args]
    out_specs = [whole(o) for o in outs]
    args, outs = list(args), list(outs)
    for k in specs or ():
        in_specs[k] = pl.BlockSpec(memory_space=pltpu.HBM)
        args[k] = pltpu.with_memory_space_constraint(args[k], pltpu.HBM)
    for k in free:
        in_specs[k] = pl.BlockSpec(memory_space=pl.ANY)
    for k in outs_in or ():
        out_specs[k] = pl.BlockSpec(memory_space=pltpu.HBM)
        outs[k] = pltpu.HBM(outs[k].shape, outs[k].dtype)
    result = pl.pallas_call(
        body,
        grid_spec=pltpu.PrefetchScalarGridSpec(
            num_scalar_prefetch=1,
            grid=(1,),
            in_specs=in_specs,
            out_specs=out_specs,
            scratch_shapes=list(scratch),
        ),
        out_shape=list(outs),
        compiler_params=pltpu.CompilerParams(
            dimension_semantics=("arbitrary",), vmem_limit_bytes=vmem
        ),
    )(place, *args)
    return result if isinstance(out_shape, (list, tuple)) else result[0]


def dispatch_body(experts, cap, place, ids_h, wts_h, x_h, og_h, send_h, pick_h, ids, wts, x, og, send, pick, sems):
    n, cols = x.shape
    half = cap // 2
    mine = pl.ds(pl.multiple_of(place[0] * cols, cols), cols)
    got = copies(
        ((ids_h, ids), (wts_h, wts), (x_h.at[:, mine], x), (og_h.at[:, mine], og)), sems
    )
    before = lax.broadcasted_iota(jnp.int32, (n, n), 0) < lax.broadcasted_iota(
        jnp.int32, (n, n), 1
    )
    before = jnp.where(before, 1.0, 0.0).astype(BF16)
    row = lax.broadcasted_iota(jnp.int32, (experts, n), 0)
    got[0].wait()
    got[1].wait()
    m0, m1 = ids[0:1, :] == row, ids[1:2, :] == row
    named = jnp.where(m0 | m1, 1.0, 0.0).astype(F32)
    wt = jnp.where(m0, wts[0:1, :], 0.0) + jnp.where(m1, wts[1:2, :], 0.0)
    position = nn(named.astype(BF16), before)
    position = jnp.where(named > 0.0, position, -1.0)
    slot = lax.broadcasted_iota(jnp.int32, (experts, half, n), 1).astype(F32)
    at = lambda first: jnp.where(position[:, None, :] == slot + first, 1.0, 0.0).astype(F32)
    hot = at((place[1] * half).astype(F32))
    scale = jnp.sum(hot * wt[:, None, :], axis=2, keepdims=True).reshape(experts * half, 1)
    hot = hot.reshape(experts * half, n).astype(BF16)
    got[2].wait()
    got[3].wait()
    out, wide = [], cols // 2
    for k in range(2):
        where = slice(k * wide, (k + 1) * wide)
        send[:, where] = nn(hot, x[:, where]).astype(BF16)
        there = slice(cols + k * wide, cols + (k + 1) * wide)
        send[:, there] = (nn(hot, og[:, where]) * scale).astype(BF16)
        for cut in (where, there):
            copy = pltpu.make_async_copy(
                send.at[:, cut], send_h.at[:, cut], sems.at[4 + len(out)]
            )
            copy.start()
            out.append(copy)
    pick[...] = (
        jnp.concatenate([at(0.0), at(float(half))], axis=1)
        .reshape(experts * cap, n)
        .astype(BF16)
    )
    kept = pltpu.make_async_copy(pick, pick_h, sems.at[8])
    kept.start()
    for copy in (*out, kept):
        copy.wait()


def split3(v):
    a = v.astype(BF16).astype(F32)
    b = (v - a).astype(BF16).astype(F32)
    return a, b, (v - a - b).astype(BF16).astype(F32)


def prep_body(place, gate, states, decay, gated, weight, tail):
    st, gt, dec = states[...], gate[...].astype(F32), decay[...]
    gated[...] = (gt * st).astype(BF16)
    n = st.shape[0]
    t = lax.broadcasted_iota(jnp.int32, st.shape, 0)
    prefix, k = dec, 1
    while k < n:
        prefix = prefix * jnp.where(t >= k, pltpu.roll(prefix, k, 0), 1.0)
        k *= 2
    weight[...] = prefix * gt
    values = split3(prefix[n - 1 : n])
    line = lax.broadcasted_iota(jnp.int32, tail.shape, 0)
    rows = jnp.zeros(tail.shape, F32)
    for k, v in enumerate(values):
        rows = jnp.where(line == 3 + k, jnp.broadcast_to(v, tail.shape), rows)
    tail[...] = rows


def weight_copies(wg, wu, wd, wa, wb, w_s, where, count):
    h = wg.shape[0]
    q = (w_s.shape[1] - h) // 2
    pairs = []
    for k, w in enumerate((wg, wu, wd)[:count]):
        piece = pl.ds(k * q, q)
        pairs.append((w.at[:, where], w_s.at[k, pl.ds(0, h)]))
        pairs.append((wa.at[piece, where], w_s.at[k, pl.ds(h, q)]))
        pairs.append((wb.at[piece, where], w_s.at[k, pl.ds(h + q, q)]))
    return pairs


def columns(core, cols):
    return pl.ds(pl.multiple_of(core * cols, cols), cols)


def product(k, rows, w_s, loads):
    for copy in loads[3 * k : 3 * k + 3]:
        copy.wait()
    cols = w_s.shape[2]
    side = rows[:, 0:cols] if k < 2 else rows[:, cols:]
    return nt(side, w_s[k])


def first_body(place, own, wg, wu, wd, wa, wb, part, other, w_s, sems):
    cols = w_s.shape[2]
    sides = (w_s, columns(place[0], cols)), (other, columns(1 - place[0], cols))
    pairs = []
    for to, where in sides:
        pairs += weight_copies(wg, wu, wd, wa, wb, to, where, 3)
    loads = copies(pairs, sems)
    for k in range(3):
        part[k] = product(k, own, w_s, loads)
    for copy in loads[9:]:
        copy.wait()


def partials(out, gb, ub, w_s):
    width = out.shape[2]
    p = nn(gb, w_s[0]) + nn(ub, w_s[1])
    for k in range(out.shape[0]):
        out[k] = p[:, k * width : (k + 1) * width].astype(out.dtype)


def expert_body(place, par, part, w_s, psend, pair, mix_h, mix, sems):
    units = w_s.shape[1]
    gate = part[0] + product(0, par, w_s, ())
    up = part[1] + product(1, par, w_s, ())
    grad = part[2] + product(2, par, w_s, ())
    sig = jax.nn.sigmoid(gate)
    silu = gate * sig
    ub = (grad * silu).astype(BF16)
    gb = (grad * up * sig * (1.0 + gate * (1.0 - sig))).astype(BF16)
    mix[:, 0:units] = gb
    mix[:, units : 2 * units] = ub
    mix[:, 2 * units :] = (silu * up).astype(BF16)
    (kept,) = copies(((mix, mix_h),), sems)
    partials(psend, gb, ub, w_s)
    pair[:, 0:units] = gb
    pair[:, units:] = ub
    kept.wait()


def keep_body(place, pair, w_s, pkeep):
    units = w_s.shape[1]
    partials(pkeep, pair[:, 0:units], pair[:, units:], w_s)


def fetch_body(place, pick_h, og_h, w_h, gated_h, weight_h, tail_h, pick, og, w, gated, weight, tail, sems):
    there = og_h.at[:, columns(place[3], og.shape[1])]
    for copy in copies(
        (
            (pick_h, pick), (there, og), (w_h, w),
            (gated_h, gated), (weight_h, weight), (tail_h, tail),
        ),
        sems,
    ):
        copy.wait()


def weight_body(place, own, par, mix, gown_h, ga_h, gb_h, gown, ga, gb, sems):
    c = place[0]
    h, q = gown.shape[0] // 3, ga.shape[0] // 3
    units, cols = h + 2 * q, gown.shape[1] // 2
    stored = []
    for k in range(3):
        mine, near = pl.ds(k * h, h), pl.ds(k * q, q)
        for src, core in ((own, c), (par, 1 - c)):
            where = columns(core, cols)
            side = src[:, 0:cols] if k < 2 else src[:, cols:]
            g = tn(mix[:, k * units : (k + 1) * units], side)
            gown[mine, where] = g[0:h]
            ga[near, where] = g[h : h + q].astype(BF16)
            gb[near, where] = g[h + q :].astype(BF16)
        stored += copies(
            (
                (ga.at[near], ga_h.at[near]), (gb.at[near], gb_h.at[near]),
                (gown.at[mine], gown_h.at[mine]),
            ),
            sems.at[pl.ds(3 * k, 3)],
        )
    for copy in stored:
        copy.wait()


def fold_body(place, parts, out):
    members, _, ch = parts.shape
    dests, cap = out.shape[0], out.shape[1]
    both = []
    for low in range(2):
        total = parts[low].astype(F32)
        for m in range(low + 2, members, 2):
            total = total + parts[m].astype(F32)
        both.append(total.reshape(dests, cap // 2, ch))
    out[...] = jnp.concatenate(both, axis=1).astype(BF16)


def combine_body(place, pick, back, og, mid):
    block = (og[...].astype(F32) + tn(pick[...], back[...])).astype(BF16)
    for k in range(mid.shape[0]):
        mid[k] = block


def half_body(place, mid, gated, w, grad, act):
    full = jnp.concatenate([mid[k] for k in range(mid.shape[0])], axis=1)
    grad[...] = tn(full, gated[...]).astype(BF16)
    act[...] = nn(full, w[columns(place[0], full.shape[1]), :])


def project_body(
    place, mid, grad_mine, act_mine, gated, w, weight, tail, out_h, act_o, out, sems
):
    c = place[0]
    full = jnp.concatenate([mid[k] for k in range(mid.shape[0])], axis=1)
    each = out.shape[0] // 2
    rows = full.shape[1] // each
    act = act_mine[...] + nn(full, w[columns(1 - c, full.shape[1]), :])
    act_o[...] = act
    total = jnp.sum(weight[...] * act, axis=0, keepdims=True)
    extra = tail[...]
    line = lax.broadcasted_iota(jnp.int32, extra.shape, 0)
    for k, v in enumerate(split3(total)):
        extra = jnp.where(line == k, jnp.broadcast_to(v, extra.shape), extra)
    extra = extra.astype(BF16)
    sent = []
    for k, core in enumerate((c, 1 - c)):
        grad = grad_mine[...] if k == 0 else tn(full, gated[...]).astype(BF16)
        first = core * each
        for d in range(each):
            out[first + d, 0:rows, :] = grad[d * rows : (d + 1) * rows]
            out[first + d, rows:, :] = extra
        part = pl.ds(first, each)
        sent += copies(((out.at[part], out_h.at[part]),), sems.at[pl.ds(k, 1)])
    for copy in sent:
        copy.wait()


def scan_body(place, act, gate, states, decay, branch, local, prod):
    st, gt, dec = states[...], gate[...].astype(F32), decay[...]
    branch[...] = (act[...] * st).astype(BF16)
    n = st.shape[0]
    t = lax.broadcasted_iota(jnp.int32, st.shape, 0)
    ahead = lambda v, k, fill: jnp.where(t < n - k, pltpu.roll(v, n - k, 0), fill)
    b, a = act[...] * gt, ahead(dec, 1, 1.0)
    k = 1
    while k < n:
        b, a = b + a * ahead(b, k, 0.0), a * ahead(a, k, 1.0)
        k *= 2
    local[...] = b
    prod[...] = a


def finish_body(place, got, local, prod, states, before, proj, drive, ddecay):
    rows = proj.shape[0]
    members = got.shape[0]
    s = place[2]
    total = got[0, 0:rows, :].astype(F32)
    for m in range(1, members):
        total = total + got[m, 0:rows, :].astype(F32)
    proj[...] = total
    carry = jnp.zeros((1, local.shape[1]), F32)
    for m in range(members - 1, -1, -1):
        v = got[m, rows : rows + 8, :].astype(F32)
        later = m > s
        b = jnp.where(later, v[0:1] + v[1:2] + v[2:3], 0.0)
        a = jnp.where(later, v[3:4] + v[4:5] + v[5:6], 1.0)
        carry = b + a * carry
    g = local[...] + prod[...] * carry
    drive[...] = g
    st = states[...]
    t = lax.broadcasted_iota(jnp.int32, st.shape, 0)
    previous = jnp.where(t == 0, jnp.broadcast_to(before[...], st.shape), pltpu.roll(st, 1, 0))
    ddecay[...] = g * previous


def local(
    sizes, mixer_out, out_grad, route_ids, route_weights, gate_branch, states, decay,
    w_proj, w_gate, w_up, w_down,
):
    n_sp, n_y = sizes
    tokens, width = mixer_out.shape
    ch = states.shape[1]
    hidden = w_gate.shape[1]
    cap = 2 * route_ids.shape[1] * tokens // n_sp
    half = cap // 2
    shape = jax.ShapeDtypeStruct
    c, yl, yh = lax.axis_index("c"), lax.axis_index("yl"), lax.axis_index("yh")
    place = jnp.stack([c, yl, lax.axis_index(SP), c * n_y + yh * 2 + yl]).astype(jnp.int32)
    ring = lambda k: [(i, (i + k) % n_y) for i in range(n_y)]
    swap = [(0, 1), (1, 0)]
    wg, wu, wd = w_gate[0], w_up[0], w_down[0]
    q = hidden // 2

    cols = width // 2
    small = pltpu.VMEM((2, tokens), jnp.int32), pltpu.VMEM((2, tokens), F32)
    block = pltpu.VMEM((tokens, cols), BF16)
    send, pick = call(
        functools.partial(dispatch_body, n_sp, cap),
        [shape((n_sp * half, width), BF16), shape((n_sp * cap, tokens), BF16)],
        place, route_ids.T, route_weights.T, mixer_out, out_grad,
        specs=(0, 1, 2, 3), outs_in=(0, 1),
        scratch=[
            *small, block, block,
            pltpu.VMEM((n_sp * half, width), BF16),
            pltpu.VMEM((n_sp * cap, tokens), BF16),
            pltpu.SemaphoreType.DMA((9,)),
        ],
    )
    own = lax.all_to_all(send.reshape(n_sp, half, width), SP, 0, 0, tiled=True)
    own = own.reshape(n_sp * half, width)

    def cut(*refs):
        w, (lo, hi) = refs[:3], refs[3:]
        return [
            (w[k].at[pl.ds(side * q, q)], to.at[pl.ds(k * q, q)])
            for side, to in enumerate((lo, hi))
            for k in range(3)
        ]

    w_lo, w_hi = move(cut, [shape((3 * q, width), BF16)] * 2, 6, wg, wu, wd)
    wa = lax.ppermute(w_lo, Y, ring(1))
    wb = lax.ppermute(w_hi, Y, ring(-1))
    par = lax.ppermute(own, "c", swap)

    units = hidden + 2 * q
    tail = 8
    before = lax.ppermute(states[tokens - 1 :], SP, [(k, k + 1) for k in range(n_sp - 1)])
    gated, weight, tails = call(
        prep_body,
        [shape((tokens, ch), BF16), shape((tokens, ch), F32), shape((tail, ch), F32)],
        place, gate_branch, states, decay,
    )

    slots = n_sp * half
    wide = cols // n_y
    weights = (wg, wu, wd, wa, wb)
    part, other, mine = call(
        first_body,
        [shape((3, slots, units), F32)] + [shape((3, units, cols), BF16)] * 2,
        place, own, *weights,
        specs=(1, 2, 3), free=(4, 5), scratch=[pltpu.SemaphoreType.DMA((18,))],
    )
    psend, pair, mix = call(
        expert_body,
        [
            shape((n_y, slots, wide), BF16), shape((slots, 2 * units), BF16),
            shape((slots, 3 * units), BF16),
        ],
        place, par, part, other,
        outs_in=(2,),
        scratch=[pltpu.VMEM((slots, 3 * units), BF16), pltpu.SemaphoreType.DMA((1,))],
    )
    pkeep = call(keep_body, shape((n_y, slots, wide), F32), place, pair, mine)
    precv = lax.ppermute(psend, "c", swap)
    gown, ga, gb = call(
        weight_body,
        [shape((3 * hidden, width), F32), shape((3 * q, width), BF16), shape((3 * q, width), BF16)],
        place, own, par, mix,
        outs_in=(0, 1, 2),
        scratch=[
            pltpu.VMEM((3 * hidden, width), F32), pltpu.VMEM((3 * q, width), BF16),
            pltpu.VMEM((3 * q, width), BF16), pltpu.SemaphoreType.DMA((9,)),
        ],
    )
    pick, og, w_p, gated, weight, tails = call(
        fetch_body,
        [
            shape(pick.shape, BF16), shape((tokens, ch), BF16), shape(w_proj.shape, BF16),
            shape(gated.shape, BF16), shape(weight.shape, F32), shape(tails.shape, F32),
        ],
        place, pick, out_grad, w_proj, gated, weight, tails,
        specs=tuple(range(6)), scratch=[pltpu.SemaphoreType.DMA((6,))],
    )
    back_lo = lax.ppermute(ga, Y, ring(-1))
    back_hi = lax.ppermute(gb, Y, ring(1))

    psum = (pkeep + precv.astype(F32)).astype(BF16)
    parts = lax.all_to_all(psum, Y, 0, 0, tiled=True)
    ret = call(fold_body, shape((n_sp, cap, wide), BF16), place, parts)
    back = lax.all_to_all(ret, SP, 0, 0, tiled=True)
    mid = call(
        combine_body,
        shape((n_y, tokens, ch), BF16),
        place, pick, back.reshape(n_sp * cap, wide), og,
    )
    mid = lax.all_to_all(mid, Y, 0, 0, tiled=True)
    mid_other = lax.ppermute(mid, "c", swap)

    rows = width // n_sp
    row = lambda t: shape((tokens, ch), t)
    grad_half, act_half = call(
        half_body, [shape((cols, ch), BF16), row(F32)], place, mid, gated, w_p,
    )
    out, act = call(
        project_body,
        [shape((n_sp, rows + tail, ch), BF16), row(F32)],
        place, mid_other, grad_half, act_half, gated, w_p, weight, tails,
        outs_in=(0,),
        scratch=[
            pltpu.VMEM((n_sp, rows + tail, ch), BF16), pltpu.SemaphoreType.DMA((2,)),
        ],
    )
    branch, loc, prod = call(
        scan_body, [row(BF16), row(F32), row(F32)],
        place, act, gate_branch, states, decay,
    )
    got = lax.all_to_all(out, SP, 0, 0, tiled=True)
    proj, drive, ddecay = call(
        finish_body, [shape((rows, ch), F32), row(F32), row(F32)],
        place, got, loc, prod, states, before,
    )

    def total(k):
        mine = gown[k * hidden : (k + 1) * hidden]
        other = jnp.concatenate(
            [back_lo[k * q : (k + 1) * q], back_hi[k * q : (k + 1) * q]], axis=0
        )
        return (mine + other.astype(F32)).astype(BF16)[None]

    return (total(0), total(1), total(2), proj, branch, drive, ddecay)


def solution(mesh):
    devices = mesh.devices
    n_sp, n_tp = devices.shape
    n_yh = n_tp // 4
    x = 4
    fine = Mesh(
        devices.reshape(n_sp // x, x, n_yh, 2, 2), ("z", "x", "yh", "yl", "c")
    )
    rows, both, weight = P(SP, None), P(SP, TP), P(SP, TP, None)
    return jax.shard_map(
        functools.partial(local, (n_sp, n_tp // 2)),
        mesh=fine,
        in_specs=(rows, rows, rows, rows, both, both, both, P(None, TP), weight, weight, weight),
        out_specs=(weight, weight, weight, both, both, both, both),
        check_vma=False,
    )
```
